32 devices in a mesh: grp: 2 (over y), fs: 4 (over z), tp: 4 (over x, core).
Axes of the slice: x: 2, y: 2, z: 4, core: 2. Of those that a mesh axis runs over, the one named last changes fastest.
Arguments:
- tokens: bfloat16 [1536, 2048], P(('grp', 'tp')), parts along dimension 0, may hold values from -6 to 6
- norm_gain: float32 [2048], P('fs'), may hold values from 0.1 to 1.9
- up_trained: float32 [2048, 8192], P('fs', 'tp'), may hold values from -0.125 to 0.125
- down_trained: float32 [2048, 8192], P('fs', 'tp'), may hold values from -0.09375 to 0.09375
Outputs:
- up_serving: bfloat16 [4096, 8192], P('grp', 'fs'), parts along dimension 0
- down_serving: bfloat16 [4096, 8192], P('grp', 'fs'), parts along dimension 0
- prompt_output: bfloat16 [1536, 2048], P(('grp', 'tp'), 'fs'), parts along dimension 0
The draws below stay inside these ranges and needn't reach their ends.
There are 2 independent parts, one for each index of `grp`. The reference program is written for one: setup_inputs(seed, part) draws one part's arguments, and reference() takes and returns one part's arrays. A program takes and returns all parts, laid end to end along the dimension named above; an argument that names none is the same for every part. Nothing has to cross between parts.
All inputs are finite; a program needn't handle non-finite values.
Results may differ from the reference program's by a relative error of at most 0.0074.
Values may be sent and summed in bfloat16 or wider, within the bound.
A program may use at most 128 MiB of HBM per device.

```python
import jax
import jax.numpy as jnp
from jax import lax

D = 2048
FF = 8192
TOKENS = 768


def with_spikes(entries, stream_key, source, target, parts, factor):
    owner, partner = [(jnp.arange(entries.shape[axis_at]) // (entries.shape[axis_at] // parts)).reshape([-1 if axis == axis_at else 1 for axis in range(entries.ndim)]) for axis_at in (source, target)]
    chosen = jax.random.permutation(stream_key, parts)[partner]
    strong = (owner == chosen) | (owner == (partner + parts // 2) % parts)
    return jnp.where(strong, factor * entries, entries)


def levels(rng, extent, shards, least, top_value):
    def one(dim, blocks):
        heights = jax.random.uniform(jax.random.fold_in(jax.random.fold_in(rng, 6), dim), (blocks,), jnp.float32, least / len(shards), top_value / len(shards))
        return jnp.repeat(jnp.exp(heights), extent[dim] // blocks).reshape((-1,) + (1,) * (len(extent) - dim - 1))

    factor_of = one(*shards[0])
    for cut in shards[1:]:
        factor_of = factor_of * one(*cut)
    return factor_of


def normal_values(rng, shape, spread, most, shards=(), dtype=jnp.bfloat16):
    entries = jax.random.normal(rng, shape, jnp.float32) * spread
    if len(shards) > 0:
        entries = levels(rng, shape, shards, -0.22, 0.18) * entries
    return jnp.clip(entries, min=-most, max=most).astype(dtype)


def bell_draw_with(stream_key, extent, scale, reach, cuts, heavy, kind=jnp.bfloat16):
    entries = scale * jax.random.normal(stream_key, extent, jnp.float32)
    if cuts:
        entries = entries * levels(stream_key, extent, cuts, -0.22, 0.18)
    return jnp.clip(with_spikes(entries, jax.random.fold_in(stream_key, 3), *heavy), -reach, reach).astype(kind)


def setup_inputs(seed: int = 0, part: int = 0) -> dict:
    streams_of = jax.random.split(jax.random.key(seed), 5)
    own_keys = jax.random.split(jax.random.fold_in(streams_of[4], part), 5)
    return {
        "tokens": normal_values(own_keys[0], (TOKENS, D), 1.0, 6.0, ((0, 4),)),
        "norm_gain": jnp.clip(1.0 + 0.18 * jax.random.normal(streams_of[1], (D,), jnp.float32), 0.1, 1.9),
        "up_trained": normal_values(streams_of[2], (D, FF), D ** -0.5, 0.125, ((0, 4), (1, 4)), jnp.float32),
        "down_trained": bell_draw_with(streams_of[3], (D, FF), FF ** -0.5, 0.09375, ((0, 4), (1, 4)), (1, 0, 4, 2.0), jnp.float32),
    }


epsilon = 1e-06

def reference(tokens, norm_gain, up_trained, down_trained):
    up_serving = (norm_gain[:, None] * up_trained).astype(jnp.bfloat16)
    down_serving = down_trained.astype(jnp.bfloat16)
    values = tokens.astype(jnp.float32)
    scale = lax.rsqrt(lax.optimization_barrier(jnp.mean(values * values, axis=1, keepdims=True)) + epsilon)
    normed = (values * scale).astype(jnp.bfloat16)
    hidden = jnp.dot(normed, up_serving, preferred_element_type=jnp.float32)
    active = jnp.square(jax.nn.relu(hidden)).astype(jnp.bfloat16)
    prompt_output = jnp.dot(active, down_serving.T, preferred_element_type=jnp.float32).astype(jnp.bfloat16)
    return (up_serving, down_serving, prompt_output)
```

```python
import functools

import jax
import jax.numpy as jnp
from jax import lax
from jax.experimental import pallas as pl
from jax.experimental.pallas import tpu as pltpu
from jax.sharding import PartitionSpec as P

epsilon = 1e-06
MESH = pl.DeviceIdType.MESH


def local_plain(tokens, norm_gain, up_trained, down_trained):
    shards = lax.axis_size("fs")
    groups = lax.axis_size("tp")
    rows_local = up_trained.shape[0]
    cols_local = up_trained.shape[1]
    folded = (norm_gain[:, None] * up_trained).astype(jnp.bfloat16)
    stacked = jnp.stack([folded, down_trained.astype(jnp.bfloat16)])
    served_width = cols_local * groups // shards
    blocks_here = cols_local // served_width
    quarter_rows = rows_local // groups
    pieces = stacked.reshape(2, groups, quarter_rows, blocks_here, served_width)
    moved = lax.all_to_all(pieces, "tp", split_axis=1, concat_axis=3, tiled=True)
    placed = lax.all_to_all(moved, "fs", split_axis=3, concat_axis=2, tiled=True)
    ordered = placed.reshape(2, shards, quarter_rows, served_width)
    joined = lax.all_gather(ordered, "tp", axis=2, tiled=True)
    owned = joined.reshape(2, rows_local * shards, served_width)
    up_serving = owned[0]
    down_serving = owned[1]
    values = tokens.astype(jnp.float32)
    scale = lax.rsqrt(jnp.mean(values * values, axis=1, keepdims=True) + epsilon)
    normed = (values * scale).astype(jnp.bfloat16)
    hidden = jnp.dot(normed, up_serving, preferred_element_type=jnp.float32)
    active = jnp.square(jax.nn.relu(hidden)).astype(jnp.bfloat16)
    summed = lax.psum_scatter(
        lax.dot_general(
            down_serving, active, (((1,), (1,)), ((), ())), preferred_element_type=jnp.float32
        ),
        "fs",
        scatter_dimension=0,
        tiled=True,
    )
    prompt_output = summed.T.astype(jnp.bfloat16)
    return (up_serving, down_serving, prompt_output)


def xor2(a, k):
    if k % 2:
        a = a + 1 - 2 * (a % 2)
    if k // 2:
        a = a + 2 - 4 * (a // 2)
    return a


def kernel(
    tokens_hbm, gain_hbm, up_hbm, down_hbm, whole, prompt_out,
    raw, gain, cast, swapped, toks, normed, hidden, active, rs_send, rs_recv, rs_own,
    in_sem, misc_sem, own_sem,
    x1_send, x1_recv, z_send, z_recv,
    ax_send, ax_recv, ay_send, ay_recv, dg_send, dg_recv, d2_send, d2_recv,
    rs_ssem, rs_rsem,
):
    y = lax.axis_index("grp")
    z = lax.axis_index("fs")
    t = lax.axis_index("tp")
    x, c = t // 2, t % 2
    t_x = xor2(t, 2)
    t_c = xor2(t, 1)
    to_x = {"tp": t_x}
    to_c = {"tp": t_c}
    to_y = {"grp": 1 - y}
    quarter, width = cast.shape[2], cast.shape[3]
    rows_local = 4 * quarter
    trained = (up_hbm, down_hbm)

    def part_rows(px, py):
        return pl.multiple_of((2 * px + py) * quarter, quarter)

    fetch = {}
    for m in range(2):
        for s, px in ((0, 1 - x), (1, x)):
            fetch[m, s] = pltpu.make_async_copy(
                trained[m].at[pl.ds(part_rows(px, y), quarter)], raw.at[m, s], in_sem.at[m, s]
            )
    get_gain = pltpu.make_async_copy(gain_hbm, gain, misc_sem.at[0])
    get_toks = pltpu.make_async_copy(tokens_hbm, toks, misc_sem.at[1])
    get_gain.start()
    for m in range(2):
        for s in range(2):
            fetch[m, s].start()
    get_toks.start()

    barrier = pltpu.get_barrier_semaphore()
    for where in (to_x, to_c, to_y, {"fs": xor2(z, 1)}, {"fs": xor2(z, 2)}, {"fs": xor2(z, 3)}):
        pl.semaphore_signal(barrier, inc=1, device_id=where, device_id_type=MESH)
    pl.semaphore_wait(barrier, 6)

    def remote(src, dst, ssem, rsem, where):
        return pltpu.make_async_remote_copy(
            src_ref=src, dst_ref=dst, send_sem=ssem, recv_sem=rsem,
            device_id=where, device_id_type=MESH,
        )

    def unit(m, r, px, py):
        start = pl.multiple_of(r * rows_local + (2 * px + py) * quarter, quarter)
        return whole.at[m, pl.ds(start, quarter)]

    def hop(m, j):
        block = (t, t_x)[j]
        src = (cast.at[m, 1], swapped.at[m])[j]
        k = (z + block) % 2 + 2 * ((z // 2 + block // 2) % 2)
        return remote(
            src, unit(m, z, x, y), z_send.at[m, j], z_recv.at[m, k], {"fs": block}
        )

    def own_copy(m, j):
        src = (cast.at[m, 1], swapped.at[m])[j]
        return pltpu.make_async_copy(src, unit(m, z, x, y), own_sem.at[m])

    def start_hop(m, j):
        block = (t, t_x)[j]

        @pl.when(z != block)
        def _():
            hop(m, j).start()

        @pl.when(z == block)
        def _():
            own_copy(m, j).start()

    swap = {
        m: remote(cast.at[m, 0], swapped.at[m], x1_send.at[m], x1_recv.at[m], to_x)
        for m in range(2)
    }

    piece = 16

    def cast_part(m, s):
        px = 1 - x if s == 0 else x
        base = part_rows(px, y)
        fetch[m, s].wait()

        @pl.loop(0, quarter // piece)
        def _(i):
            here = pl.ds(pl.multiple_of(i * piece, piece), piece)
            values = raw[m, s, here, :]
            if m == 0:
                values = values * gain[pl.ds(pl.multiple_of(base + i * piece, piece), piece), :]
            cast[m, s, here, :] = values.astype(jnp.bfloat16)

    get_gain.wait()
    cast_part(0, 0)
    swap[0].start()
    cast_part(0, 1)
    start_hop(0, 0)
    cast_part(1, 0)
    swap[1].start()
    cast_part(1, 1)
    start_hop(1, 0)

    get_toks.wait()
    tokens_here = toks.shape[0]

    @pl.loop(0, tokens_here // piece)
    def _(i):
        here = pl.ds(pl.multiple_of(i * piece, piece), piece)
        values = toks[here, :].astype(jnp.float32)
        scale = lax.rsqrt(jnp.mean(values * values, axis=1, keepdims=True) + epsilon)
        normed[here, :] = (values * scale).astype(jnp.bfloat16)

    swap[0].wait_recv()
    start_hop(0, 1)

    steps = [(m, k) for m in range(2) for k in range(4)]
    diag_by_x = {(0, 2), (1, 2)}

    def copies(m, k):
        r = xor2(z, k)
        mine = unit(m, r, x, y)
        from_x = unit(m, r, 1 - x, y)
        from_y = unit(m, r, x, 1 - y)
        diag = unit(m, r, 1 - x, 1 - y)
        made = {
            "x": remote(mine, mine, ax_send.at[m, k], ax_recv.at[m, k], to_x),
            "y": remote(mine, mine, ay_send.at[m, k], ay_recv.at[m, k], to_y),
        }
        if (m, k) in diag_by_x:
            made["diag"] = remote(from_y, from_y, dg_send.at[m, k], dg_recv.at[m, k], to_x)
        else:
            made["diag"] = remote(from_x, from_x, dg_send.at[m, k], dg_recv.at[m, k], to_y)
        for p, ref in enumerate((mine, from_x, from_y, diag)):
            made[p] = remote(ref, ref, d2_send.at[m, k, p], d2_recv.at[m, k, p], to_c)
        return made

    is_active = c == z % 2
    lag_b, lag_c = 1, 2

    def stage_a(m, k):
        made = copies(m, k)
        if k == 0:
            own_copy(m, 0).wait()
        else:
            here = unit(m, xor2(z, k), x, y)
            remote(here, here, z_send.at[m, 0], z_recv.at[m, k], {"fs": xor2(z, k)}).wait_recv()
        made["x"].start()
        made["y"].start()
        made[0].start()

    def stage_b(m, k):
        made = copies(m, k)
        made["x"].wait_recv()
        if (m, k) not in diag_by_x:
            made["diag"].start()
        made[1].start()
        made["y"].wait_recv()
        if (m, k) in diag_by_x:
            made["diag"].start()
        made[2].start()

    def stage_c(m, k):
        made = copies(m, k)
        made["diag"].wait_recv()
        made[3].start()

    def listen(m, k):
        made = copies(m, k)
        for p in range(4):
            made[p].wait_recv()

    tile = 512 if width % 512 == 0 else width

    def compute_up(k):
        r = xor2(z, k)
        rows = pl.ds(pl.multiple_of(r * rows_local, rows_local), rows_local)
        left = normed[:, rows]

        @pl.loop(0, width // tile)
        def _(n):
            cols = pl.ds(pl.multiple_of(n * tile, tile), tile)
            product = jnp.dot(left, whole[0, rows, cols], preferred_element_type=jnp.float32)
            if k > 0:
                product = product + hidden[:, cols]
            if k < 3:
                hidden[:, cols] = product
            else:
                active[:, cols] = jnp.square(jnp.maximum(product, 0.0)).astype(jnp.bfloat16)

    d_tile = 256 if rows_local % 256 == 0 else rows_local

    def compute_down(k):
        r = xor2(z, k)

        @pl.loop(0, rows_local // d_tile)
        def _(n):
            cols = pl.ds(pl.multiple_of(n * d_tile, d_tile), d_tile)
            rows = pl.ds(pl.multiple_of(r * rows_local + n * d_tile, d_tile), d_tile)
            product = lax.dot_general(
                active[...], whole[1, rows, :], (((1,), (1,)), ((), ())),
                preferred_element_type=jnp.float32,
            )
            if k > 0:
                rs_send[k - 1, :, cols] = product.astype(jnp.bfloat16)
            else:
                rs_own[:, cols] = product

    def scatter(k):
        return remote(
            rs_send.at[k - 1], rs_recv.at[k - 1], rs_ssem.at[k - 1], rs_rsem.at[k - 1],
            {"fs": xor2(z, k)},
        )

    for i in range(len(steps) + lag_c):
        @pl.when(is_active)
        def _():
            if i < len(steps):
                stage_a(*steps[i])
            if 0 <= i - lag_b < len(steps):
                stage_b(*steps[i - lag_b])
            if 0 <= i - lag_c < len(steps):
                stage_c(*steps[i - lag_c])

        if i == 1:
            swap[1].wait_recv()
            start_hop(1, 1)
        if i < lag_c:
            continue
        m, k = steps[i - lag_c]

        @pl.when(jnp.logical_not(is_active))
        def _():
            listen(m, k)

        if m == 0:
            compute_up(k)
        elif k > 0:
            compute_down(k)
            scatter(k).start()

    compute_down(0)
    for k in range(1, 4):
        scatter(k).wait_recv()

    @pl.loop(0, tokens_here // piece)
    def _(i):
        here = pl.ds(pl.multiple_of(i * piece, piece), piece)
        total = rs_own[here, :]
        for k in range(3):
            total = total + rs_recv[k, here, :].astype(jnp.float32)
        prompt_out[here, :] = total.astype(prompt_out.dtype)

    for m in range(2):
        swap[m].wait_send()
        for j in range(2):
            block = (t, t_x)[j]

            @pl.when(z != block)
            def _():
                hop(m, j).wait_send()
    for k in range(1, 4):
        scatter(k).wait_send()

    @pl.when(is_active)
    def _():
        for m, k in steps:
            made = copies(m, k)
            for copy in made.values():
                copy.wait_send()


pieces_out = 8


def deliver(whole, prompt, up_out, down_out, prompt_out, sems, last):
    rows = whole.shape[1] // pieces_out
    copies = [
        pltpu.make_async_copy(
            whole.at[m, pl.ds(i * rows, rows)], out.at[pl.ds(i * rows, rows)], sems.at[m, i]
        )
        for m, out in enumerate((up_out, down_out))
        for i in range(pieces_out)
    ]
    copies.append(pltpu.make_async_copy(prompt, prompt_out, last))
    for copy in copies:
        copy.start()
    for copy in copies:
        copy.wait()


def local_kernel(tokens, norm_gain, up_trained, down_trained):
    shards = lax.axis_size("fs")
    rows_local, width = up_trained.shape
    quarter = rows_local // 4
    tokens_here, features = tokens.shape
    any_space = pl.BlockSpec(memory_space=pl.ANY)
    dma = pltpu.SemaphoreType.DMA
    bf16, f32 = jnp.bfloat16, jnp.float32
    whole, prompt = pl.pallas_call(
        kernel,
        out_shape=(
            pltpu.VMEM((2, rows_local * shards, width), bf16),
            pltpu.VMEM((tokens_here, rows_local), bf16),
        ),
        in_specs=[any_space] * 4,
        out_specs=(pl.BlockSpec(memory_space=pltpu.VMEM),) * 2,
        scratch_shapes=[
            pltpu.VMEM((2, 2, quarter, width), f32),
            pltpu.VMEM((rows_local, 1), f32),
            pltpu.VMEM((2, 2, quarter, width), bf16),
            pltpu.VMEM((2, quarter, width), bf16),
            pltpu.VMEM((tokens_here, features), bf16),
            pltpu.VMEM((tokens_here, features), bf16),
            pltpu.VMEM((tokens_here, width), f32),
            pltpu.VMEM((tokens_here, width), bf16),
            pltpu.VMEM((3, tokens_here, rows_local), bf16),
            pltpu.VMEM((3, tokens_here, rows_local), bf16),
            pltpu.VMEM((tokens_here, rows_local), f32),
            dma((2, 2)), dma((2,)), dma((2,)),
            dma((2,)), dma((2,)), dma((2, 2)), dma((2, 4)),
            dma((2, 4)), dma((2, 4)), dma((2, 4)), dma((2, 4)),
            dma((2, 4)), dma((2, 4)), dma((2, 4, 4)), dma((2, 4, 4)),
            dma((3,)), dma((3,)),
        ],
        compiler_params=pltpu.CompilerParams(
            collective_id=0, has_side_effects=True, vmem_limit_bytes=40 * 1024 * 1024
        ),
    )(tokens, norm_gain[:, None], up_trained, down_trained)
    held = pl.BlockSpec(memory_space=pltpu.VMEM)
    return tuple(pl.pallas_call(
        deliver,
        out_shape=(
            jax.ShapeDtypeStruct((rows_local * shards, width), bf16),
            jax.ShapeDtypeStruct((rows_local * shards, width), bf16),
            jax.ShapeDtypeStruct((tokens_here, rows_local), bf16),
        ),
        in_specs=[held, held],
        out_specs=(any_space,) * 3,
        scratch_shapes=[dma((2, pieces_out)), dma(())],
        compiler_params=pltpu.CompilerParams(vmem_limit_bytes=8 * 1024 * 1024),
    )(whole, prompt))


def solution(mesh):
    in_specs = (P(("grp", "tp"), None), P("fs"), P("fs", "tp"), P("fs", "tp"))
    out_specs = (P("grp", "fs"), P("grp", "fs"), P(("grp", "tp"), "fs"))
    sizes = mesh.shape
    square = sizes["grp"] == 2 and sizes["fs"] == 4 and sizes["tp"] == 4
    local = local_kernel if square else local_plain
    return jax.shard_map(local, mesh=mesh, in_specs=in_specs, out_specs=out_specs, check_vma=False)
```

```python
import jax
import jax.numpy as jnp
from jax import lax
from jax.experimental import pallas as pl
from jax.experimental.pallas import tpu as pltpu
from jax.sharding import PartitionSpec as P

epsilon = 1e-06
MESH = pl.DeviceIdType.MESH

GET, GET_RELAY, SWAP, HOP, HOP_RELAY, SEND_X, SEND_Y, SEND_CORE = range(8)
CAST_ORDER = ((0, 0), (0, 1), (1, 0), (1, 1))
CAST_BOTH = True
ORDER = (((0, 0, 0, 0, 1, 1, 1, 1), (3, 3, 3, 3, 2, 2, 3, 3), (2, 2, 1, 1, 3, 3, 2, 2), (1, 1, 2, 2, 0, 0, 0, 0)), ((1, 1, 3, 3, 3, 3, 2, 2), (3, 3, 1, 1, 2, 2, 3, 3), (2, 2, 2, 2, 0, 0, 0, 0), (0, 0, 0, 0, 1, 1, 1, 1)))
SCHEDULE = (
    (
        ((7,0,0,0,0),),
        ((5,0,0,1,0),),
        (),
        ((7,0,0,1,0),),
        (),
        (),
        ((7,0,0,0,1),),
        (),
        (),
        ((7,0,0,1,1),),
        (),
        (),
        ((7,0,0,2,0),),
        (),
        (),
        ((7,0,0,2,1),),
        ((7,0,0,3,0),(5,0,0,0,1),(7,0,0,3,1),(7,1,0,0,0),(7,1,0,0,1),(7,1,0,1,0),(7,1,0,1,1),),
        ((7,1,0,2,0),(7,1,0,2,1),(7,1,0,3,0),(7,1,0,3,1),(0,0,1,0,0),(7,0,1,0,0),(1,0,0,0,0),(4,0,0,0,0),
        (5,0,0,3,1),(5,0,0,2,0),(0,0,2,0,0),(6,0,2,0,0),(7,0,2,0,0),(0,0,3,1,0),(6,0,3,1,0),(7,0,3,1,0),
        (0,0,1,1,0),(7,0,1,1,0),(5,0,0,2,1),(1,0,0,0,1),(4,0,0,0,1),(0,0,2,0,1),(7,0,2,0,1),(0,0,1,2,0),
        (7,0,1,2,0),(0,0,3,1,1),(7,0,3,1,1),(5,0,3,1,1),(5,0,1,0,0),(0,0,2,1,0),(6,0,2,1,0),(7,0,2,1,0),
        (0,0,3,2,0),(5,0,3,2,0),(7,0,3,2,0),(0,0,1,3,0),(7,0,1,3,0),(5,0,1,1,0),(1,1,0,0,1),(4,1,0,0,1),
        (0,0,3,0,0),(7,0,3,0,0),(0,0,2,1,1),(7,0,2,1,1),(5,0,2,0,0),(0,1,1,0,0),(7,1,1,0,0),(0,0,2,2,0),
        (7,0,2,2,0),(5,0,2,1,0),(0,1,2,0,0),(6,1,2,0,0),(7,1,2,0,0),(5,0,1,2,0),(0,1,1,1,0),(7,1,1,1,0),
        (0,0,1,0,1),(7,0,1,0,1),(5,0,1,3,0),(1,1,0,0,0),(4,1,0,0,0),(0,1,2,0,1),(7,1,2,0,1),(0,0,3,3,0),
        (6,0,3,3,0),(7,0,3,3,0),(0,0,1,2,1),(7,0,1,2,1),(5,1,1,0,0),(0,0,3,0,1),(7,0,3,0,1),(0,0,3,2,1),
        (7,0,3,2,1),(5,1,1,1,0),(0,0,3,3,1),(7,0,3,3,1),),
        ((0,0,2,3,1),(6,0,2,3,1),(7,0,2,3,1),(0,1,2,1,0),(7,1,2,1,0),(6,1,2,1,0),(5,1,2,0,0),(0,0,1,3,1),
        (7,0,1,3,1),(0,0,2,2,1),(7,0,2,2,1),(5,1,2,1,0),(0,0,2,3,0),(7,0,2,3,0),),
        ((0,1,1,2,0),(7,1,1,2,0),(0,1,3,1,0),(6,1,3,1,0),(7,1,3,1,0),(0,0,1,1,1),(7,0,1,1,1),),
        ((5,1,1,2,0),(0,1,2,1,1),(7,1,2,1,1),(0,1,3,3,0),(6,1,3,3,0),(7,1,3,3,0),(0,1,1,3,0),(7,1,1,3,0),
        (0,1,3,1,1),(7,1,3,1,1),(5,1,3,1,1),(0,1,3,3,1),(7,1,3,3,1),(0,1,1,2,1),(7,1,1,2,1),(0,1,3,2,0),
        (5,1,3,2,0),(7,1,3,2,0),(0,1,1,0,1),(7,1,1,0,1),(5,1,1,3,0),(0,1,1,3,1),(7,1,1,3,1),(0,1,1,1,1),
        (7,1,1,1,1),),
        ((5,1,0,0,1),(0,1,3,0,0),(7,1,3,0,0),(5,1,0,1,0),(5,1,0,3,1),(0,1,3,0,1),(7,1,3,0,1),(5,1,0,2,0),
        (0,1,2,2,0),(7,1,2,2,0),(5,1,0,2,1),(0,1,3,2,1),(7,1,3,2,1),),
        ((0,1,2,3,1),(6,1,2,3,1),(7,1,2,3,1),(0,1,2,2,1),(7,1,2,2,1),(0,1,2,3,0),(7,1,2,3,0),),
        (),
        (),
    ),
    (
        ((3,0,0,0,0),),
        ((2,0,0,1,0),),
        ((3,0,0,2,0),),
        (),
        (),
        (),
        (),
        (),
        (),
        (),
        (),
        (),
        (),
        (),
        (),
        (),
        ((3,0,0,3,0),(2,1,0,1,0),),
        ((1,0,0,0,0),(4,0,0,0,0),(1,0,0,3,0),(4,0,0,3,0),(1,1,0,3,0),(4,1,0,3,0),(3,1,0,0,0),),
        ((1,1,0,0,0),(4,1,0,0,0),),
        (),
        ((3,1,0,2,0),(3,0,0,3,1),(3,1,0,3,0),(3,1,0,3,1),),
        (),
        (),
        (),
        (),
    ),
    (
        ((2,0,0,0,0),),
        ((3,0,0,1,0),),
        (),
        (),
        (),
        (),
        (),
        (),
        (),
        (),
        (),
        (),
        (),
        (),
        (),
        (),
        ((2,0,0,0,1),(0,0,0,1,0),(6,0,0,1,0),(7,0,0,1,0),(2,1,0,0,1),(3,0,0,2,0),(0,0,0,1,1),(7,0,0,1,1),
        (0,0,0,0,1),(6,0,0,0,1),(7,0,0,0,1),(2,1,0,0,0),(0,0,0,3,1),(6,0,0,3,1),(7,0,0,3,1),(0,0,0,0,0),
        (7,0,0,0,0),(0,0,0,2,0),(7,0,0,2,0),(0,0,2,2,0),(7,0,2,2,0),(0,0,0,3,0),(7,0,0,3,0),(3,0,0,3,0),
        (0,0,0,2,1),(7,0,0,2,1),),
        ((0,0,3,0,0),(6,0,3,0,0),(7,0,3,0,0),(5,0,3,0,0),(5,0,2,2,0),(0,0,3,1,1),(7,0,3,1,1),(6,0,3,1,1),
        (0,0,3,0,1),(7,0,3,0,1),(0,0,1,0,0),(7,0,1,0,0),(6,0,1,0,0),(0,0,3,1,0),(7,0,3,1,0),(3,1,0,1,0),
        (0,0,3,2,0),(7,0,3,2,0),(6,0,3,2,0),(0,0,2,3,0),(7,0,2,3,0),(6,0,2,3,0),(0,0,1,0,1),(5,0,1,0,1),
        (7,0,1,0,1),(0,0,1,1,0),(7,0,1,1,0),(0,0,3,3,0),(7,0,3,3,0),(5,0,3,3,0),(6,0,3,3,0),(0,0,3,2,1),
        (7,0,3,2,1),(5,0,3,2,1),(0,0,2,0,0),(7,0,2,0,0),(6,0,1,1,0),(0,0,2,3,1),(7,0,2,3,1),(5,0,2,3,1),
        (0,0,2,1,0),(7,0,2,1,0),(0,0,3,3,1),(7,0,3,3,1),),
        ((3,1,0,2,0),(0,0,1,2,0),(7,0,1,2,0),(6,0,1,2,0),(0,0,2,2,1),(7,0,2,2,1),(5,0,2,2,1),(0,0,1,1,1),
        (7,0,1,1,1),(5,0,1,1,1),(0,0,1,3,0),(7,0,1,3,0),(6,0,1,3,0),(0,1,3,3,0),(7,1,3,3,0),(6,1,3,3,0),
        (5,1,3,3,0),(0,0,1,2,1),(7,0,1,2,1),(0,1,1,0,0),(7,1,1,0,0),(6,1,1,0,0),(0,0,1,3,1),(7,0,1,3,1),),
        ((3,0,0,3,1),(0,1,1,1,0),(7,1,1,1,0),(6,1,1,1,0),(0,1,3,3,1),(7,1,3,3,1),(0,0,2,0,1),(7,0,2,0,1),
        (0,1,2,0,0),(7,1,2,0,0),(0,1,1,0,1),(5,1,1,0,1),(7,1,1,0,1),(0,1,2,1,0),(7,1,2,1,0),(3,1,0,3,0),
        (0,1,1,1,1),(5,1,1,1,1),(7,1,1,1,1),(0,1,3,0,0),(6,1,3,0,0),(7,1,3,0,0),(5,1,3,0,0),(0,1,1,2,0),
        (6,1,1,2,0),(7,1,1,2,0),(0,0,2,1,1),(7,0,2,1,1),),
        ((0,1,3,1,1),(7,1,3,1,1),(6,1,3,1,1),(0,1,3,0,1),(7,1,3,0,1),(3,1,0,3,1),(0,1,3,2,0),(7,1,3,2,0),
        (6,1,3,2,0),(0,1,1,2,1),(7,1,1,2,1),(0,1,2,3,0),(7,1,2,3,0),(6,1,2,3,0),(0,1,1,3,0),(7,1,1,3,0),
        (0,1,3,1,0),(7,1,3,1,0),(0,1,2,2,0),(5,1,2,2,0),(7,1,2,2,0),(6,1,1,3,0),(0,1,0,0,1),(7,1,0,0,1),
        (0,1,3,2,1),(7,1,3,2,1),(5,1,3,2,1),),
        ((0,1,2,2,1),(7,1,2,2,1),(6,1,0,0,1),(0,1,0,1,0),(7,1,0,1,0),(5,1,2,2,1),(0,1,2,3,1),(7,1,2,3,1),
        (5,1,2,3,1),(0,1,2,0,1),(7,1,2,0,1),(6,1,0,1,0),(0,1,0,3,1),(7,1,0,3,1),(0,1,1,3,1),(7,1,1,3,1),),
        ((0,1,2,1,1),(7,1,2,1,1),(6,1,0,3,1),),
        ((0,1,0,2,0),(7,1,0,2,0),(0,1,0,0,0),(7,1,0,0,0),(0,1,0,2,1),(7,1,0,2,1),(0,1,0,1,1),(7,1,0,1,1),
        (0,1,0,3,0),(7,1,0,3,0),),
        (),
    ),
    (
        ((2,0,0,0,0),),
        ((3,0,0,1,0),),
        (),
        (),
        (),
        (),
        (),
        (),
        (),
        (),
        (),
        (),
        (),
        (),
        (),
        (),
        ((2,0,0,3,0),(2,1,0,3,0),(3,0,0,2,0),(2,1,0,0,0),(1,0,0,1,0),(4,0,0,1,0),),
        ((3,0,0,0,1),(3,1,0,1,0),),
        ((3,1,0,2,0),),
        ((1,1,0,1,0),(4,1,0,1,0),(3,1,0,0,1),),
        (),
        (),
        (),
        (),
        (),
    ),
    (
        ((3,0,1,0,0),),
        (),
        (),
        (),
        (),
        (),
        (),
        (),
        (),
        (),
        (),
        (),
        (),
        (),
        (),
        (),
        ((3,0,1,1,0),),
        ((1,0,1,2,0),(4,0,1,2,0),(3,0,1,2,0),(3,0,1,3,0),(1,0,1,1,1),(4,0,1,1,1),(3,1,1,0,0),(3,1,1,1,0),
        (1,0,1,3,0),(4,0,1,3,0),(3,0,1,2,1),(3,0,1,3,1),(1,1,1,2,0),(4,1,1,2,0),(3,1,1,2,0),(3,1,1,3,0),
        (1,1,1,1,1),(4,1,1,1,1),(3,1,1,2,1),),
        ((3,1,1,3,1),(1,1,1,3,0),(4,1,1,3,0),),
        (),
        (),
        (),
        (),
        (),
        (),
    ),
    (
        ((7,0,1,0,0),),
        ((5,0,1,1,0),),
        (),
        ((7,0,1,1,0),),
        ((5,0,1,0,1),),
        (),
        ((7,0,1,0,1),),
        (),
        (),
        ((7,0,1,1,1),),
        (),
        (),
        ((7,0,1,2,0),),
        (),
        (),
        ((7,0,1,2,1),),
        ((7,0,1,3,0),(5,0,1,2,1),(7,0,1,3,1),(7,1,1,0,0),(7,1,1,0,1),(0,0,0,0,0),(7,0,0,0,0),(7,1,1,1,0),),
        ((7,1,1,1,1),(7,1,1,2,0),(5,0,1,3,1),(7,1,1,2,1),(7,1,1,3,0),(7,1,1,3,1),(0,0,0,2,0),(6,0,0,2,0),
        (7,0,0,2,0),(1,0,1,2,0),(4,0,1,2,0),(5,0,0,0,0),(0,0,0,3,0),(7,0,0,3,0),(0,0,0,2,1),(7,0,0,2,1),
        (0,0,2,0,0),(6,0,2,0,0),(7,0,2,0,0),(5,0,2,0,0),(0,0,3,1,0),(6,0,3,1,0),(7,0,3,1,0),(1,0,1,3,0),
        (4,0,1,3,0),(0,0,2,0,1),(7,0,2,0,1),(5,0,2,0,1),(0,0,3,1,1),(7,0,3,1,1),(5,0,3,1,1),(5,0,0,2,1),
        (5,0,0,3,0),(0,0,2,3,1),(6,0,2,3,1),(7,0,2,3,1),(0,0,3,2,0),(6,0,3,2,0),(7,0,3,2,0),(5,1,1,0,1),
        (1,0,1,2,1),(4,0,1,2,1),(0,0,2,3,0),(7,0,2,3,0),(0,0,3,2,1),(7,0,3,2,1),(5,0,3,2,1),(0,0,2,1,0),
        (7,0,2,1,0),(5,1,1,1,0),(0,0,3,3,0),(5,0,3,3,0),(7,0,3,3,0),(5,1,1,2,1),(1,0,1,0,1),(4,0,1,0,1),
        (0,0,3,0,1),(6,0,3,0,1),(7,0,3,0,1),(5,1,1,3,1),(0,0,0,1,0),(6,0,0,1,0),(7,0,0,1,0),(0,0,3,0,0),
        (7,0,3,0,0),(0,0,2,2,1),(6,0,2,2,1),(7,0,2,2,1),(0,1,2,0,0),(7,1,2,0,0),(0,1,3,1,0),(6,1,3,1,0),
        (5,1,2,0,0),(0,0,0,1,1),(5,0,0,1,1),(7,0,0,1,1),(7,1,3,1,0),(6,1,2,0,0),(0,0,2,1,1),(7,0,2,1,1),
        (1,0,1,1,1),(4,0,1,1,1),(0,0,2,2,0),(7,0,2,2,0),),
        ((0,1,0,0,0),(7,1,0,0,0),(5,1,0,0,0),(0,1,3,1,1),(7,1,3,1,1),(5,1,3,1,1),(0,1,2,3,1),(6,1,2,3,1),
        (7,1,2,3,1),(0,1,3,2,0),(6,1,3,2,0),(0,1,2,0,1),(5,1,2,0,1),(7,1,3,2,0),(7,1,2,0,1),(1,1,1,3,0),
        (4,1,1,3,0),(0,1,2,3,0),(7,1,2,3,0),(0,0,0,0,1),(7,0,0,0,1),(0,1,3,2,1),(5,1,3,2,1),(7,1,3,2,1),
        (1,1,1,2,0),(4,1,1,2,0),(0,1,0,2,0),(6,1,0,2,0),(0,0,3,3,1),(7,0,3,3,1),),
        ((0,1,3,0,1),(6,1,3,0,1),(7,1,3,0,1),(0,1,2,1,0),(7,1,2,1,0),(7,1,0,2,0),(1,1,1,2,1),(4,1,1,2,1),
        (0,0,0,3,1),(7,0,0,3,1),),
        ((0,1,0,2,1),(5,1,0,2,1),(7,1,0,2,1),(1,1,1,0,1),(4,1,1,0,1),(0,1,0,3,0),(7,1,0,3,0),(0,1,3,3,0),
        (5,1,3,3,0),(0,1,2,2,1),(6,1,2,2,1),(7,1,3,3,0),(7,1,2,2,1),(5,1,0,3,0),(0,1,3,0,0),(7,1,3,0,0),
        (1,1,1,1,1),(4,1,1,1,1),(0,1,0,3,1),(7,1,0,3,1),(0,1,0,1,0),(6,1,0,1,0),(7,1,0,1,0),(0,1,3,3,1),
        (7,1,3,3,1),),
        ((0,1,2,2,0),(7,1,2,2,0),(0,1,2,1,1),(7,1,2,1,1),),
        ((0,1,0,1,1),(5,1,0,1,1),(7,1,0,1,1),(0,1,0,0,1),(7,1,0,0,1),),
        (),
        (),
    ),
    (
        ((3,0,1,0,0),),
        (),
        ((2,0,1,2,0),),
        (),
        (),
        (),
        (),
        (),
        (),
        (),
        (),
        (),
        (),
        (),
        (),
        (),
        ((2,0,1,1,1),(3,0,1,3,1),(2,0,1,3,0),(2,1,1,2,0),),
        ((3,0,1,1,0),(2,1,1,1,1),(2,1,1,3,0),(3,1,1,0,0),(3,1,1,3,1),),
        ((3,1,1,1,0),),
        (),
        (),
        (),
        (),
        (),
        (),
    ),
    (
        ((3,0,1,0,0),),
        (),
        ((2,0,1,2,0),),
        (),
        (),
        (),
        (),
        (),
        (),
        (),
        (),
        (),
        (),
        (),
        (),
        (),
        ((2,0,1,3,0),(0,0,1,1,0),(6,0,1,1,0),(7,0,1,1,0),(0,0,1,0,1),(6,0,1,0,1),(7,0,1,0,1),(3,0,1,1,0),
        (0,0,1,1,1),(7,0,1,1,1),(2,0,1,2,1),(0,0,1,2,1),(6,0,1,2,1),(7,0,1,2,1),(0,0,1,0,0),(7,0,1,0,0),
        (0,0,1,3,1),(6,0,1,3,1),(7,0,1,3,1),(0,0,1,2,0),(7,0,1,2,0),(2,0,1,0,1),(0,0,0,0,0),(6,0,0,0,0),
        (7,0,0,0,0),(0,0,1,3,0),(7,0,1,3,0),),
        ((0,0,2,0,0),(7,0,2,0,0),(0,0,3,0,0),(7,0,3,0,0),(0,0,2,2,0),(6,0,2,2,0),(7,0,2,2,0),(3,1,1,0,0),
        (0,0,0,0,1),(7,0,0,0,1),(2,0,1,1,1),(0,0,2,0,1),(7,0,2,0,1),(0,0,2,2,1),(7,0,2,2,1),(0,0,3,1,1),
        (6,0,3,1,1),(7,0,3,1,1),(2,1,1,3,0),(0,0,0,2,1),(6,0,0,2,1),(7,0,0,2,1),(0,0,3,1,0),(7,0,3,1,0),
        (0,0,0,1,0),(7,0,0,1,0),(3,1,1,1,0),(0,0,0,3,0),(6,0,0,3,0),(7,0,0,3,0),(0,0,3,0,1),(7,0,3,0,1),
        (0,0,2,1,1),(6,0,2,1,1),(7,0,2,1,1),(0,0,0,2,0),(7,0,0,2,0),(5,0,3,0,1),(0,1,1,0,1),(7,1,1,0,1),
        (0,0,0,3,1),(7,0,0,3,1),(5,0,0,1,0),(0,0,3,2,1),(6,0,3,2,1),(7,0,3,2,1),(0,0,2,1,0),(7,0,2,1,0),
        (5,0,2,2,1),(6,1,1,0,1),(0,0,3,3,0),(6,0,3,3,0),(7,0,3,3,0),(0,0,3,2,0),(7,0,3,2,0),(5,0,2,1,1),
        (0,1,1,1,0),(7,1,1,1,0),(0,1,3,0,1),(7,1,3,0,1),(0,0,2,3,0),(6,0,2,3,0),(7,0,2,3,0),(0,0,3,3,1),
        (7,0,3,3,1),),
        ((2,1,1,2,0),(6,1,1,1,0),(0,1,1,2,1),(7,1,1,2,1),(0,1,1,0,0),(7,1,1,0,0),(2,1,1,2,1),(6,1,1,2,1),
        (0,1,1,3,1),(7,1,1,3,1),(0,0,2,3,1),(7,0,2,3,1),),
        ((2,1,1,0,1),(0,0,0,1,1),(7,0,0,1,1),),
        ((0,1,1,1,1),(7,1,1,1,1),(5,0,0,0,1),(0,1,3,0,0),(7,1,3,0,0),(0,1,2,2,0),(6,1,2,2,0),(7,1,2,2,0),
        (0,1,2,0,0),(7,1,2,0,0),(0,1,1,2,0),(7,1,1,2,0),(5,1,3,0,1),(0,1,3,1,1),(6,1,3,1,1),(7,1,3,1,1),
        (0,1,2,2,1),(7,1,2,2,1),(2,1,1,1,1),(0,1,0,0,0),(6,1,0,0,0),(7,1,0,0,0),(0,1,3,1,0),(7,1,3,1,0),
        (0,1,2,1,1),(6,1,2,1,1),(5,1,2,2,1),(7,1,2,1,1),(6,1,1,3,1),(0,1,2,0,1),(7,1,2,0,1),(0,1,0,0,1),
        (7,1,0,0,1),(0,1,0,1,0),(7,1,0,1,0),(5,1,0,1,0),(0,1,3,2,1),(7,1,3,2,1),(6,1,3,2,1),(0,1,2,1,0),
        (7,1,2,1,0),(5,1,2,1,1),(0,1,2,3,0),(7,1,2,3,0),(6,1,2,3,0),(0,1,1,3,0),(7,1,1,3,0),(5,1,0,0,1),
        (0,1,0,2,1),(7,1,0,2,1),(0,1,3,2,0),(7,1,3,2,0),(0,1,3,3,0),(7,1,3,3,0),(6,1,3,3,0),(6,1,0,2,1),
        (0,1,2,3,1),(7,1,2,3,1),),
        ((0,1,0,3,0),(7,1,0,3,0),(6,1,0,3,0),(0,1,3,3,1),(7,1,3,3,1),),
        ((0,1,0,1,1),(7,1,0,1,1),(0,1,0,2,0),(7,1,0,2,0),(0,1,0,3,1),(7,1,0,3,1),),
        (),
        (),
    ),
)


def local_plain(tokens, norm_gain, up_trained, down_trained):
    shards = lax.axis_size("fs")
    groups = lax.axis_size("tp")
    rows_local = up_trained.shape[0]
    cols_local = up_trained.shape[1]
    folded = (norm_gain[:, None] * up_trained).astype(jnp.bfloat16)
    stacked = jnp.stack([folded, down_trained.astype(jnp.bfloat16)])
    served_width = cols_local * groups // shards
    blocks_here = cols_local // served_width
    quarter_rows = rows_local // groups
    pieces = stacked.reshape(2, groups, quarter_rows, blocks_here, served_width)
    moved = lax.all_to_all(pieces, "tp", split_axis=1, concat_axis=3, tiled=True)
    placed = lax.all_to_all(moved, "fs", split_axis=3, concat_axis=2, tiled=True)
    ordered = placed.reshape(2, shards, quarter_rows, served_width)
    joined = lax.all_gather(ordered, "tp", axis=2, tiled=True)
    owned = joined.reshape(2, rows_local * shards, served_width)
    up_serving = owned[0]
    down_serving = owned[1]
    values = tokens.astype(jnp.float32)
    scale = lax.rsqrt(jnp.mean(values * values, axis=1, keepdims=True) + epsilon)
    normed = (values * scale).astype(jnp.bfloat16)
    hidden = jnp.dot(normed, up_serving, preferred_element_type=jnp.float32)
    active = jnp.square(jax.nn.relu(hidden)).astype(jnp.bfloat16)
    summed = lax.psum_scatter(
        lax.dot_general(
            down_serving, active, (((1,), (1,)), ((), ())), preferred_element_type=jnp.float32
        ),
        "fs",
        scatter_dimension=0,
        tiled=True,
    )
    prompt_output = summed.T.astype(jnp.bfloat16)
    return (up_serving, down_serving, prompt_output)


def kernel(
    tokens_hbm, gain_hbm, up_hbm, down_hbm, whole, prompt_out,
    raw, gain_rows, gain, cast, relay, toks, normed, hidden, active, rs_send, rs_recv, rs_own,
    in_sem, misc_sem, got_sem, relay_sem, block_sem, src_sem, out_sem, rs_ssem, rs_rsem,
):
    y = lax.axis_index("grp")
    z = lax.axis_index("fs")
    t = lax.axis_index("tp")
    mirrored = z // 2
    role = jnp.where(mirrored == 1, 4 * (3 - z) + (3 - t), 4 * z + t)
    is_own = z == t
    is_active = t % 2 == z % 2
    t_x = jnp.where(t < 2, t + 2, t - 2)
    t_c = t + 1 - 2 * (t % 2)
    to_x = {"tp": t_x}
    to_c = {"tp": t_c}
    to_y = {"grp": 1 - y}
    rows_local, width = cast.shape[1], cast.shape[2]
    size = rows_local // 8
    trained = (up_hbm, down_hbm)
    planes = [jnp.where(mirrored == 1, 3 - k, k) for k in range(4)]
    sides = [y, 1 - y]

    def part(pair, side):
        return 2 * pair + sides[side]

    def ds(start, extent):
        return pl.ds(pl.multiple_of(start, extent), extent)

    def local_rows(pair, side):
        return ds(part(pair, side) * size, size)

    def unit(m, plane, pair, side):
        return whole.at[m, ds(plane * rows_local + part(pair, side) * size, size)]

    def remote(src, dst, ssem, rsem, where):
        return pltpu.make_async_remote_copy(
            src_ref=src, dst_ref=dst, send_sem=ssem, recv_sem=rsem,
            device_id=where, device_id_type=MESH,
        )

    def fetch(m, pair, side):
        rows = local_rows(pair, side)
        return pltpu.make_async_copy(
            trained[m].at[rows], raw.at[m, rows], in_sem.at[m, 2 * pair + side]
        )

    get_gain = pltpu.make_async_copy(gain_hbm, gain_rows, misc_sem.at[0])
    get_toks = pltpu.make_async_copy(tokens_hbm, toks, misc_sem.at[1])
    get_gain.start()
    for m, side in CAST_ORDER:
        def start_fetches():
            for pair in range(4):
                fetch(m, pair, side).start()
        if side == 0 or CAST_BOTH:
            start_fetches()
        else:
            pl.when(is_own)(start_fetches)
    get_toks.start()

    barrier = pltpu.get_barrier_semaphore()
    others = [{"fs": lax.rem(z + k, 4)} for k in range(1, 4)]
    for where in [to_x, to_c, to_y] + others:
        pl.semaphore_signal(barrier, inc=1, device_id=where, device_id_type=MESH)

    get_gain.wait()
    lanes = gain_rows.shape[1]
    for q in range(gain_rows.shape[0]):
        square = (lanes, lanes)
        chosen = jnp.where(
            lax.broadcasted_iota(jnp.int32, square, 0) == lax.broadcasted_iota(jnp.int32, square, 1),
            jnp.broadcast_to(gain_rows[pl.ds(q, 1), :], square), 0.0,
        )
        gain[pl.ds(q * lanes, lanes), :] = jnp.sum(chosen, axis=1, keepdims=True)

    piece = 16

    def cast_unit(m, pair, side):
        fetch(m, pair, side).wait()
        base = part(pair, side) * size

        def store(into, shift):
            @pl.loop(0, size // piece)
            def _(i):
                here = ds(base + i * piece, piece)
                values = raw[m, here, :]
                if m == 0:
                    values = values * gain[here, :]
                into[m, ds(shift + base + i * piece, piece), :] = values.astype(jnp.bfloat16)

        @pl.when(is_own)
        def _():
            store(whole, z * rows_local)

        if side == 0 or CAST_BOTH:
            @pl.when(jnp.logical_not(is_own))
            def _():
                store(cast, 0)

    def step(kind, m, k, pair, side):
        plane = planes[k]
        place = part(pair, side)
        if kind == GET:
            here = unit(m, plane, pair, side)
            remote(here, here, out_sem.at[0, m], got_sem.at[m, plane, place], to_x).wait_recv()
        elif kind == GET_RELAY:
            here = relay.at[m, ds(place * size, size)]
            remote(here, here, src_sem.at[m], relay_sem.at[m, place], to_x).wait_recv()
        elif kind == SWAP:
            remote(
                cast.at[m, local_rows(pair, side)], relay.at[m, ds(place * size, size)],
                src_sem.at[m], relay_sem.at[m, place], to_x,
            ).start()
        elif kind in (HOP, HOP_RELAY):
            src = (cast if kind == HOP else relay).at[m, ds(place * size, size)]
            remote(
                src, unit(m, z, pair, side), src_sem.at[m], got_sem.at[m, z, place],
                {"fs": t if kind == HOP else t_x},
            ).start()
        elif kind == SEND_CORE:
            here = unit(m, plane, pair, side)
            remote(here, here, out_sem.at[2, m], block_sem.at[m, plane], to_c).start()
        else:
            here = unit(m, plane, pair, side)
            i = kind - SEND_X
            remote(
                here, here, out_sem.at[i, m], got_sem.at[m, plane, place], (to_x, to_y)[i]
            ).start()

    def run(segment):
        for r in range(8):
            if SCHEDULE[r][segment]:
                @pl.when(role == r)
                def _():
                    for s in SCHEDULE[r][segment]:
                        step(*s)

    casts = [(m, pair, side) for m, side in CAST_ORDER for pair in range(4)]
    first = True
    segment = 0
    for m, pair, side in casts:
        if side == 1 and not CAST_BOTH:
            pl.when(is_own)(lambda: cast_unit(m, pair, side))
        else:
            cast_unit(m, pair, side)
        if first:
            pl.semaphore_wait(barrier, 6)
            first = False
        run(segment)
        segment += 1

    get_toks.wait()
    tokens_here = toks.shape[0]

    @pl.loop(0, tokens_here // piece)
    def _(i):
        here = ds(i * piece, piece)
        values = toks[here, :].astype(jnp.float32)
        scale = lax.rsqrt(jnp.mean(values * values, axis=1, keepdims=True) + epsilon)
        normed[here, :] = (values * scale).astype(jnp.bfloat16)

    def pick(table):
        chosen = planes[table[0]]
        for r in range(1, 8):
            if table[r] != table[0]:
                chosen = jnp.where(role == r, planes[table[r]], chosen)
        return chosen

    def listen(m, plane):
        @pl.when(jnp.logical_not(is_active))
        def _():
            here = whole.at[m, ds(plane * rows_local, rows_local)]
            remote(here, here, out_sem.at[2, m], block_sem.at[m, plane], to_c).wait_recv()

    tile = 512 if width % 512 == 0 else width

    def compute_up(k):
        plane = pick(ORDER[0][k])
        listen(0, plane)
        rows = ds(plane * rows_local, rows_local)

        @pl.loop(0, width // tile)
        def _(n):
            cols = ds(n * tile, tile)
            product = jnp.dot(
                normed[:, rows], whole[0, rows, cols], preferred_element_type=jnp.float32
            )
            if k > 0:
                product = product + hidden[:, cols]
            if k < 3:
                hidden[:, cols] = product
            else:
                active[:, cols] = jnp.square(jnp.maximum(product, 0.0)).astype(jnp.bfloat16)

    d_tile = 256 if rows_local % 256 == 0 else rows_local

    def scatter(k, plane):
        slot = lax.rem(z - plane + 3, 4)
        return remote(
            rs_send.at[k], rs_recv.at[slot], rs_ssem.at[k], rs_rsem.at[slot], {"fs": plane}
        )

    def compute_down(k):
        plane = pick(ORDER[1][k])
        listen(1, plane)

        @pl.loop(0, rows_local // d_tile)
        def _(n):
            cols = ds(n * d_tile, d_tile)
            product = lax.dot_general(
                active[...], whole[1, ds(plane * rows_local + n * d_tile, d_tile), :],
                (((1,), (1,)), ((), ())), preferred_element_type=jnp.float32,
            )
            if k < 3:
                rs_send[k, :, cols] = product.astype(jnp.bfloat16)
            else:
                rs_own[:, cols] = product
        if k < 3:
            scatter(k, plane).start()

    for m in range(2):
        for k in range(4):
            run(segment)
            segment += 1
            (compute_up, compute_down)[m](k)
    run(segment)

    for k in range(3):
        here = rs_recv.at[k]
        remote(here, here, rs_ssem.at[k], rs_rsem.at[k], {"fs": lax.rem(z + 1, 4)}).wait_recv()

    @pl.loop(0, tokens_here // piece)
    def _(i):
        here = ds(i * piece, piece)
        total = rs_own[here, :]
        for k in range(3):
            total = total + rs_recv[k, here, :].astype(jnp.float32)
        prompt_out[here, :] = total.astype(prompt_out.dtype)

    def drain(sem, m, count):
        sent = whole.at[m, pl.ds(0, count * size)]
        remote(sent, sent, sem, got_sem.at[0, 0, 0], to_x).wait_send()

    for r in range(8):
        @pl.when(role == r)
        def _():
            for m in range(2):
                steps = [s for part_of in SCHEDULE[r] for s in part_of if s[1] == m]
                hops = sum(s[0] in (SWAP, HOP, HOP_RELAY) for s in steps)
                if hops:
                    drain(src_sem.at[m], m, hops)
                for i, kind in enumerate((SEND_X, SEND_Y, SEND_CORE)):
                    sends = sum(s[0] == kind for s in steps)
                    if sends:
                        drain(out_sem.at[i, m], m, sends)
    for k in range(3):
        here = rs_send.at[k]
        remote(here, here, rs_ssem.at[k], rs_rsem.at[k], {"fs": lax.rem(z + 1, 4)}).wait_send()


pieces_out = 8


def deliver(whole, prompt, up_out, down_out, prompt_out, sems, last):
    rows = whole.shape[1] // pieces_out
    copies = [
        pltpu.make_async_copy(
            whole.at[m, pl.ds(i * rows, rows)], out.at[pl.ds(i * rows, rows)], sems.at[m, i]
        )
        for m, out in enumerate((up_out, down_out))
        for i in range(pieces_out)
    ]
    copies.append(pltpu.make_async_copy(prompt, prompt_out, last))
    for copy in copies:
        copy.start()
    for copy in copies:
        copy.wait()


def local_kernel(tokens, norm_gain, up_trained, down_trained):
    shards = lax.axis_size("fs")
    rows_local, width = up_trained.shape
    tokens_here, features = tokens.shape
    any_space = pl.BlockSpec(memory_space=pl.ANY)
    dma = pltpu.SemaphoreType.DMA
    bf16, f32 = jnp.bfloat16, jnp.float32
    whole, prompt = pl.pallas_call(
        kernel,
        out_shape=(
            pltpu.VMEM((2, rows_local * shards, width), bf16),
            pltpu.VMEM((tokens_here, rows_local), bf16),
        ),
        in_specs=[any_space] * 4,
        out_specs=(pl.BlockSpec(memory_space=pltpu.VMEM),) * 2,
        scratch_shapes=[
            pltpu.VMEM((2, rows_local, width), f32),
            pltpu.VMEM((rows_local // 128, 128), f32),
            pltpu.VMEM((rows_local, 1), f32),
            pltpu.VMEM((2, rows_local, width), bf16),
            pltpu.VMEM((2, rows_local, width), bf16),
            pltpu.VMEM((tokens_here, features), bf16),
            pltpu.VMEM((tokens_here, features), bf16),
            pltpu.VMEM((tokens_here, width), f32),
            pltpu.VMEM((tokens_here, width), bf16),
            pltpu.VMEM((3, tokens_here, rows_local), bf16),
            pltpu.VMEM((3, tokens_here, rows_local), bf16),
            pltpu.VMEM((tokens_here, rows_local), f32),
            dma((2, 8)), dma((2,)),
            dma((2, 4, 8)), dma((2, 8)), dma((2, 4)),
            dma((2,)), dma((3, 2)), dma((3,)), dma((3,)),
        ],
        compiler_params=pltpu.CompilerParams(
            collective_id=0, has_side_effects=True, vmem_limit_bytes=40 * 1024 * 1024
        ),
    )(tokens, norm_gain.reshape(rows_local // 128, 128), up_trained, down_trained)
    held = pl.BlockSpec(memory_space=pltpu.VMEM)
    return tuple(pl.pallas_call(
        deliver,
        out_shape=(
            jax.ShapeDtypeStruct((rows_local * shards, width), bf16),
            jax.ShapeDtypeStruct((rows_local * shards, width), bf16),
            jax.ShapeDtypeStruct((tokens_here, rows_local), bf16),
        ),
        in_specs=[held, held],
        out_specs=(any_space,) * 3,
        scratch_shapes=[dma((2, pieces_out)), dma(())],
        compiler_params=pltpu.CompilerParams(vmem_limit_bytes=8 * 1024 * 1024),
    )(whole, prompt))


def solution(mesh):
    in_specs = (P(("grp", "tp"), None), P("fs"), P("fs", "tp"), P("fs", "tp"))
    out_specs = (P("grp", "fs"), P("grp", "fs"), P(("grp", "tp"), "fs"))
    sizes = mesh.shape
    square = sizes["grp"] == 2 and sizes["fs"] == 4 and sizes["tp"] == 4
    local = local_kernel if square else local_plain
    return jax.shard_map(local, mesh=mesh, in_specs=in_specs, out_specs=out_specs, check_vma=False)
```

```python
import jax
import jax.numpy as jnp
from jax import lax
from jax.experimental import pallas as pl
from jax.experimental.pallas import tpu as pltpu
from jax.sharding import PartitionSpec as P

epsilon = 1e-06
MESH = pl.DeviceIdType.MESH

GET, GET_RELAY, SWAP, HOP, HOP_RELAY, SEND_X, SEND_Y, SEND_CORE = range(8)
PAIRS = 4
ORDER = (
    (
        (0, 0, 1, 1, 1, 1, 1, 1),
        (1, 1, 0, 0, 3, 3, 0, 0),
        (2, 2, 3, 3, 0, 0, 3, 3),
        (3, 3, 2, 2, 2, 2, 2, 2),
    ),
    (
        (3, 3, 3, 3, 0, 0, 0, 0),
        (2, 2, 2, 2, 3, 3, 3, 3),
        (1, 1, 1, 1, 2, 2, 2, 2),
        (0, 0, 0, 0, 1, 1, 1, 1),
    ),
)
SCHEDULE = (
    (
        ((5, 0, 0, 0, 0), (7, 0, 0, 0, 0),),
        (),
        (),
        (),
        (),
        ((7, 0, 0, 0, 1),),
        (),
        (),
        (),
        (),
        ((7, 0, 0, 1, 0),),
        (),
        (),
        (),
        (),
        ((5, 0, 0, 1, 1), (7, 0, 0, 1, 1),),
        ((7, 0, 0, 2, 0), (7, 0, 0, 2, 1), (7, 0, 0, 3, 0), (7, 0, 0, 3, 1), (7, 1, 0, 0, 0),),
        ((7, 1, 0, 0, 1), (7, 1, 0, 1, 0), (7, 1, 0, 1, 1), (7, 1, 0, 2, 0), (7, 1, 0, 2, 1),
         (7, 1, 0, 3, 0), (7, 1, 0, 3, 1), (0, 0, 1, 0, 0), (5, 0, 1, 0, 0), (7, 0, 1, 0, 0),
         (1, 0, 0, 1, 0), (4, 0, 0, 1, 0), (0, 0, 3, 2, 0), (7, 0, 3, 2, 0), (5, 0, 3, 2, 0),
         (0, 0, 1, 1, 0), (7, 0, 1, 1, 0), (5, 0, 1, 1, 0), (1, 0, 0, 2, 0), (4, 0, 0, 2, 0),
         (5, 0, 0, 2, 1), (0, 1, 3, 1, 0), (6, 1, 3, 1, 0), (7, 1, 3, 1, 0), (0, 0, 1, 2, 0),
         (7, 0, 1, 2, 0), (5, 0, 1, 2, 0), (1, 0, 0, 3, 0), (4, 0, 0, 3, 0), (0, 1, 3, 1, 1),
         (7, 1, 3, 1, 1), (5, 0, 0, 3, 1), (0, 1, 3, 3, 0), (7, 1, 3, 3, 0), (5, 1, 3, 3, 0),
         (0, 0, 1, 3, 0), (7, 0, 1, 3, 0), (1, 1, 0, 1, 0), (4, 1, 0, 1, 0), (5, 1, 3, 1, 1),
         (0, 0, 3, 0, 0), (6, 0, 3, 0, 0), (7, 0, 3, 0, 0), (0, 1, 3, 2, 0), (7, 1, 3, 2, 0),
         (6, 1, 3, 2, 0), (1, 1, 0, 2, 0), (4, 1, 0, 2, 0), (0, 1, 1, 0, 0), (7, 1, 1, 0, 0),
         (5, 1, 1, 0, 0), (0, 0, 2, 0, 0), (7, 0, 2, 0, 0), (6, 0, 2, 0, 0), (0, 0, 3, 0, 1),
         (7, 0, 3, 0, 1), (5, 0, 3, 0, 1), (6, 1, 1, 0, 0), (0, 0, 1, 0, 1), (7, 0, 1, 0, 1),
         (0, 1, 3, 2, 1), (7, 1, 3, 2, 1), (0, 0, 1, 1, 1), (7, 0, 1, 1, 1), (0, 1, 1, 2, 0),
         (7, 1, 1, 2, 0), (0, 0, 2, 1, 0), (6, 0, 2, 1, 0), (5, 0, 2, 1, 0), (7, 0, 2, 1, 0),
         (0, 0, 2, 0, 1), (5, 0, 2, 0, 1), (7, 0, 2, 0, 1), (6, 1, 1, 2, 0), (0, 0, 1, 2, 1),
         (7, 0, 1, 2, 1), (5, 1, 1, 2, 0), (0, 1, 1, 0, 1), (7, 1, 1, 0, 1), (0, 0, 1, 3, 1),
         (7, 0, 1, 3, 1),),
        ((5, 1, 3, 2, 0), (0, 1, 1, 1, 0), (7, 1, 1, 1, 0), (0, 1, 2, 3, 0), (6, 1, 2, 3, 0),
         (7, 1, 2, 3, 0), (0, 0, 2, 1, 1), (7, 0, 2, 1, 1), (0, 0, 2, 2, 0), (7, 0, 2, 2, 0),
         (6, 0, 2, 2, 0), (0, 1, 1, 2, 1), (7, 1, 1, 2, 1), (0, 0, 3, 1, 1), (7, 0, 3, 1, 1),
         (6, 0, 3, 1, 1), (0, 1, 1, 3, 0), (7, 1, 1, 3, 0), (0, 1, 2, 2, 0), (5, 1, 2, 2, 0),
         (7, 1, 2, 2, 0), (0, 1, 2, 3, 1), (7, 1, 2, 3, 1), (0, 0, 2, 3, 0), (7, 0, 2, 3, 0),
         (6, 0, 2, 3, 0), (5, 1, 2, 3, 1), (0, 0, 2, 2, 1), (7, 0, 2, 2, 1), (5, 0, 2, 2, 1),
         (0, 0, 3, 3, 0), (7, 0, 3, 3, 0), (6, 0, 3, 3, 0), (0, 1, 2, 1, 0), (7, 1, 2, 1, 0),
         (0, 0, 3, 1, 0), (7, 0, 3, 1, 0), (6, 1, 2, 2, 0), (1, 1, 0, 3, 0), (4, 1, 0, 3, 0),
         (5, 1, 3, 2, 1), (0, 0, 2, 3, 1), (7, 0, 2, 3, 1), (5, 0, 2, 3, 1),),
        ((0, 1, 2, 0, 0), (7, 1, 2, 0, 0), (6, 1, 2, 0, 0), (5, 1, 0, 0, 0), (0, 0, 3, 3, 1),
         (7, 0, 3, 3, 1), (0, 0, 3, 2, 1), (7, 0, 3, 2, 1),),
        ((0, 1, 2, 2, 1), (7, 1, 2, 2, 1), (0, 1, 3, 0, 0), (6, 1, 3, 0, 0), (7, 1, 3, 0, 0),
         (5, 1, 0, 1, 1), (0, 1, 2, 0, 1), (7, 1, 2, 0, 1), (5, 1, 2, 0, 1), (0, 1, 3, 3, 1),
         (7, 1, 3, 3, 1), (5, 1, 0, 3, 1), (0, 1, 3, 0, 1), (7, 1, 3, 0, 1),),
        ((0, 1, 2, 1, 1), (7, 1, 2, 1, 1),),
        ((5, 1, 0, 2, 0), (0, 1, 1, 1, 1), (7, 1, 1, 1, 1), (5, 1, 0, 2, 1), (0, 1, 1, 3, 1),
         (7, 1, 1, 3, 1),),
        (),
        (),
    ),
    (
        ((3, 0, 0, 0, 0),),
        ((3, 0, 0, 1, 0),),
        (),
        (),
        (),
        (),
        (),
        (),
        ((2, 1, 0, 0, 0),),
        (),
        (),
        (),
        (),
        (),
        (),
        (),
        ((3, 0, 0, 3, 0),),
        ((1, 0, 0, 0, 0), (4, 0, 0, 0, 0), (1, 0, 0, 1, 0), (4, 0, 0, 1, 0), (3, 0, 0, 2, 0),
         (1, 0, 0, 3, 0), (4, 0, 0, 3, 0), (3, 1, 0, 1, 0), (3, 1, 0, 2, 0), (3, 1, 0, 3, 0),
         (1, 1, 0, 0, 0), (4, 1, 0, 0, 0), (3, 1, 0, 0, 0),),
        (),
        (),
        (),
        (),
        (),
        (),
        (),
    ),
    (
        ((3, 0, 0, 0, 0),),
        ((2, 0, 0, 1, 0),),
        (),
        (),
        (),
        (),
        (),
        (),
        (),
        (),
        (),
        (),
        (),
        (),
        (),
        (),
        ((3, 0, 0, 1, 0), (2, 0, 0, 2, 0), (0, 0, 0, 0, 0), (6, 0, 0, 0, 0), (7, 0, 0, 0, 0),
         (3, 1, 0, 0, 0), (2, 0, 0, 3, 0), (0, 0, 0, 1, 1), (6, 0, 0, 1, 1), (7, 0, 0, 1, 1),
         (0, 0, 0, 0, 1), (7, 0, 0, 0, 1), (0, 0, 1, 0, 0), (6, 0, 1, 0, 0), (7, 0, 1, 0, 0),
         (3, 1, 0, 3, 0), (0, 0, 1, 3, 0), (6, 0, 1, 3, 0), (2, 1, 0, 1, 0), (7, 0, 1, 3, 0),
         (0, 0, 0, 1, 0), (7, 0, 0, 1, 0), (0, 0, 3, 2, 0), (7, 0, 3, 2, 0), (6, 0, 3, 2, 0),
         (0, 0, 1, 0, 1), (7, 0, 1, 0, 1), (0, 0, 1, 1, 0), (7, 0, 1, 1, 0), (6, 0, 1, 1, 0),
         (0, 0, 3, 0, 0), (5, 0, 3, 0, 0), (7, 0, 3, 0, 0), (0, 0, 1, 3, 1), (7, 0, 1, 3, 1),
         (0, 1, 1, 1, 0), (7, 1, 1, 1, 0), (0, 0, 0, 2, 1), (7, 0, 0, 2, 1), (6, 0, 0, 2, 1),
         (2, 1, 0, 2, 0), (0, 0, 3, 2, 1), (7, 0, 3, 2, 1), (0, 0, 1, 2, 0), (7, 0, 1, 2, 0),
         (6, 0, 1, 2, 0), (5, 0, 1, 0, 1), (0, 0, 3, 1, 0), (7, 0, 3, 1, 0), (0, 1, 1, 3, 0),
         (7, 1, 1, 3, 0), (0, 0, 1, 1, 1), (7, 0, 1, 1, 1), (6, 0, 3, 1, 0), (0, 0, 0, 3, 1),
         (7, 0, 0, 3, 1), (5, 0, 1, 1, 1), (0, 0, 0, 2, 0), (7, 0, 0, 2, 0), (6, 0, 0, 3, 1),
         (0, 1, 3, 3, 0), (7, 1, 3, 3, 0), (0, 0, 1, 2, 1), (7, 0, 1, 2, 1), (5, 0, 1, 2, 1),),
        ((6, 1, 3, 3, 0), (0, 1, 3, 1, 1), (7, 1, 3, 1, 1), (5, 0, 1, 3, 1), (0, 0, 3, 1, 1),
         (7, 0, 3, 1, 1), (0, 0, 3, 0, 1), (7, 0, 3, 0, 1), (0, 0, 3, 3, 0), (6, 0, 3, 3, 0),
         (7, 0, 3, 3, 0), (0, 0, 0, 3, 0), (7, 0, 0, 3, 0),),
        ((6, 1, 1, 1, 0), (0, 0, 2, 2, 0), (7, 0, 2, 2, 0), (5, 0, 2, 2, 0), (0, 1, 1, 0, 0),
         (7, 1, 1, 0, 0), (5, 0, 3, 1, 1), (0, 1, 3, 3, 1), (7, 1, 3, 3, 1), (0, 0, 2, 0, 1),
         (7, 0, 2, 0, 1), (6, 0, 2, 0, 1), (0, 0, 3, 3, 1), (7, 0, 3, 3, 1),),
        ((0, 0, 2, 3, 0), (7, 0, 2, 3, 0), (5, 0, 2, 3, 0), (0, 0, 2, 1, 0), (7, 0, 2, 1, 0),
         (6, 0, 2, 1, 0), (5, 0, 3, 3, 0), (0, 1, 1, 1, 1), (7, 1, 1, 1, 1), (6, 1, 1, 3, 0),
         (0, 1, 1, 2, 0), (7, 1, 1, 2, 0), (2, 1, 0, 3, 0), (0, 0, 2, 0, 0), (7, 0, 2, 0, 0),
         (0, 1, 3, 0, 0), (6, 1, 3, 0, 0), (7, 1, 3, 0, 0), (0, 1, 3, 2, 0), (7, 1, 3, 2, 0),
         (0, 0, 2, 1, 1), (7, 0, 2, 1, 1), (0, 1, 2, 0, 0), (7, 1, 2, 0, 0), (5, 1, 2, 0, 0),
         (0, 1, 2, 2, 0), (7, 1, 2, 2, 0), (6, 1, 2, 2, 0), (5, 0, 3, 2, 1), (0, 1, 1, 3, 1),
         (7, 1, 1, 3, 1), (6, 1, 3, 1, 1), (0, 0, 2, 2, 1), (7, 0, 2, 2, 1), (5, 1, 3, 0, 0),
         (0, 1, 3, 0, 1), (7, 1, 3, 0, 1), (0, 1, 2, 3, 1), (7, 1, 2, 3, 1), (5, 1, 3, 3, 1),
         (0, 1, 2, 2, 1), (7, 1, 2, 2, 1), (6, 1, 2, 3, 1), (0, 1, 2, 1, 0), (7, 1, 2, 1, 0),
         (6, 1, 2, 1, 0), (0, 0, 2, 3, 1), (7, 0, 2, 3, 1),),
        ((0, 1, 3, 1, 0), (7, 1, 3, 1, 0), (6, 1, 1, 0, 0), (0, 1, 3, 2, 1), (7, 1, 3, 2, 1),),
        ((5, 1, 1, 1, 1), (0, 1, 2, 1, 1), (7, 1, 2, 1, 1), (5, 1, 2, 1, 1), (6, 1, 1, 2, 0),
         (0, 1, 0, 0, 0), (7, 1, 0, 0, 0), (5, 1, 1, 3, 1), (0, 1, 2, 3, 0), (7, 1, 2, 3, 0),
         (6, 1, 0, 0, 0), (0, 1, 2, 0, 1), (7, 1, 2, 0, 1),),
        ((0, 1, 1, 0, 1), (7, 1, 1, 0, 1), (0, 1, 0, 1, 1), (7, 1, 0, 1, 1), (6, 1, 0, 1, 1),
         (0, 1, 1, 2, 1), (7, 1, 1, 2, 1),),
        ((0, 1, 0, 3, 1), (7, 1, 0, 3, 1), (6, 1, 0, 3, 1), (0, 1, 0, 0, 1), (7, 1, 0, 0, 1),
         (0, 1, 0, 2, 0), (7, 1, 0, 2, 0), (0, 1, 0, 1, 0), (7, 1, 0, 1, 0), (0, 1, 0, 2, 1),
         (7, 1, 0, 2, 1), (0, 1, 0, 3, 0), (7, 1, 0, 3, 0),),
        (),
    ),
    (
        ((2, 0, 0, 0, 0),),
        (),
        ((3, 0, 0, 2, 0),),
        (),
        (),
        (),
        (),
        (),
        (),
        (),
        (),
        (),
        (),
        (),
        (),
        (),
        ((2, 0, 0, 1, 0), (3, 1, 0, 1, 0), (2, 0, 0, 3, 0), (3, 1, 0, 3, 0), (2, 1, 0, 0, 0),
         (1, 1, 0, 0, 0), (4, 1, 0, 0, 0), (3, 1, 0, 2, 0),),
        (),
        (),
        (),
        (),
        (),
        (),
        (),
        (),
    ),
    (
        ((3, 0, 1, 0, 0),),
        (),
        (),
        ((2, 0, 1, 3, 0),),
        (),
        (),
        (),
        (),
        (),
        (),
        (),
        (),
        (),
        (),
        (),
        (),
        ((3, 0, 1, 1, 0), (2, 1, 1, 1, 0),),
        ((1, 0, 1, 0, 0), (4, 0, 1, 0, 0), (3, 0, 1, 2, 0), (2, 1, 1, 3, 0), (3, 0, 1, 3, 0),
         (3, 1, 1, 0, 0), (3, 1, 1, 2, 0), (3, 1, 1, 1, 0), (1, 0, 1, 1, 0), (4, 0, 1, 1, 0),
         (3, 1, 1, 3, 0), (1, 0, 1, 2, 0), (4, 0, 1, 2, 0),),
        (),
        ((1, 1, 1, 3, 0), (4, 1, 1, 3, 0), (1, 1, 1, 1, 0), (4, 1, 1, 1, 0), (1, 1, 1, 2, 0),
         (4, 1, 1, 2, 0),),
        ((1, 1, 1, 0, 0), (4, 1, 1, 0, 0),),
        (),
        (),
        (),
        (),
    ),
    (
        ((5, 0, 1, 0, 0), (7, 0, 1, 0, 0),),
        (),
        (),
        (),
        (),
        ((7, 0, 1, 0, 1),),
        (),
        (),
        (),
        (),
        ((7, 0, 1, 1, 0),),
        (),
        (),
        (),
        (),
        ((7, 0, 1, 1, 1),),
        ((5, 0, 1, 1, 0), (7, 0, 1, 2, 0), (7, 0, 1, 2, 1), (7, 0, 1, 3, 0), (7, 0, 1, 3, 1),
         (7, 1, 1, 0, 0),),
        ((7, 1, 1, 0, 1), (0, 0, 0, 0, 0), (6, 0, 0, 0, 0), (7, 0, 0, 0, 0), (7, 1, 1, 1, 0),
         (7, 1, 1, 1, 1), (7, 1, 1, 2, 0), (7, 1, 1, 2, 1), (7, 1, 1, 3, 0), (0, 0, 0, 1, 0),
         (6, 0, 0, 1, 0), (7, 0, 0, 1, 0), (5, 0, 1, 2, 1), (1, 0, 1, 2, 0), (4, 0, 1, 2, 0),
         (7, 1, 1, 3, 1), (0, 0, 3, 0, 0), (6, 0, 3, 0, 0), (7, 0, 3, 0, 0), (0, 0, 0, 0, 1),
         (7, 0, 0, 0, 1), (0, 0, 0, 1, 1), (7, 0, 0, 1, 1), (0, 0, 0, 3, 0), (7, 0, 0, 3, 0),
         (0, 0, 3, 1, 0), (6, 0, 3, 1, 0), (7, 0, 3, 1, 0), (0, 0, 3, 0, 1), (7, 0, 3, 0, 1),
         (5, 0, 3, 0, 1), (5, 0, 0, 3, 0), (0, 0, 3, 1, 1), (7, 0, 3, 1, 1), (5, 0, 1, 3, 0),
         (0, 1, 3, 0, 0), (6, 1, 3, 0, 0), (7, 1, 3, 0, 0), (5, 0, 0, 0, 0), (0, 1, 3, 0, 1),
         (7, 1, 3, 0, 1), (5, 0, 0, 1, 1), (0, 1, 3, 3, 0), (6, 1, 3, 3, 0), (7, 1, 3, 3, 0),
         (0, 0, 0, 2, 0), (6, 0, 0, 2, 0), (7, 0, 0, 2, 0), (5, 0, 0, 2, 0), (0, 1, 3, 3, 1),
         (7, 1, 3, 3, 1), (0, 0, 2, 0, 0), (7, 0, 2, 0, 0), (0, 0, 3, 2, 0), (6, 0, 3, 2, 0),
         (7, 0, 3, 2, 0), (1, 0, 1, 3, 0), (4, 0, 1, 3, 0), (0, 0, 0, 2, 1), (7, 0, 0, 2, 1),
         (5, 0, 0, 2, 1), (0, 0, 3, 2, 1), (7, 0, 3, 2, 1), (5, 0, 3, 2, 1), (0, 0, 3, 3, 0),
         (6, 0, 3, 3, 0), (7, 0, 3, 3, 0), (0, 0, 2, 3, 0), (7, 0, 2, 3, 0), (1, 1, 1, 0, 0),
         (4, 1, 1, 0, 0), (0, 1, 0, 1, 0), (7, 1, 0, 1, 0), (6, 1, 0, 1, 0), (5, 0, 2, 3, 0),
         (0, 0, 3, 3, 1), (7, 0, 3, 3, 1), (5, 0, 3, 3, 1),),
        ((0, 0, 2, 2, 0), (7, 0, 2, 2, 0), (6, 0, 2, 2, 0), (0, 1, 0, 2, 0), (6, 1, 0, 2, 0),
         (5, 1, 0, 1, 0), (0, 0, 0, 3, 1), (7, 0, 0, 3, 1),),
        ((7, 1, 0, 2, 0), (0, 1, 0, 1, 1), (7, 1, 0, 1, 1), (0, 1, 0, 3, 0), (7, 1, 0, 3, 0),
         (5, 1, 0, 3, 0), (0, 1, 3, 2, 0), (7, 1, 3, 2, 0), (0, 1, 0, 2, 1), (7, 1, 0, 2, 1),
         (1, 1, 1, 1, 0), (4, 1, 1, 1, 0), (6, 1, 0, 3, 0), (0, 1, 2, 0, 0), (7, 1, 2, 0, 0),
         (0, 0, 2, 1, 0), (6, 0, 2, 1, 0), (5, 1, 3, 0, 1), (7, 0, 2, 1, 0), (0, 0, 2, 2, 1),
         (7, 0, 2, 2, 1), (6, 1, 2, 0, 0), (0, 1, 0, 0, 0), (7, 1, 0, 0, 0), (5, 1, 0, 2, 0),
         (0, 0, 2, 0, 1), (7, 0, 2, 0, 1), (0, 0, 2, 1, 1), (7, 0, 2, 1, 1), (0, 1, 2, 2, 0),
         (7, 1, 2, 2, 0), (0, 1, 3, 1, 1), (6, 1, 3, 1, 1), (5, 1, 0, 2, 1), (7, 1, 3, 1, 1),
         (0, 1, 0, 3, 1), (7, 1, 0, 3, 1), (6, 1, 3, 2, 0), (0, 1, 0, 0, 1), (7, 1, 0, 0, 1),
         (5, 1, 1, 0, 0), (0, 1, 2, 0, 1), (7, 1, 2, 0, 1), (0, 0, 2, 3, 1), (7, 0, 2, 3, 1),),
        ((5, 1, 1, 1, 1),),
        ((0, 1, 3, 1, 0), (7, 1, 3, 1, 0), (0, 1, 2, 3, 0), (7, 1, 2, 3, 0), (6, 1, 2, 3, 0),
         (5, 1, 1, 2, 1), (0, 1, 3, 2, 1), (7, 1, 3, 2, 1),),
        ((5, 1, 2, 0, 1), (0, 1, 2, 3, 1), (7, 1, 2, 3, 1), (0, 1, 2, 1, 0), (6, 1, 2, 1, 0),
         (7, 1, 2, 1, 0), (5, 1, 2, 3, 1), (5, 1, 1, 3, 0), (0, 1, 2, 1, 1), (7, 1, 2, 1, 1),
         (5, 1, 1, 3, 1), (0, 1, 2, 2, 1), (7, 1, 2, 2, 1),),
        (),
        (),
    ),
    (
        ((2, 0, 1, 0, 0), (3, 0, 1, 0, 0),),
        (),
        (),
        (),
        (),
        (),
        (),
        (),
        (),
        (),
        (),
        (),
        (),
        (),
        (),
        (),
        ((2, 0, 1, 1, 0), (2, 0, 1, 2, 0), (1, 0, 1, 3, 0), (4, 0, 1, 3, 0), (2, 1, 1, 3, 0),
         (1, 1, 1, 1, 0), (4, 1, 1, 1, 0), (2, 1, 1, 1, 0), (1, 1, 1, 3, 0), (4, 1, 1, 3, 0),
         (2, 1, 1, 2, 0), (3, 0, 1, 3, 0), (2, 1, 1, 0, 0), (3, 0, 1, 2, 0),),
        ((3, 1, 1, 0, 0),),
        ((3, 1, 1, 2, 0),),
        (),
        (),
        (),
        (),
        (),
        (),
    ),
    (
        ((3, 0, 1, 0, 0),),
        (),
        ((2, 0, 1, 2, 0),),
        (),
        (),
        (),
        (),
        (),
        (),
        (),
        (),
        (),
        (),
        (),
        (),
        (),
        ((2, 0, 1, 3, 0), (0, 0, 1, 0, 0), (6, 0, 1, 0, 0), (7, 0, 1, 0, 0), (2, 1, 1, 0, 0),
         (0, 0, 1, 0, 1), (7, 0, 1, 0, 1), (0, 0, 1, 1, 0), (6, 0, 1, 1, 0), (7, 0, 1, 1, 0),
         (2, 1, 1, 1, 0), (0, 0, 3, 1, 0), (7, 0, 3, 1, 0), (6, 0, 3, 1, 0), (0, 0, 1, 1, 1),
         (7, 0, 1, 1, 1), (0, 0, 1, 2, 1), (6, 0, 1, 2, 1), (7, 0, 1, 2, 1), (0, 0, 3, 1, 1),
         (7, 0, 3, 1, 1), (0, 0, 3, 2, 0), (7, 0, 3, 2, 0), (5, 0, 3, 2, 0), (0, 0, 3, 0, 1),
         (6, 0, 3, 0, 1), (7, 0, 3, 0, 1), (0, 0, 1, 2, 0), (7, 0, 1, 2, 0), (0, 0, 0, 3, 0),
         (6, 0, 0, 3, 0), (7, 0, 0, 3, 0), (0, 1, 0, 0, 0), (6, 1, 0, 0, 0), (3, 0, 1, 1, 0),
         (7, 1, 0, 0, 0), (0, 0, 3, 0, 0), (7, 0, 3, 0, 0), (0, 0, 3, 3, 0), (7, 0, 3, 3, 0),
         (5, 0, 3, 3, 0), (0, 0, 1, 3, 0), (7, 0, 1, 3, 0), (6, 0, 1, 3, 0), (0, 0, 0, 3, 1),
         (7, 0, 0, 3, 1), (0, 0, 0, 0, 0), (7, 0, 0, 0, 0), (6, 0, 0, 0, 0), (3, 1, 1, 3, 0),
         (5, 0, 0, 3, 1), (0, 1, 0, 0, 1), (7, 1, 0, 0, 1), (0, 1, 3, 1, 0), (7, 1, 3, 1, 0),
         (0, 0, 0, 1, 1), (7, 0, 0, 1, 1), (6, 0, 0, 1, 1), (0, 0, 1, 3, 1), (7, 0, 1, 3, 1),),
        ((0, 0, 0, 2, 0), (7, 0, 0, 2, 0), (0, 0, 2, 0, 0), (6, 0, 2, 0, 0), (3, 1, 1, 2, 0),
         (7, 0, 2, 0, 0), (0, 0, 0, 0, 1), (7, 0, 0, 0, 1), (6, 1, 3, 1, 0), (0, 1, 3, 2, 0),
         (7, 1, 3, 2, 0), (5, 1, 3, 2, 0), (0, 0, 0, 2, 1), (7, 0, 0, 2, 1), (0, 0, 0, 1, 0),
         (7, 0, 0, 1, 0),),
        ((0, 0, 3, 2, 1), (7, 0, 3, 2, 1), (3, 1, 1, 1, 0), (0, 0, 2, 1, 0), (7, 0, 2, 1, 0),
         (5, 0, 2, 1, 0), (6, 0, 2, 1, 0), (0, 0, 2, 0, 1), (7, 0, 2, 0, 1), (5, 0, 2, 0, 1),
         (6, 1, 3, 2, 0), (0, 0, 3, 3, 1), (7, 0, 3, 3, 1),),
        ((0, 1, 3, 1, 1), (7, 1, 3, 1, 1), (5, 1, 3, 1, 1), (0, 0, 2, 3, 0), (7, 0, 2, 3, 0),
         (6, 0, 2, 3, 0), (5, 1, 0, 0, 1), (0, 0, 2, 1, 1), (7, 0, 2, 1, 1), (0, 1, 0, 1, 0),
         (7, 1, 0, 1, 0), (0, 0, 2, 2, 0), (7, 0, 2, 2, 0), (6, 0, 2, 2, 0), (0, 1, 3, 2, 1),
         (7, 1, 3, 2, 1), (6, 1, 0, 1, 0), (0, 1, 0, 3, 0), (7, 1, 0, 3, 0), (0, 0, 2, 3, 1),
         (7, 0, 2, 3, 1), (5, 0, 2, 3, 1), (6, 1, 0, 3, 0), (0, 1, 3, 0, 1), (7, 1, 3, 0, 1),
         (0, 1, 2, 3, 0), (7, 1, 2, 3, 0), (5, 1, 2, 3, 0), (0, 0, 2, 2, 1), (7, 0, 2, 2, 1),),
        ((6, 1, 3, 0, 1), (0, 1, 0, 2, 0), (7, 1, 0, 2, 0), (0, 1, 0, 1, 1), (7, 1, 0, 1, 1),
         (0, 1, 3, 3, 0), (7, 1, 3, 3, 0), (6, 1, 3, 3, 0), (0, 1, 0, 2, 1), (7, 1, 0, 2, 1),
         (0, 1, 2, 1, 0), (5, 1, 2, 1, 0), (7, 1, 2, 1, 0), (0, 1, 0, 3, 1), (7, 1, 0, 3, 1),),
        ((0, 1, 1, 0, 0), (7, 1, 1, 0, 0), (0, 1, 2, 2, 0), (7, 1, 2, 2, 0), (6, 1, 2, 2, 0),
         (0, 1, 3, 0, 0), (7, 1, 3, 0, 0), (6, 1, 2, 1, 0), (0, 1, 1, 1, 1), (7, 1, 1, 1, 1),
         (0, 1, 2, 0, 0), (7, 1, 2, 0, 0), (0, 1, 3, 3, 1), (7, 1, 3, 3, 1),),
        ((6, 1, 1, 0, 0), (0, 1, 1, 2, 1), (7, 1, 1, 2, 1), (0, 1, 2, 2, 1), (5, 1, 2, 2, 1),
         (7, 1, 2, 2, 1), (6, 1, 1, 1, 1), (0, 1, 2, 0, 1), (7, 1, 2, 0, 1), (0, 1, 2, 1, 1),
         (7, 1, 2, 1, 1), (6, 1, 1, 2, 1), (0, 1, 2, 3, 1), (7, 1, 2, 3, 1),),
        ((0, 1, 1, 0, 1), (7, 1, 1, 0, 1), (0, 1, 1, 3, 0), (7, 1, 1, 3, 0), (0, 1, 1, 1, 0),
         (7, 1, 1, 1, 0), (0, 1, 1, 3, 1), (7, 1, 1, 3, 1), (0, 1, 1, 2, 0), (7, 1, 1, 2, 0),),
        (),
    ),
)


def local_plain(tokens, norm_gain, up_trained, down_trained):
    shards = lax.axis_size("fs")
    groups = lax.axis_size("tp")
    rows_local = up_trained.shape[0]
    cols_local = up_trained.shape[1]
    folded = (norm_gain[:, None] * up_trained).astype(jnp.bfloat16)
    stacked = jnp.stack([folded, down_trained.astype(jnp.bfloat16)])
    served_width = cols_local * groups // shards
    blocks_here = cols_local // served_width
    quarter_rows = rows_local // groups
    pieces = stacked.reshape(2, groups, quarter_rows, blocks_here, served_width)
    moved = lax.all_to_all(pieces, "tp", split_axis=1, concat_axis=3, tiled=True)
    placed = lax.all_to_all(moved, "fs", split_axis=3, concat_axis=2, tiled=True)
    ordered = placed.reshape(2, shards, quarter_rows, served_width)
    joined = lax.all_gather(ordered, "tp", axis=2, tiled=True)
    owned = joined.reshape(2, rows_local * shards, served_width)
    up_serving = owned[0]
    down_serving = owned[1]
    values = tokens.astype(jnp.float32)
    scale = lax.rsqrt(jnp.mean(values * values, axis=1, keepdims=True) + epsilon)
    normed = (values * scale).astype(jnp.bfloat16)
    hidden = jnp.dot(normed, up_serving, preferred_element_type=jnp.float32)
    active = jnp.square(jax.nn.relu(hidden)).astype(jnp.bfloat16)
    summed = lax.psum_scatter(
        lax.dot_general(
            down_serving, active, (((1,), (1,)), ((), ())), preferred_element_type=jnp.float32
        ),
        "fs",
        scatter_dimension=0,
        tiled=True,
    )
    prompt_output = summed.T.astype(jnp.bfloat16)
    return (up_serving, down_serving, prompt_output)


def kernel(
    tokens_hbm, gain_hbm, up_hbm, down_hbm, whole, prompt_out,
    raw, gain_rows, gain, cast, relay, toks, normed, hidden, active, rs_send, rs_recv, rs_own,
    in_sem, misc_sem, got_sem, relay_sem, block_sem, src_sem, out_sem, rs_ssem, rs_rsem,
):
    y = lax.axis_index("grp")
    z = lax.axis_index("fs")
    t = lax.axis_index("tp")
    mirrored = z // 2
    role = jnp.where(mirrored == 1, 4 * (3 - z) + (3 - t), 4 * z + t)
    is_own = z == t
    is_active = t % 2 == z % 2
    t_x = jnp.where(t < 2, t + 2, t - 2)
    t_c = t + 1 - 2 * (t % 2)
    to_x = {"tp": t_x}
    to_c = {"tp": t_c}
    to_y = {"grp": 1 - y}
    rows_local, width = cast.shape[1], cast.shape[2]
    size = rows_local // (2 * PAIRS)
    trained = (up_hbm, down_hbm)
    planes = [jnp.where(mirrored == 1, 3 - k, k) for k in range(4)]
    sides = [y, 1 - y]

    def part(pair, side):
        return 2 * pair + sides[side]

    def ds(start, extent):
        return pl.ds(pl.multiple_of(start, extent), extent)

    def local_rows(pair, side):
        return ds(part(pair, side) * size, size)

    def unit(m, plane, pair, side):
        return whole.at[m, ds(plane * rows_local + part(pair, side) * size, size)]

    def remote(src, dst, ssem, rsem, where):
        return pltpu.make_async_remote_copy(
            src_ref=src, dst_ref=dst, send_sem=ssem, recv_sem=rsem,
            device_id=where, device_id_type=MESH,
        )

    def fetch(m, pair, side):
        rows = local_rows(pair, side)
        return pltpu.make_async_copy(
            trained[m].at[rows], raw.at[m, rows], in_sem.at[m, 2 * pair + side]
        )

    get_gain = pltpu.make_async_copy(gain_hbm, gain_rows, misc_sem.at[0])
    get_toks = pltpu.make_async_copy(tokens_hbm, toks, misc_sem.at[1])
    get_gain.start()
    for pair in range(PAIRS):
        fetch(0, pair, 0).start()

    barrier = pltpu.get_barrier_semaphore()
    others = [{"fs": lax.rem(z + k, 4)} for k in range(1, 4)]
    for where in [to_x, to_c, to_y] + others:
        pl.semaphore_signal(barrier, inc=1, device_id=where, device_id_type=MESH)

    get_gain.wait()
    lanes = gain_rows.shape[1]
    for q in range(gain_rows.shape[0]):
        square = (lanes, lanes)
        chosen = jnp.where(
            lax.broadcasted_iota(jnp.int32, square, 0) == lax.broadcasted_iota(jnp.int32, square, 1),
            jnp.broadcast_to(gain_rows[pl.ds(q, 1), :], square), 0.0,
        )
        column = jnp.sum(chosen, axis=1, keepdims=True)
        gain[pl.ds(q * lanes, lanes), :] = jnp.broadcast_to(column, square)

    piece = 16

    def cast_unit(m, pair, side):
        fetch(m, pair, side).wait()
        base = part(pair, side) * size

        def store(into, shift):
            @pl.loop(0, size // piece)
            def _(i):
                here = ds(base + i * piece, piece)
                there = ds(shift + base + i * piece, piece)
                if m == 0:
                    factor = gain[here, :]
                    for j in range(width // lanes):
                        cols = pl.ds(j * lanes, lanes)
                        into[0, there, cols] = (raw[0, here, cols] * factor).astype(jnp.bfloat16)
                else:
                    into[m, there, :] = raw[m, here, :].astype(jnp.bfloat16)

        @pl.when(is_own)
        def _():
            store(whole, z * rows_local)

        if side == 0:
            @pl.when(jnp.logical_not(is_own))
            def _():
                store(cast, 0)

    def step(kind, m, k, pair, side):
        plane = planes[k]
        place = part(pair, side)
        if kind == GET:
            here = unit(m, plane, pair, side)
            remote(here, here, out_sem.at[0, m], got_sem.at[m, plane, place], to_x).wait_recv()
        elif kind == GET_RELAY:
            here = relay.at[m, ds(place * size, size)]
            remote(here, here, src_sem.at[m], relay_sem.at[m, place], to_x).wait_recv()
        elif kind == SWAP:
            remote(
                cast.at[m, local_rows(pair, side)], relay.at[m, ds(place * size, size)],
                src_sem.at[m], relay_sem.at[m, place], to_x,
            ).start()
        elif kind in (HOP, HOP_RELAY):
            src = (cast if kind == HOP else relay).at[m, ds(place * size, size)]
            remote(
                src, unit(m, z, pair, side), src_sem.at[m], got_sem.at[m, z, place],
                {"fs": t if kind == HOP else t_x},
            ).start()
        elif kind == SEND_CORE:
            here = unit(m, plane, pair, side)
            remote(here, here, out_sem.at[2, m], block_sem.at[m, plane], to_c).start()
        else:
            here = unit(m, plane, pair, side)
            i = kind - SEND_X
            remote(
                here, here, out_sem.at[i, m], got_sem.at[m, plane, place], (to_x, to_y)[i]
            ).start()

    def run(segment):
        for r in range(8):
            if SCHEDULE[r][segment]:
                @pl.when(role == r)
                def _():
                    for s in SCHEDULE[r][segment]:
                        step(*s)

    casts = [(m, pair, side) for m in range(2) for side in range(2) for pair in range(PAIRS)]
    segment = 0
    for m, pair, side in casts:
        if side == 1:
            pl.when(is_own)(lambda: cast_unit(m, pair, side))
        else:
            cast_unit(m, pair, side)
        if segment == 0:
            @pl.when(is_own)
            def _():
                for p in range(PAIRS):
                    fetch(0, p, 1).start()
            for p in range(PAIRS):
                fetch(1, p, 0).start()
            @pl.when(is_own)
            def _():
                for p in range(PAIRS):
                    fetch(1, p, 1).start()
            get_toks.start()
            pl.semaphore_wait(barrier, 6)
        run(segment)
        segment += 1

    get_toks.wait()
    tokens_here = toks.shape[0]

    @pl.loop(0, tokens_here // piece)
    def _(i):
        here = ds(i * piece, piece)
        values = toks[here, :].astype(jnp.float32)
        scale = lax.rsqrt(jnp.mean(values * values, axis=1, keepdims=True) + epsilon)
        normed[here, :] = (values * scale).astype(jnp.bfloat16)

    def pick(table):
        chosen = planes[table[0]]
        for r in range(1, 8):
            if table[r] != table[0]:
                chosen = jnp.where(role == r, planes[table[r]], chosen)
        return chosen

    def listen(m, plane):
        @pl.when(jnp.logical_not(is_active))
        def _():
            here = whole.at[m, ds(plane * rows_local, rows_local)]
            remote(here, here, out_sem.at[2, m], block_sem.at[m, plane], to_c).wait_recv()

    tile = 512 if width % 512 == 0 else width

    def compute_up(k):
        plane = pick(ORDER[0][k])
        listen(0, plane)
        rows = ds(plane * rows_local, rows_local)

        @pl.loop(0, width // tile)
        def _(n):
            cols = ds(n * tile, tile)
            product = jnp.dot(
                normed[:, rows], whole[0, rows, cols], preferred_element_type=jnp.float32
            )
            if k > 0:
                product = product + hidden[:, cols]
            if k < 3:
                hidden[:, cols] = product
            else:
                active[:, cols] = jnp.square(jnp.maximum(product, 0.0)).astype(jnp.bfloat16)

    d_tile = 256 if rows_local % 256 == 0 else rows_local

    def scatter(k, plane):
        slot = lax.rem(z - plane + 3, 4)
        return remote(
            rs_send.at[k], rs_recv.at[slot], rs_ssem.at[k], rs_rsem.at[slot], {"fs": plane}
        )

    def compute_down(k):
        plane = pick(ORDER[1][k])
        listen(1, plane)

        @pl.loop(0, rows_local // d_tile)
        def _(n):
            cols = ds(n * d_tile, d_tile)
            product = lax.dot_general(
                active[...], whole[1, ds(plane * rows_local + n * d_tile, d_tile), :],
                (((1,), (1,)), ((), ())), preferred_element_type=jnp.float32,
            )
            if k < 3:
                rs_send[k, :, cols] = product.astype(jnp.bfloat16)
            else:
                rs_own[:, cols] = product
        if k < 3:
            scatter(k, plane).start()

    for m in range(2):
        for k in range(4):
            run(segment)
            segment += 1
            (compute_up, compute_down)[m](k)
    run(segment)

    for k in range(3):
        here = rs_recv.at[k]
        remote(here, here, rs_ssem.at[k], rs_rsem.at[k], {"fs": lax.rem(z + 1, 4)}).wait_recv()

    @pl.loop(0, tokens_here // piece)
    def _(i):
        here = ds(i * piece, piece)
        total = rs_own[here, :]
        for k in range(3):
            total = total + rs_recv[k, here, :].astype(jnp.float32)
        prompt_out[here, :] = total.astype(prompt_out.dtype)

    def drain(sem, m, count):
        sent = whole.at[m, pl.ds(0, count * size)]
        remote(sent, sent, sem, got_sem.at[0, 0, 0], to_x).wait_send()

    for r in range(8):
        @pl.when(role == r)
        def _():
            for m in range(2):
                steps = [s for part_of in SCHEDULE[r] for s in part_of if s[1] == m]
                hops = sum(s[0] in (SWAP, HOP, HOP_RELAY) for s in steps)
                if hops:
                    drain(src_sem.at[m], m, hops)
                for i, kind in enumerate((SEND_X, SEND_Y, SEND_CORE)):
                    sends = sum(s[0] == kind for s in steps)
                    if sends:
                        drain(out_sem.at[i, m], m, sends)
    for k in range(3):
        here = rs_send.at[k]
        remote(here, here, rs_ssem.at[k], rs_rsem.at[k], {"fs": lax.rem(z + 1, 4)}).wait_send()


pieces_out = 8


def deliver(whole, prompt, up_out, down_out, prompt_out, sems, last):
    rows = whole.shape[1] // pieces_out
    copies = [
        pltpu.make_async_copy(
            whole.at[m, pl.ds(i * rows, rows)], out.at[pl.ds(i * rows, rows)], sems.at[m, i]
        )
        for m, out in enumerate((up_out, down_out))
        for i in range(pieces_out)
    ]
    copies.append(pltpu.make_async_copy(prompt, prompt_out, last))
    for copy in copies:
        copy.start()
    for copy in copies:
        copy.wait()


def local_kernel(tokens, norm_gain, up_trained, down_trained):
    shards = lax.axis_size("fs")
    rows_local, width = up_trained.shape
    tokens_here, features = tokens.shape
    any_space = pl.BlockSpec(memory_space=pl.ANY)
    dma = pltpu.SemaphoreType.DMA
    bf16, f32 = jnp.bfloat16, jnp.float32
    whole, prompt = pl.pallas_call(
        kernel,
        out_shape=(
            pltpu.VMEM((2, rows_local * shards, width), bf16),
            pltpu.VMEM((tokens_here, rows_local), bf16),
        ),
        in_specs=[any_space] * 4,
        out_specs=(pl.BlockSpec(memory_space=pltpu.VMEM),) * 2,
        scratch_shapes=[
            pltpu.VMEM((2, rows_local, width), f32),
            pltpu.VMEM((rows_local // 128, 128), f32),
            pltpu.VMEM((rows_local, 128), f32),
            pltpu.VMEM((2, rows_local, width), bf16),
            pltpu.VMEM((2, rows_local, width), bf16),
            pltpu.VMEM((tokens_here, features), bf16),
            pltpu.VMEM((tokens_here, features), bf16),
            pltpu.VMEM((tokens_here, width), f32),
            pltpu.VMEM((tokens_here, width), bf16),
            pltpu.VMEM((3, tokens_here, rows_local), bf16),
            pltpu.VMEM((3, tokens_here, rows_local), bf16),
            pltpu.VMEM((tokens_here, rows_local), f32),
            dma((2, 2 * PAIRS)), dma((2,)),
            dma((2, 4, 2 * PAIRS)), dma((2, 2 * PAIRS)), dma((2, 4)),
            dma((2,)), dma((3, 2)), dma((3,)), dma((3,)),
        ],
        compiler_params=pltpu.CompilerParams(
            collective_id=0, has_side_effects=True, vmem_limit_bytes=40 * 1024 * 1024
        ),
    )(tokens, norm_gain.reshape(rows_local // 128, 128), up_trained, down_trained)
    held = pl.BlockSpec(memory_space=pltpu.VMEM)
    return tuple(pl.pallas_call(
        deliver,
        out_shape=(
            jax.ShapeDtypeStruct((rows_local * shards, width), bf16),
            jax.ShapeDtypeStruct((rows_local * shards, width), bf16),
            jax.ShapeDtypeStruct((tokens_here, rows_local), bf16),
        ),
        in_specs=[held, held],
        out_specs=(any_space,) * 3,
        scratch_shapes=[dma((2, pieces_out)), dma(())],
        compiler_params=pltpu.CompilerParams(vmem_limit_bytes=8 * 1024 * 1024),
    )(whole, prompt))


def solution(mesh):
    in_specs = (P(("grp", "tp"), None), P("fs"), P("fs", "tp"), P("fs", "tp"))
    out_specs = (P("grp", "fs"), P("grp", "fs"), P(("grp", "tp"), "fs"))
    sizes = mesh.shape
    square = sizes["grp"] == 2 and sizes["fs"] == 4 and sizes["tp"] == 4
    local = local_kernel if square else local_plain
    return jax.shard_map(local, mesh=mesh, in_specs=in_specs, out_specs=out_specs, check_vma=False)
```

```python
import jax
import jax.numpy as jnp
from jax import lax
from jax.experimental import pallas as pl
from jax.experimental.pallas import tpu as pltpu
from jax.sharding import PartitionSpec as P

epsilon = 1e-06
MESH = pl.DeviceIdType.MESH

GET, GET_RELAY, SWAP, HOP, HOP_RELAY, SEND_X, SEND_Y, SEND_CORE = range(8)
PAIRS = 4
ORDER = (
    (
        (0, 0, 0, 0, 1, 1, 3, 3),
        (3, 3, 3, 3, 3, 3, 1, 1),
        (1, 1, 1, 1, 0, 0, 0, 0),
        (2, 2, 2, 2, 2, 2, 2, 2),
    ),
    (
        (1, 1, 1, 1, 3, 3, 3, 3),
        (2, 2, 3, 3, 0, 0, 2, 2),
        (3, 3, 2, 2, 2, 2, 0, 0),
        (0, 0, 0, 0, 1, 1, 1, 1),
    ),
)
SCHEDULE = (
    (
        ((5, 0, 0, 0, 0), (7, 0, 0, 0, 0),),
        ((5, 0, 0, 1, 0),),
        (),
        (),
        (),
        ((7, 0, 0, 0, 1),),
        (),
        ((5, 0, 0, 2, 0),),
        (),
        (),
        ((7, 0, 0, 1, 0),),
        (),
        (),
        (),
        (),
        ((7, 0, 0, 1, 1),),
        ((7, 0, 0, 2, 0), (7, 0, 0, 2, 1), (7, 0, 0, 3, 0), (7, 0, 0, 3, 1), (7, 1, 0, 0, 0),),
        ((7, 1, 0, 0, 1), (7, 1, 0, 1, 0), (7, 1, 0, 1, 1), (7, 1, 0, 2, 0), (7, 1, 0, 2, 1),
         (7, 1, 0, 3, 0), (5, 0, 0, 3, 0), (7, 1, 0, 3, 1), (1, 0, 0, 0, 0), (4, 0, 0, 0, 0),
         (0, 0, 1, 0, 0), (7, 0, 1, 0, 0), (5, 0, 1, 0, 0), (0, 0, 3, 0, 0), (6, 0, 3, 0, 0),
         (7, 0, 3, 0, 0), (5, 1, 0, 0, 1), (0, 0, 3, 0, 1), (7, 0, 3, 0, 1), (1, 0, 0, 1, 0),
         (4, 0, 0, 1, 0), (0, 0, 1, 2, 0), (7, 0, 1, 2, 0), (5, 0, 1, 2, 0), (0, 0, 3, 2, 0),
         (6, 0, 3, 2, 0), (7, 0, 3, 2, 0), (0, 0, 3, 2, 1), (7, 0, 3, 2, 1), (5, 0, 3, 2, 1),
         (1, 0, 0, 3, 0), (4, 0, 0, 3, 0), (0, 0, 1, 3, 0), (6, 0, 1, 3, 0), (7, 0, 1, 3, 0),
         (0, 0, 3, 3, 0), (7, 0, 3, 3, 0), (6, 0, 3, 3, 0), (5, 0, 3, 3, 0), (0, 0, 1, 3, 1),
         (7, 0, 1, 3, 1), (5, 0, 1, 3, 1), (1, 1, 0, 0, 0), (4, 1, 0, 0, 0), (0, 1, 3, 0, 0),
         (7, 1, 3, 0, 0), (0, 0, 3, 3, 1), (7, 0, 3, 3, 1), (5, 1, 3, 0, 0), (1, 1, 0, 1, 0),
         (4, 1, 0, 1, 0), (0, 1, 1, 0, 0), (7, 1, 1, 0, 0), (5, 1, 1, 0, 0), (0, 1, 3, 3, 0),
         (6, 1, 3, 3, 0), (7, 1, 3, 3, 0), (0, 0, 3, 1, 0), (7, 0, 3, 1, 0), (5, 1, 3, 3, 0),
         (0, 1, 3, 3, 1), (7, 1, 3, 3, 1), (0, 0, 1, 0, 1), (7, 0, 1, 0, 1), (0, 0, 2, 0, 0),
         (6, 0, 2, 0, 0), (5, 0, 2, 0, 0), (0, 0, 1, 1, 0), (7, 0, 1, 1, 0), (7, 0, 2, 0, 0),
         (0, 0, 3, 1, 1), (7, 0, 3, 1, 1),),
        ((0, 0, 2, 0, 1), (7, 0, 2, 0, 1), (5, 0, 2, 0, 1), (0, 0, 1, 1, 1), (7, 0, 1, 1, 1),
         (0, 1, 1, 2, 0), (6, 1, 1, 2, 0), (5, 1, 1, 2, 0), (7, 1, 1, 2, 0), (0, 0, 2, 3, 0),
         (6, 0, 2, 3, 0), (7, 0, 2, 3, 0), (0, 0, 1, 2, 1), (7, 0, 1, 2, 1),),
        ((0, 1, 1, 2, 1), (7, 1, 1, 2, 1), (1, 1, 0, 2, 0), (4, 1, 0, 2, 0), (0, 1, 1, 3, 0),
         (6, 1, 1, 3, 0), (7, 1, 1, 3, 0), (0, 0, 2, 1, 0), (7, 0, 2, 1, 0), (5, 0, 2, 1, 0),
         (6, 0, 2, 1, 0), (0, 0, 2, 3, 1), (7, 0, 2, 3, 1), (5, 0, 2, 3, 1), (0, 1, 3, 2, 1),
         (7, 1, 3, 2, 1), (6, 1, 3, 2, 1), (0, 1, 1, 3, 1), (7, 1, 1, 3, 1), (5, 1, 1, 2, 1),
         (0, 1, 1, 0, 1), (7, 1, 1, 0, 1), (0, 0, 2, 2, 0), (7, 0, 2, 2, 0), (5, 0, 2, 2, 0),
         (6, 0, 2, 2, 0), (0, 0, 2, 1, 1), (7, 0, 2, 1, 1), (5, 1, 1, 3, 0), (0, 1, 1, 1, 1),
         (7, 1, 1, 1, 1), (0, 1, 2, 2, 0), (7, 1, 2, 2, 0), (6, 1, 2, 2, 0), (0, 1, 3, 2, 0),
         (7, 1, 3, 2, 0), (5, 1, 1, 3, 1), (0, 1, 1, 1, 0), (7, 1, 1, 1, 0), (0, 1, 2, 1, 0),
         (6, 1, 2, 1, 0), (7, 1, 2, 1, 0), (0, 1, 2, 3, 0), (6, 1, 2, 3, 0), (7, 1, 2, 3, 0),
         (0, 0, 2, 2, 1), (7, 0, 2, 2, 1),),
        ((5, 1, 0, 1, 0),),
        ((0, 1, 3, 0, 1), (7, 1, 3, 0, 1), (0, 1, 2, 2, 1), (7, 1, 2, 2, 1), (5, 1, 0, 2, 0),
         (0, 1, 3, 1, 0), (7, 1, 3, 1, 0), (0, 1, 2, 1, 1), (7, 1, 2, 1, 1), (5, 1, 2, 2, 0),
         (0, 1, 2, 0, 0), (7, 1, 2, 0, 0), (0, 1, 2, 3, 1), (7, 1, 2, 3, 1), (5, 1, 2, 2, 1),
         (0, 1, 2, 0, 1), (7, 1, 2, 0, 1),),
        ((5, 1, 0, 3, 0), (0, 1, 3, 1, 1), (7, 1, 3, 1, 1),),
        (),
        ((5, 1, 0, 3, 1),),
    ),
    (
        ((3, 0, 0, 0, 0),),
        ((3, 0, 0, 1, 0),),
        (),
        (),
        (),
        (),
        (),
        (),
        (),
        (),
        (),
        ((3, 0, 0, 3, 0),),
        (),
        (),
        (),
        (),
        (),
        ((1, 0, 0, 0, 0), (4, 0, 0, 0, 0), (1, 0, 0, 1, 0), (4, 0, 0, 1, 0), (3, 0, 0, 2, 0),
         (1, 1, 0, 2, 0), (4, 1, 0, 2, 0), (3, 1, 0, 1, 0), (3, 1, 0, 2, 0), (3, 1, 0, 3, 0),),
        ((1, 1, 0, 1, 0), (4, 1, 0, 1, 0), (3, 1, 0, 0, 0),),
        (),
        (),
        (),
        (),
        (),
        (),
    ),
    (
        ((2, 0, 0, 0, 0),),
        (),
        ((3, 0, 0, 2, 0),),
        (),
        (),
        (),
        (),
        (),
        (),
        (),
        (),
        ((2, 0, 0, 1, 0),),
        (),
        (),
        (),
        (),
        ((3, 0, 0, 3, 0), (0, 0, 0, 0, 0), (6, 0, 0, 0, 0), (7, 0, 0, 0, 0), (2, 0, 0, 3, 0),
         (3, 1, 0, 2, 0), (0, 0, 0, 1, 0), (6, 0, 0, 1, 0), (7, 0, 0, 1, 0), (0, 0, 0, 0, 1),
         (7, 0, 0, 0, 1), (0, 0, 0, 2, 0), (6, 0, 0, 2, 0), (7, 0, 0, 2, 0), (0, 0, 0, 1, 1),
         (7, 0, 0, 1, 1), (2, 1, 0, 0, 0), (3, 1, 0, 3, 0), (0, 0, 1, 1, 0), (7, 0, 1, 1, 0),
         (6, 0, 1, 1, 0), (0, 0, 1, 0, 0), (6, 0, 1, 0, 0), (7, 0, 1, 0, 0), (0, 0, 0, 2, 1),
         (7, 0, 0, 2, 1), (0, 0, 0, 3, 0), (7, 0, 0, 3, 0), (6, 0, 0, 3, 0), (0, 0, 1, 1, 1),
         (7, 0, 1, 1, 1), (2, 1, 0, 1, 0), (0, 0, 1, 2, 0), (7, 0, 1, 2, 0), (6, 0, 1, 2, 0),
         (0, 0, 3, 0, 0), (7, 0, 3, 0, 0), (6, 0, 3, 0, 0), (0, 0, 1, 0, 1), (7, 0, 1, 0, 1),
         (0, 1, 1, 1, 0), (7, 1, 1, 1, 0), (0, 1, 0, 0, 1), (7, 1, 0, 0, 1), (0, 0, 0, 3, 1),
         (7, 0, 0, 3, 1),),
        ((5, 0, 1, 0, 1), (0, 0, 3, 2, 1), (7, 0, 3, 2, 1), (0, 0, 3, 1, 0), (5, 0, 3, 1, 0),
         (6, 0, 3, 1, 0), (7, 0, 3, 1, 0), (6, 0, 3, 2, 1), (0, 0, 1, 2, 1), (7, 0, 1, 2, 1),
         (0, 0, 3, 3, 0), (7, 0, 3, 3, 0), (6, 0, 3, 3, 0), (0, 0, 3, 0, 1), (7, 0, 3, 0, 1),
         (5, 0, 1, 1, 1), (0, 0, 1, 3, 1), (7, 0, 1, 3, 1), (6, 0, 1, 3, 1), (0, 0, 3, 1, 1),
         (7, 0, 3, 1, 1), (5, 0, 3, 1, 1), (5, 0, 1, 2, 1), (0, 1, 1, 0, 0), (7, 1, 1, 0, 0),
         (0, 0, 3, 2, 0), (7, 0, 3, 2, 0), (2, 1, 0, 2, 0), (0, 1, 3, 0, 0), (7, 1, 3, 0, 0),
         (0, 1, 3, 2, 0), (6, 1, 3, 2, 0), (7, 1, 3, 2, 0), (6, 1, 1, 0, 0), (0, 0, 3, 3, 1),
         (7, 0, 3, 3, 1),),
        ((0, 1, 2, 0, 0), (7, 1, 2, 0, 0), (0, 0, 2, 0, 0), (7, 0, 2, 0, 0), (6, 1, 1, 1, 0),
         (0, 0, 1, 3, 0), (7, 0, 1, 3, 0),),
        ((0, 1, 3, 3, 0), (7, 1, 3, 3, 0), (6, 1, 3, 0, 0), (0, 1, 3, 2, 1), (7, 1, 3, 2, 1),
         (5, 1, 3, 2, 1), (0, 1, 2, 1, 0), (7, 1, 2, 1, 0), (0, 0, 2, 0, 1), (7, 0, 2, 0, 1),
         (6, 1, 2, 0, 0), (0, 1, 1, 0, 1), (7, 1, 1, 0, 1), (5, 1, 1, 0, 1), (5, 1, 2, 1, 0),
         (0, 1, 1, 2, 0), (7, 1, 1, 2, 0), (0, 1, 1, 1, 1), (7, 1, 1, 1, 1), (5, 1, 1, 1, 1),
         (0, 0, 2, 1, 0), (7, 0, 2, 1, 0), (6, 0, 2, 1, 0), (0, 1, 3, 1, 0), (7, 1, 3, 1, 0),
         (0, 1, 3, 0, 1), (7, 1, 3, 0, 1), (5, 1, 3, 0, 1), (5, 1, 3, 1, 0), (0, 0, 2, 3, 1),
         (7, 0, 2, 3, 1), (6, 0, 2, 3, 1), (0, 1, 2, 0, 1), (7, 1, 2, 0, 1), (5, 1, 2, 0, 0),
         (0, 1, 2, 3, 0), (7, 1, 2, 3, 0), (0, 0, 2, 2, 0), (7, 0, 2, 2, 0), (6, 0, 2, 2, 0),
         (6, 1, 3, 1, 0), (0, 0, 2, 1, 1), (7, 0, 2, 1, 1), (5, 1, 2, 0, 1), (0, 1, 1, 2, 1),
         (7, 1, 1, 2, 1), (6, 1, 3, 3, 0), (0, 0, 2, 3, 0), (7, 0, 2, 3, 0), (0, 1, 1, 3, 0),
         (7, 1, 1, 3, 0), (6, 1, 2, 1, 0), (0, 0, 2, 2, 1), (7, 0, 2, 2, 1),),
        ((0, 1, 1, 3, 1), (7, 1, 1, 3, 1),),
        ((6, 1, 2, 3, 0), (0, 1, 3, 1, 1), (7, 1, 3, 1, 1), (5, 1, 3, 1, 1), (0, 1, 0, 1, 0),
         (7, 1, 0, 1, 0), (6, 1, 0, 0, 1), (0, 1, 3, 3, 1), (7, 1, 3, 3, 1),),
        ((0, 1, 0, 2, 0), (7, 1, 0, 2, 0), (6, 1, 0, 1, 0), (0, 1, 2, 1, 1), (7, 1, 2, 1, 1),
         (0, 1, 2, 2, 0), (7, 1, 2, 2, 0), (6, 1, 0, 2, 0), (0, 1, 2, 3, 1), (7, 1, 2, 3, 1),
         (0, 1, 2, 2, 1), (7, 1, 2, 2, 1),),
        ((0, 1, 0, 0, 0), (7, 1, 0, 0, 0), (0, 1, 0, 3, 0), (7, 1, 0, 3, 0), (0, 1, 0, 1, 1),
         (7, 1, 0, 1, 1), (0, 1, 0, 3, 1), (7, 1, 0, 3, 1), (0, 1, 0, 2, 1), (7, 1, 0, 2, 1),),
        (),
    ),
    (
        ((2, 0, 0, 0, 0), (3, 0, 0, 0, 0),),
        (),
        (),
        (),
        (),
        (),
        (),
        (),
        (),
        ((3, 0, 0, 2, 0),),
        (),
        ((2, 0, 0, 1, 0),),
        (),
        (),
        (),
        (),
        ((3, 0, 0, 3, 0), (2, 1, 0, 2, 0), (3, 1, 0, 0, 0), (2, 1, 0, 1, 0), (3, 1, 0, 3, 0),),
        (),
        (),
        (),
        (),
        (),
        (),
        (),
        (),
    ),
    (
        ((3, 0, 1, 0, 0),),
        ((2, 0, 1, 1, 0),),
        (),
        (),
        (),
        (),
        (),
        (),
        (),
        (),
        (),
        (),
        (),
        (),
        (),
        (),
        ((2, 1, 1, 1, 0), (3, 0, 1, 2, 0),),
        ((3, 0, 1, 3, 0), (1, 0, 1, 0, 0), (4, 0, 1, 0, 0), (3, 1, 1, 0, 0), (3, 0, 1, 1, 0),
         (3, 1, 1, 2, 0), (1, 0, 1, 3, 0), (4, 0, 1, 3, 0), (3, 1, 1, 3, 0), (1, 1, 1, 0, 0),
         (4, 1, 1, 0, 0), (3, 1, 1, 1, 0),),
        ((1, 1, 1, 1, 0), (4, 1, 1, 1, 0),),
        ((1, 1, 1, 2, 0), (4, 1, 1, 2, 0),),
        ((1, 0, 1, 2, 0), (4, 0, 1, 2, 0), (1, 1, 1, 3, 0), (4, 1, 1, 3, 0),),
        (),
        (),
        (),
        (),
    ),
    (
        ((5, 0, 1, 0, 0), (7, 0, 1, 0, 0),),
        (),
        (),
        (),
        (),
        ((7, 0, 1, 0, 1),),
        (),
        (),
        (),
        (),
        ((7, 0, 1, 1, 0),),
        (),
        (),
        (),
        (),
        ((7, 0, 1, 1, 1),),
        ((7, 0, 1, 2, 0), (7, 0, 1, 2, 1), (7, 0, 1, 3, 0), (7, 0, 1, 3, 1), (7, 1, 1, 0, 0),),
        ((7, 1, 1, 0, 1), (0, 0, 0, 0, 0), (5, 0, 0, 0, 0), (7, 0, 0, 0, 0), (7, 1, 1, 1, 0),
         (7, 1, 1, 1, 1), (7, 1, 1, 2, 0), (7, 1, 1, 2, 1), (7, 1, 1, 3, 0), (0, 0, 0, 1, 0),
         (5, 0, 0, 1, 0), (7, 0, 0, 1, 0), (1, 1, 1, 0, 0), (4, 1, 1, 0, 0), (7, 1, 1, 3, 1),
         (0, 0, 3, 2, 0), (6, 0, 3, 2, 0), (7, 0, 3, 2, 0), (0, 0, 0, 3, 0), (7, 0, 0, 3, 0),
         (5, 0, 0, 3, 0), (0, 0, 3, 2, 1), (7, 0, 3, 2, 1), (5, 0, 3, 2, 1), (0, 0, 3, 3, 0),
         (6, 0, 3, 3, 0), (7, 0, 3, 3, 0), (5, 0, 1, 1, 1), (5, 0, 1, 2, 0), (0, 0, 3, 3, 1),
         (7, 0, 3, 3, 1), (0, 1, 3, 2, 0), (6, 1, 3, 2, 0), (7, 1, 3, 2, 0), (5, 0, 1, 2, 1),
         (5, 0, 1, 3, 0), (0, 1, 3, 2, 1), (7, 1, 3, 2, 1), (0, 0, 3, 0, 0), (6, 0, 3, 0, 0),
         (7, 0, 3, 0, 0), (0, 1, 3, 3, 0), (7, 1, 3, 3, 0), (6, 1, 3, 3, 0), (5, 0, 1, 3, 1),
         (0, 0, 0, 2, 0), (7, 0, 0, 2, 0), (6, 0, 0, 2, 0), (0, 0, 3, 0, 1), (7, 0, 3, 0, 1),
         (5, 0, 0, 2, 0), (0, 0, 0, 0, 1), (7, 0, 0, 0, 1), (1, 1, 1, 1, 0), (4, 1, 1, 1, 0),
         (0, 1, 3, 3, 1), (7, 1, 3, 3, 1), (0, 0, 2, 1, 0), (7, 0, 2, 1, 0), (6, 0, 2, 1, 0),
         (0, 0, 0, 2, 1), (7, 0, 0, 2, 1), (5, 0, 0, 2, 1), (0, 0, 3, 1, 1), (6, 0, 3, 1, 1),
         (7, 0, 3, 1, 1), (1, 1, 1, 3, 0), (4, 1, 1, 3, 0), (0, 0, 2, 1, 1), (7, 0, 2, 1, 1),
         (5, 0, 2, 1, 1), (5, 1, 3, 3, 0), (0, 0, 2, 2, 0), (7, 0, 2, 2, 0), (6, 0, 2, 2, 0),
         (0, 1, 0, 1, 0), (7, 1, 0, 1, 0), (0, 0, 3, 1, 0), (7, 0, 3, 1, 0),),
        ((0, 1, 0, 2, 0), (7, 1, 0, 2, 0), (6, 1, 0, 2, 0), (0, 0, 0, 1, 1), (7, 0, 0, 1, 1),
         (0, 0, 2, 2, 1), (7, 0, 2, 2, 1), (5, 0, 2, 2, 1), (5, 1, 0, 1, 0), (0, 0, 2, 3, 0),
         (7, 0, 2, 3, 0), (6, 0, 2, 3, 0), (0, 0, 2, 0, 0), (6, 0, 2, 0, 0), (7, 0, 2, 0, 0),
         (0, 1, 0, 3, 0), (7, 1, 0, 3, 0), (6, 1, 0, 3, 0), (0, 1, 0, 2, 1), (7, 1, 0, 2, 1),
         (5, 1, 3, 2, 1), (0, 0, 0, 3, 1), (7, 0, 0, 3, 1),),
        ((0, 0, 2, 0, 1), (7, 0, 2, 0, 1), (5, 1, 0, 2, 1), (0, 1, 2, 3, 0), (7, 1, 2, 3, 0),
         (0, 1, 3, 0, 1), (6, 1, 3, 0, 1), (7, 1, 3, 0, 1), (0, 0, 2, 3, 1), (7, 0, 2, 3, 1),),
        ((0, 1, 0, 0, 0), (7, 1, 0, 0, 0), (0, 1, 3, 1, 1), (6, 1, 3, 1, 1), (7, 1, 3, 1, 1),
         (6, 1, 0, 0, 0), (0, 1, 0, 3, 1), (7, 1, 0, 3, 1), (5, 1, 0, 3, 1), (5, 1, 1, 0, 0),
         (0, 1, 3, 0, 0), (7, 1, 3, 0, 0), (0, 1, 2, 0, 0), (6, 1, 2, 0, 0), (7, 1, 2, 0, 0),
         (5, 1, 1, 1, 1), (0, 1, 3, 1, 0), (7, 1, 3, 1, 0),),
        ((5, 1, 1, 3, 0), (0, 1, 2, 1, 0), (7, 1, 2, 1, 0), (6, 1, 2, 1, 0), (6, 1, 2, 3, 0),
         (0, 1, 0, 0, 1), (7, 1, 0, 0, 1), (5, 1, 0, 0, 0), (0, 1, 0, 1, 1), (7, 1, 0, 1, 1),),
        ((0, 1, 2, 0, 1), (7, 1, 2, 0, 1), (5, 1, 0, 0, 1), (0, 1, 2, 2, 0), (7, 1, 2, 2, 0),
         (0, 1, 2, 1, 1), (7, 1, 2, 1, 1), (5, 1, 1, 2, 0), (0, 1, 2, 2, 1), (7, 1, 2, 2, 1),
         (0, 1, 2, 3, 1), (7, 1, 2, 3, 1),),
        ((5, 1, 1, 2, 1),),
        (),
    ),
    (
        ((2, 0, 1, 0, 0),),
        ((3, 0, 1, 1, 0),),
        (),
        ((2, 0, 1, 3, 0),),
        (),
        (),
        (),
        (),
        (),
        (),
        (),
        (),
        (),
        (),
        (),
        (),
        ((2, 1, 1, 0, 0), (1, 0, 1, 1, 0), (4, 0, 1, 1, 0), (2, 1, 1, 1, 0), (1, 1, 1, 1, 0),
         (4, 1, 1, 1, 0), (2, 1, 1, 2, 0), (2, 0, 1, 2, 0), (3, 0, 1, 2, 0), (2, 1, 1, 3, 0),
         (3, 0, 1, 3, 0),),
        ((3, 1, 1, 3, 0),),
        (),
        (),
        (),
        (),
        (),
        (),
        (),
    ),
    (
        ((3, 0, 1, 0, 0),),
        (),
        (),
        (),
        (),
        (),
        (),
        (),
        ((2, 1, 1, 0, 0),),
        (),
        (),
        (),
        (),
        (),
        (),
        (),
        ((2, 1, 1, 1, 0), (2, 1, 1, 3, 0), (0, 0, 1, 0, 0), (6, 0, 1, 0, 0), (7, 0, 1, 0, 0),
         (0, 0, 1, 0, 1), (7, 0, 1, 0, 1), (0, 0, 0, 0, 0), (6, 0, 0, 0, 0), (7, 0, 0, 0, 0),
         (0, 0, 3, 0, 0), (7, 0, 3, 0, 0), (6, 0, 3, 0, 0), (5, 0, 3, 0, 0), (0, 0, 0, 1, 0),
         (7, 0, 0, 1, 0), (6, 0, 0, 1, 0), (0, 0, 0, 0, 1), (7, 0, 0, 0, 1), (5, 0, 0, 0, 1),
         (0, 0, 3, 2, 1), (7, 0, 3, 2, 1), (6, 0, 3, 2, 1), (0, 0, 3, 0, 1), (7, 0, 3, 0, 1),
         (0, 0, 3, 1, 0), (7, 0, 3, 1, 0), (6, 0, 3, 1, 0), (0, 0, 0, 3, 0), (7, 0, 0, 3, 0),
         (0, 0, 0, 1, 1), (7, 0, 0, 1, 1), (0, 0, 1, 1, 1), (7, 0, 1, 1, 1), (6, 0, 0, 3, 0),
         (0, 0, 3, 1, 1), (7, 0, 3, 1, 1), (5, 0, 3, 1, 1), (0, 0, 3, 3, 0), (7, 0, 3, 3, 0),
         (6, 0, 3, 3, 0), (3, 0, 1, 3, 0), (0, 0, 1, 2, 0), (7, 0, 1, 2, 0), (6, 0, 1, 1, 1),
         (0, 0, 3, 2, 0), (7, 0, 3, 2, 0), (5, 0, 0, 1, 1), (0, 0, 1, 2, 1), (7, 0, 1, 2, 1),
         (0, 0, 3, 3, 1), (7, 0, 3, 3, 1),),
        ((0, 1, 3, 0, 0), (7, 1, 3, 0, 0), (6, 1, 3, 0, 0), (3, 0, 1, 1, 0), (0, 0, 1, 3, 0),
         (7, 0, 1, 3, 0), (0, 0, 0, 3, 1), (7, 0, 0, 3, 1), (0, 0, 2, 0, 0), (7, 0, 2, 0, 0),
         (5, 0, 2, 0, 0), (0, 0, 1, 3, 1), (7, 0, 1, 3, 1), (6, 0, 2, 0, 0), (0, 0, 1, 1, 0),
         (7, 0, 1, 1, 0),),
        ((0, 1, 3, 1, 0), (7, 1, 3, 1, 0), (6, 1, 3, 1, 0), (3, 0, 1, 2, 0), (5, 0, 0, 3, 1),
         (0, 0, 0, 2, 0), (7, 0, 0, 2, 0), (0, 1, 3, 0, 1), (7, 1, 3, 0, 1), (5, 1, 3, 0, 1),
         (0, 0, 0, 2, 1), (7, 0, 0, 2, 1),),
        ((0, 0, 2, 3, 0), (6, 0, 2, 3, 0), (7, 0, 2, 3, 0), (0, 1, 3, 1, 1), (7, 1, 3, 1, 1),
         (3, 1, 1, 2, 0), (5, 1, 3, 1, 1), (0, 0, 2, 1, 1), (7, 0, 2, 1, 1), (6, 0, 2, 1, 1),
         (0, 0, 2, 0, 1), (7, 0, 2, 0, 1), (3, 1, 1, 3, 0), (0, 1, 3, 3, 0), (7, 1, 3, 3, 0),
         (6, 1, 3, 3, 0), (0, 0, 2, 3, 1), (7, 0, 2, 3, 1), (0, 0, 2, 2, 1), (7, 0, 2, 2, 1),
         (0, 0, 2, 1, 0), (7, 0, 2, 1, 0), (0, 1, 3, 2, 0), (7, 1, 3, 2, 0), (0, 1, 0, 1, 0),
         (6, 1, 0, 1, 0), (7, 1, 0, 1, 0), (0, 1, 2, 0, 0), (5, 1, 2, 0, 0), (6, 1, 2, 0, 0),
         (7, 1, 2, 0, 0), (0, 1, 3, 3, 1), (7, 1, 3, 3, 1), (0, 1, 3, 2, 1), (7, 1, 3, 2, 1),
         (0, 1, 2, 1, 0), (5, 1, 2, 1, 0), (7, 1, 2, 1, 0), (6, 1, 2, 1, 0), (0, 1, 0, 1, 1),
         (5, 1, 0, 1, 1), (7, 1, 0, 1, 1), (0, 1, 0, 2, 1), (7, 1, 0, 2, 1), (6, 1, 0, 2, 1),
         (0, 1, 2, 2, 0), (7, 1, 2, 2, 0), (6, 1, 2, 2, 0), (5, 1, 2, 2, 0), (0, 1, 2, 0, 1),
         (7, 1, 2, 0, 1), (0, 1, 0, 3, 1), (7, 1, 0, 3, 1), (0, 0, 2, 2, 0), (7, 0, 2, 2, 0),),
        ((0, 1, 2, 1, 1), (7, 1, 2, 1, 1),),
        ((0, 1, 1, 0, 0), (7, 1, 1, 0, 0), (6, 1, 0, 3, 1), (0, 1, 2, 3, 0), (7, 1, 2, 3, 0),
         (6, 1, 2, 3, 0), (0, 1, 2, 2, 1), (5, 1, 2, 2, 1), (7, 1, 2, 2, 1), (0, 1, 1, 1, 1),
         (7, 1, 1, 1, 1), (6, 1, 1, 0, 0), (0, 1, 0, 2, 0), (7, 1, 0, 2, 0), (0, 1, 1, 3, 0),
         (7, 1, 1, 3, 0), (6, 1, 1, 1, 1), (0, 1, 2, 3, 1), (7, 1, 2, 3, 1),),
        ((0, 1, 0, 0, 0), (7, 1, 0, 0, 0), (6, 1, 1, 3, 0), (0, 1, 0, 3, 0), (7, 1, 0, 3, 0),
         (0, 1, 0, 0, 1), (7, 1, 0, 0, 1),),
        ((0, 1, 1, 0, 1), (7, 1, 1, 0, 1), (0, 1, 1, 2, 0), (7, 1, 1, 2, 0), (0, 1, 1, 1, 0),
         (7, 1, 1, 1, 0), (0, 1, 1, 2, 1), (7, 1, 1, 2, 1), (0, 1, 1, 3, 1), (7, 1, 1, 3, 1),),
        (),
    ),
)


def local_plain(tokens, norm_gain, up_trained, down_trained):
    shards = lax.axis_size("fs")
    groups = lax.axis_size("tp")
    rows_local = up_trained.shape[0]
    cols_local = up_trained.shape[1]
    folded = (norm_gain[:, None] * up_trained).astype(jnp.bfloat16)
    stacked = jnp.stack([folded, down_trained.astype(jnp.bfloat16)])
    served_width = cols_local * groups // shards
    blocks_here = cols_local // served_width
    quarter_rows = rows_local // groups
    pieces = stacked.reshape(2, groups, quarter_rows, blocks_here, served_width)
    moved = lax.all_to_all(pieces, "tp", split_axis=1, concat_axis=3, tiled=True)
    placed = lax.all_to_all(moved, "fs", split_axis=3, concat_axis=2, tiled=True)
    ordered = placed.reshape(2, shards, quarter_rows, served_width)
    joined = lax.all_gather(ordered, "tp", axis=2, tiled=True)
    owned = joined.reshape(2, rows_local * shards, served_width)
    up_serving = owned[0]
    down_serving = owned[1]
    values = tokens.astype(jnp.float32)
    scale = lax.rsqrt(jnp.mean(values * values, axis=1, keepdims=True) + epsilon)
    normed = (values * scale).astype(jnp.bfloat16)
    hidden = jnp.dot(normed, up_serving, preferred_element_type=jnp.float32)
    active = jnp.square(jax.nn.relu(hidden)).astype(jnp.bfloat16)
    summed = lax.psum_scatter(
        lax.dot_general(
            down_serving, active, (((1,), (1,)), ((), ())), preferred_element_type=jnp.float32
        ),
        "fs",
        scatter_dimension=0,
        tiled=True,
    )
    prompt_output = summed.T.astype(jnp.bfloat16)
    return (up_serving, down_serving, prompt_output)


def down_block(active, whole, plane, put):
    rows_local = whole.shape[1] // 4
    tile = 256 if rows_local % 256 == 0 else rows_local

    @pl.loop(0, rows_local // tile)
    def _(n):
        rows = pl.ds(pl.multiple_of(plane * rows_local + n * tile, tile), tile)
        product = lax.dot_general(
            active[...], whole[1, rows, :], (((1,), (1,)), ((), ())),
            preferred_element_type=jnp.float32,
        )
        put(pl.ds(pl.multiple_of(n * tile, tile), tile), product)


def kernel(
    tokens_hbm, gain_hbm, up_hbm, down_hbm, whole, active, rs_recv,
    raw, gain_rows, gain, cast, relay, toks, normed, hidden, rs_send,
    in_sem, misc_sem, got_sem, relay_sem, block_sem, src_sem, out_sem, rs_ssem, rs_rsem,
):
    y = lax.axis_index("grp")
    z = lax.axis_index("fs")
    t = lax.axis_index("tp")
    mirrored = z // 2
    role = jnp.where(mirrored == 1, 4 * (3 - z) + (3 - t), 4 * z + t)
    is_own = z == t
    is_active = t % 2 == z % 2
    t_x = jnp.where(t < 2, t + 2, t - 2)
    t_c = t + 1 - 2 * (t % 2)
    to_x = {"tp": t_x}
    to_c = {"tp": t_c}
    to_y = {"grp": 1 - y}
    rows_local, width = cast.shape[1], cast.shape[2]
    size = rows_local // (2 * PAIRS)
    trained = (up_hbm, down_hbm)
    planes = [jnp.where(mirrored == 1, 3 - k, k) for k in range(4)]
    sides = [y, 1 - y]

    def part(pair, side):
        return 2 * pair + sides[side]

    def ds(start, extent):
        return pl.ds(pl.multiple_of(start, extent), extent)

    def local_rows(pair, side):
        return ds(part(pair, side) * size, size)

    def unit(m, plane, pair, side):
        return whole.at[m, ds(plane * rows_local + part(pair, side) * size, size)]

    def remote(src, dst, ssem, rsem, where):
        return pltpu.make_async_remote_copy(
            src_ref=src, dst_ref=dst, send_sem=ssem, recv_sem=rsem,
            device_id=where, device_id_type=MESH,
        )

    def fetch(m, pair, side):
        rows = local_rows(pair, side)
        return pltpu.make_async_copy(
            trained[m].at[rows], raw.at[m, rows], in_sem.at[m, 2 * pair + side]
        )

    get_gain = pltpu.make_async_copy(gain_hbm, gain_rows, misc_sem.at[0])
    get_toks = pltpu.make_async_copy(tokens_hbm, toks, misc_sem.at[1])
    get_gain.start()
    for pair in range(PAIRS):
        fetch(0, pair, 0).start()

    barrier = pltpu.get_barrier_semaphore()
    others = [{"fs": lax.rem(z + k, 4)} for k in range(1, 4)]
    for where in [to_x, to_c, to_y] + others:
        pl.semaphore_signal(barrier, inc=1, device_id=where, device_id_type=MESH)

    get_gain.wait()
    lanes = gain_rows.shape[1]
    for q in range(gain_rows.shape[0]):
        square = (lanes, lanes)
        chosen = jnp.where(
            lax.broadcasted_iota(jnp.int32, square, 0) == lax.broadcasted_iota(jnp.int32, square, 1),
            jnp.broadcast_to(gain_rows[pl.ds(q, 1), :], square), 0.0,
        )
        column = jnp.sum(chosen, axis=1, keepdims=True)
        gain[pl.ds(q * lanes, lanes), :] = jnp.broadcast_to(column, square)

    piece = 16

    def cast_unit(m, pair, side):
        fetch(m, pair, side).wait()
        base = part(pair, side) * size

        def store(into, shift):
            @pl.loop(0, size // piece)
            def _(i):
                here = ds(base + i * piece, piece)
                there = ds(shift + base + i * piece, piece)
                if m == 0:
                    factor = gain[here, :]
                    for j in range(width // lanes):
                        cols = pl.ds(j * lanes, lanes)
                        into[0, there, cols] = (raw[0, here, cols] * factor).astype(jnp.bfloat16)
                else:
                    into[m, there, :] = raw[m, here, :].astype(jnp.bfloat16)

        @pl.when(is_own)
        def _():
            store(whole, z * rows_local)

        if side == 0:
            @pl.when(jnp.logical_not(is_own))
            def _():
                store(cast, 0)

    def step(kind, m, k, pair, side):
        plane = planes[k]
        place = part(pair, side)
        if kind == GET:
            here = unit(m, plane, pair, side)
            remote(here, here, out_sem.at[0, m], got_sem.at[m, plane, place], to_x).wait_recv()
        elif kind == GET_RELAY:
            here = relay.at[m, ds(place * size, size)]
            remote(here, here, src_sem.at[m], relay_sem.at[m, place], to_x).wait_recv()
        elif kind == SWAP:
            remote(
                cast.at[m, local_rows(pair, side)], relay.at[m, ds(place * size, size)],
                src_sem.at[m], relay_sem.at[m, place], to_x,
            ).start()
        elif kind in (HOP, HOP_RELAY):
            src = (cast if kind == HOP else relay).at[m, ds(place * size, size)]
            remote(
                src, unit(m, z, pair, side), src_sem.at[m], got_sem.at[m, z, place],
                {"fs": t if kind == HOP else t_x},
            ).start()
        elif kind == SEND_CORE:
            here = unit(m, plane, pair, side)
            remote(here, here, out_sem.at[2, m], block_sem.at[m, plane], to_c).start()
        else:
            here = unit(m, plane, pair, side)
            i = kind - SEND_X
            remote(
                here, here, out_sem.at[i, m], got_sem.at[m, plane, place], (to_x, to_y)[i]
            ).start()

    def run(segment):
        for r in range(8):
            if SCHEDULE[r][segment]:
                @pl.when(role == r)
                def _():
                    for s in SCHEDULE[r][segment]:
                        step(*s)

    casts = [(m, pair, side) for m in range(2) for side in range(2) for pair in range(PAIRS)]
    segment = 0
    for m, pair, side in casts:
        if side == 1:
            pl.when(is_own)(lambda: cast_unit(m, pair, side))
        else:
            cast_unit(m, pair, side)
        if segment == 0:
            @pl.when(is_own)
            def _():
                for p in range(PAIRS):
                    fetch(0, p, 1).start()
            for p in range(PAIRS):
                fetch(1, p, 0).start()
            @pl.when(is_own)
            def _():
                for p in range(PAIRS):
                    fetch(1, p, 1).start()
            get_toks.start()
            pl.semaphore_wait(barrier, 6)
        run(segment)
        segment += 1

    get_toks.wait()
    tokens_here = toks.shape[0]

    @pl.loop(0, tokens_here // piece)
    def _(i):
        here = ds(i * piece, piece)
        values = toks[here, :].astype(jnp.float32)
        scale = lax.rsqrt(jnp.mean(values * values, axis=1, keepdims=True) + epsilon)
        normed[here, :] = (values * scale).astype(jnp.bfloat16)

    def pick(table):
        chosen = planes[table[0]]
        for r in range(1, 8):
            if table[r] != table[0]:
                chosen = jnp.where(role == r, planes[table[r]], chosen)
        return chosen

    def listen(m, plane):
        @pl.when(jnp.logical_not(is_active))
        def _():
            here = whole.at[m, ds(plane * rows_local, rows_local)]
            remote(here, here, out_sem.at[2, m], block_sem.at[m, plane], to_c).wait_recv()

    tile = 512 if width % 512 == 0 else width

    def compute_up(k):
        plane = pick(ORDER[0][k])
        listen(0, plane)
        rows = ds(plane * rows_local, rows_local)

        @pl.loop(0, width // tile)
        def _(n):
            cols = ds(n * tile, tile)
            product = jnp.dot(
                normed[:, rows], whole[0, rows, cols], preferred_element_type=jnp.float32
            )
            if k > 0:
                product = product + hidden[:, cols]
            if k < 3:
                hidden[:, cols] = product
            else:
                active[:, cols] = jnp.square(jnp.maximum(product, 0.0)).astype(jnp.bfloat16)

    def scatter(k, plane):
        slot = lax.rem(z - plane + 3, 4)
        return remote(
            rs_send.at[k], rs_recv.at[slot], rs_ssem.at[k], rs_rsem.at[slot], {"fs": plane}
        )

    def compute_down(k):
        plane = pick(ORDER[1][k])
        listen(1, plane)

        down_block(
            active, whole, plane,
            lambda cols, product: rs_send.__setitem__((k, slice(None), cols), product.astype(jnp.bfloat16)),
        )
        scatter(k, plane).start()

    for m in range(2):
        for k in range(4):
            run(segment)
            segment += 1
            if m == 0:
                compute_up(k)
            elif k < 3:
                compute_down(k)
            else:
                listen(1, z)
    run(segment)

    for k in range(3):
        here = rs_recv.at[k]
        remote(here, here, rs_ssem.at[k], rs_rsem.at[k], {"fs": lax.rem(z + 1, 4)}).wait_recv()

    def drain(sem, m, count):
        sent = whole.at[m, pl.ds(0, count * size)]
        remote(sent, sent, sem, got_sem.at[0, 0, 0], to_x).wait_send()

    for r in range(8):
        @pl.when(role == r)
        def _():
            for m in range(2):
                steps = [s for part_of in SCHEDULE[r] for s in part_of if s[1] == m]
                hops = sum(s[0] in (SWAP, HOP, HOP_RELAY) for s in steps)
                if hops:
                    drain(src_sem.at[m], m, hops)
                for i, kind in enumerate((SEND_X, SEND_Y, SEND_CORE)):
                    sends = sum(s[0] == kind for s in steps)
                    if sends:
                        drain(out_sem.at[i, m], m, sends)
    for k in range(3):
        here = rs_send.at[k]
        remote(here, here, rs_ssem.at[k], rs_rsem.at[k], {"fs": lax.rem(z + 1, 4)}).wait_send()


pieces_out = 8


def deliver(whole, active, rs_recv, up_out, down_out, prompt_out, own, prompt, sems, last):
    rows = whole.shape[1] // pieces_out
    copies = [
        pltpu.make_async_copy(
            whole.at[m, pl.ds(i * rows, rows)], out.at[pl.ds(i * rows, rows)], sems.at[m, i]
        )
        for m, out in enumerate((up_out, down_out))
        for i in range(pieces_out)
    ]
    for copy in copies:
        copy.start()
    down_block(
        active, whole, lax.axis_index("fs"),
        lambda cols, product: own.__setitem__((slice(None), cols), product),
    )
    piece = 16

    @pl.loop(0, own.shape[0] // piece)
    def _(i):
        here = pl.ds(pl.multiple_of(i * piece, piece), piece)
        total = own[here, :]
        for k in range(3):
            total = total + rs_recv[k, here, :].astype(jnp.float32)
        prompt[here, :] = total.astype(prompt.dtype)

    copies.append(pltpu.make_async_copy(prompt, prompt_out, last))
    copies[-1].start()
    for copy in copies:
        copy.wait()


def local_kernel(tokens, norm_gain, up_trained, down_trained):
    shards = lax.axis_size("fs")
    rows_local, width = up_trained.shape
    tokens_here, features = tokens.shape
    any_space = pl.BlockSpec(memory_space=pl.ANY)
    dma = pltpu.SemaphoreType.DMA
    bf16, f32 = jnp.bfloat16, jnp.float32
    results = pl.pallas_call(
        kernel,
        out_shape=(
            pltpu.VMEM((2, rows_local * shards, width), bf16),
            pltpu.VMEM((tokens_here, width), bf16),
            pltpu.VMEM((3, tokens_here, rows_local), bf16),
        ),
        in_specs=[any_space] * 4,
        out_specs=(pl.BlockSpec(memory_space=pltpu.VMEM),) * 3,
        scratch_shapes=[
            pltpu.VMEM((2, rows_local, width), f32),
            pltpu.VMEM((rows_local // 128, 128), f32),
            pltpu.VMEM((rows_local, 128), f32),
            pltpu.VMEM((2, rows_local, width), bf16),
            pltpu.VMEM((2, rows_local, width), bf16),
            pltpu.VMEM((tokens_here, features), bf16),
            pltpu.VMEM((tokens_here, features), bf16),
            pltpu.VMEM((tokens_here, width), f32),
            pltpu.VMEM((3, tokens_here, rows_local), bf16),
            dma((2, 2 * PAIRS)), dma((2,)),
            dma((2, 4, 2 * PAIRS)), dma((2, 2 * PAIRS)), dma((2, 4)),
            dma((2,)), dma((3, 2)), dma((3,)), dma((3,)),
        ],
        compiler_params=pltpu.CompilerParams(
            collective_id=0, has_side_effects=True, vmem_limit_bytes=40 * 1024 * 1024
        ),
    )(tokens, norm_gain.reshape(rows_local // 128, 128), up_trained, down_trained)
    held = pl.BlockSpec(memory_space=pltpu.VMEM)
    return tuple(pl.pallas_call(
        deliver,
        out_shape=(
            jax.ShapeDtypeStruct((rows_local * shards, width), bf16),
            jax.ShapeDtypeStruct((rows_local * shards, width), bf16),
            jax.ShapeDtypeStruct((tokens_here, rows_local), bf16),
        ),
        in_specs=[held] * 3,
        out_specs=(any_space,) * 3,
        scratch_shapes=[
            pltpu.VMEM((tokens_here, rows_local), f32), pltpu.VMEM((tokens_here, rows_local), bf16),
            dma((2, pieces_out)), dma(()),
        ],
        compiler_params=pltpu.CompilerParams(vmem_limit_bytes=8 * 1024 * 1024),
    )(*results))


def solution(mesh):
    in_specs = (P(("grp", "tp"), None), P("fs"), P("fs", "tp"), P("fs", "tp"))
    out_specs = (P("grp", "fs"), P("grp", "fs"), P(("grp", "tp"), "fs"))
    sizes = mesh.shape
    square = sizes["grp"] == 2 and sizes["fs"] == 4 and sizes["tp"] == 4
    local = local_kernel if square else local_plain
    return jax.shard_map(local, mesh=mesh, in_specs=in_specs, out_specs=out_specs, check_vma=False)
```

```python
import jax
import jax.numpy as jnp
from jax import lax
from jax.experimental import pallas as pl
from jax.experimental.pallas import tpu as pltpu
from jax.sharding import PartitionSpec as P

epsilon = 1e-06
MESH = pl.DeviceIdType.MESH

GET, GET_RELAY, SWAP, HOP, HOP_RELAY, SEND_X, SEND_Y, SEND_CORE = range(8)
PAIRS = 4
ORDER = (
    (
        (0, 0, 0, 0, 1, 1, 3, 3),
        (3, 3, 3, 3, 3, 3, 1, 1),
        (1, 1, 1, 1, 0, 0, 0, 0),
        (2, 2, 2, 2, 2, 2, 2, 2),
    ),
    (
        (1, 1, 1, 1, 3, 3, 3, 3),
        (2, 2, 3, 3, 0, 0, 2, 2),
        (3, 3, 2, 2, 2, 2, 0, 0),
        (0, 0, 0, 0, 1, 1, 1, 1),
    ),
)
SCHEDULE = (
    (
        ((5, 0, 0, 0, 0), (7, 0, 0, 0, 0),),
        ((5, 0, 0, 1, 0),),
        (),
        (),
        (),
        ((7, 0, 0, 0, 1),),
        (),
        ((5, 0, 0, 2, 0),),
        (),
        (),
        ((7, 0, 0, 1, 0),),
        (),
        (),
        (),
        (),
        ((7, 0, 0, 1, 1),),
        ((7, 0, 0, 2, 0), (7, 0, 0, 2, 1), (7, 0, 0, 3, 0), (7, 0, 0, 3, 1), (7, 1, 0, 0, 0),),
        ((7, 1, 0, 0, 1), (7, 1, 0, 1, 0), (7, 1, 0, 1, 1), (7, 1, 0, 2, 0), (7, 1, 0, 2, 1),
         (7, 1, 0, 3, 0), (5, 0, 0, 3, 0), (7, 1, 0, 3, 1), (1, 0, 0, 0, 0), (4, 0, 0, 0, 0),
         (0, 0, 1, 0, 0), (7, 0, 1, 0, 0), (5, 0, 1, 0, 0), (0, 0, 3, 0, 0), (6, 0, 3, 0, 0),
         (7, 0, 3, 0, 0), (5, 1, 0, 0, 1), (0, 0, 3, 0, 1), (7, 0, 3, 0, 1), (1, 0, 0, 1, 0),
         (4, 0, 0, 1, 0), (0, 0, 1, 2, 0), (7, 0, 1, 2, 0), (5, 0, 1, 2, 0), (0, 0, 3, 2, 0),
         (6, 0, 3, 2, 0), (7, 0, 3, 2, 0), (0, 0, 3, 2, 1), (7, 0, 3, 2, 1), (5, 0, 3, 2, 1),
         (1, 0, 0, 3, 0), (4, 0, 0, 3, 0), (0, 0, 1, 3, 0), (6, 0, 1, 3, 0), (7, 0, 1, 3, 0),
         (0, 0, 3, 3, 0), (7, 0, 3, 3, 0), (6, 0, 3, 3, 0), (5, 0, 3, 3, 0), (0, 0, 1, 3, 1),
         (7, 0, 1, 3, 1), (5, 0, 1, 3, 1), (1, 1, 0, 0, 0), (4, 1, 0, 0, 0), (0, 1, 3, 0, 0),
         (7, 1, 3, 0, 0), (0, 0, 3, 3, 1), (7, 0, 3, 3, 1), (5, 1, 3, 0, 0), (1, 1, 0, 1, 0),
         (4, 1, 0, 1, 0), (0, 1, 1, 0, 0), (7, 1, 1, 0, 0), (5, 1, 1, 0, 0), (0, 1, 3, 3, 0),
         (6, 1, 3, 3, 0), (7, 1, 3, 3, 0), (0, 0, 3, 1, 0), (7, 0, 3, 1, 0), (5, 1, 3, 3, 0),
         (0, 1, 3, 3, 1), (7, 1, 3, 3, 1), (0, 0, 1, 0, 1), (7, 0, 1, 0, 1), (0, 0, 2, 0, 0),
         (6, 0, 2, 0, 0), (5, 0, 2, 0, 0), (0, 0, 1, 1, 0), (7, 0, 1, 1, 0), (7, 0, 2, 0, 0),
         (0, 0, 3, 1, 1), (7, 0, 3, 1, 1),),
        ((0, 0, 2, 0, 1), (7, 0, 2, 0, 1), (5, 0, 2, 0, 1), (0, 0, 1, 1, 1), (7, 0, 1, 1, 1),
         (0, 1, 1, 2, 0), (6, 1, 1, 2, 0), (5, 1, 1, 2, 0), (7, 1, 1, 2, 0), (0, 0, 2, 3, 0),
         (6, 0, 2, 3, 0), (7, 0, 2, 3, 0), (0, 0, 1, 2, 1), (7, 0, 1, 2, 1),),
        ((0, 1, 1, 2, 1), (7, 1, 1, 2, 1), (1, 1, 0, 2, 0), (4, 1, 0, 2, 0), (0, 1, 1, 3, 0),
         (6, 1, 1, 3, 0), (7, 1, 1, 3, 0), (0, 0, 2, 1, 0), (7, 0, 2, 1, 0), (5, 0, 2, 1, 0),
         (6, 0, 2, 1, 0), (0, 0, 2, 3, 1), (7, 0, 2, 3, 1), (5, 0, 2, 3, 1), (0, 1, 3, 2, 1),
         (7, 1, 3, 2, 1), (6, 1, 3, 2, 1), (0, 1, 1, 3, 1), (7, 1, 1, 3, 1), (5, 1, 1, 2, 1),
         (0, 1, 1, 0, 1), (7, 1, 1, 0, 1), (0, 0, 2, 2, 0), (7, 0, 2, 2, 0), (5, 0, 2, 2, 0),
         (6, 0, 2, 2, 0), (0, 0, 2, 1, 1), (7, 0, 2, 1, 1), (5, 1, 1, 3, 0), (0, 1, 1, 1, 1),
         (7, 1, 1, 1, 1), (0, 1, 2, 2, 0), (7, 1, 2, 2, 0), (6, 1, 2, 2, 0), (0, 1, 3, 2, 0),
         (7, 1, 3, 2, 0), (5, 1, 1, 3, 1), (0, 1, 1, 1, 0), (7, 1, 1, 1, 0), (0, 1, 2, 1, 0),
         (6, 1, 2, 1, 0), (7, 1, 2, 1, 0), (0, 1, 2, 3, 0), (6, 1, 2, 3, 0), (7, 1, 2, 3, 0),
         (0, 0, 2, 2, 1), (7, 0, 2, 2, 1),),
        ((5, 1, 0, 1, 0),),
        ((0, 1, 3, 0, 1), (7, 1, 3, 0, 1), (0, 1, 2, 2, 1), (7, 1, 2, 2, 1), (5, 1, 0, 2, 0),
         (0, 1, 3, 1, 0), (7, 1, 3, 1, 0), (0, 1, 2, 1, 1), (7, 1, 2, 1, 1), (5, 1, 2, 2, 0),
         (0, 1, 2, 0, 0), (7, 1, 2, 0, 0), (0, 1, 2, 3, 1), (7, 1, 2, 3, 1), (5, 1, 2, 2, 1),
         (0, 1, 2, 0, 1), (7, 1, 2, 0, 1),),
        ((5, 1, 0, 3, 0), (0, 1, 3, 1, 1), (7, 1, 3, 1, 1),),
        (),
        ((5, 1, 0, 3, 1),),
    ),
    (
        ((3, 0, 0, 0, 0),),
        ((3, 0, 0, 1, 0),),
        (),
        (),
        (),
        (),
        (),
        (),
        (),
        (),
        (),
        ((3, 0, 0, 3, 0),),
        (),
        (),
        (),
        (),
        (),
        ((1, 0, 0, 0, 0), (4, 0, 0, 0, 0), (1, 0, 0, 1, 0), (4, 0, 0, 1, 0), (3, 0, 0, 2, 0),
         (1, 1, 0, 2, 0), (4, 1, 0, 2, 0), (3, 1, 0, 1, 0), (3, 1, 0, 2, 0), (3, 1, 0, 3, 0),),
        ((1, 1, 0, 1, 0), (4, 1, 0, 1, 0), (3, 1, 0, 0, 0),),
        (),
        (),
        (),
        (),
        (),
        (),
    ),
    (
        ((2, 0, 0, 0, 0),),
        (),
        ((3, 0, 0, 2, 0),),
        (),
        (),
        (),
        (),
        (),
        (),
        (),
        (),
        ((2, 0, 0, 1, 0),),
        (),
        (),
        (),
        (),
        ((3, 0, 0, 3, 0), (0, 0, 0, 0, 0), (6, 0, 0, 0, 0), (7, 0, 0, 0, 0), (2, 0, 0, 3, 0),
         (3, 1, 0, 2, 0), (0, 0, 0, 1, 0), (6, 0, 0, 1, 0), (7, 0, 0, 1, 0), (0, 0, 0, 0, 1),
         (7, 0, 0, 0, 1), (0, 0, 0, 2, 0), (6, 0, 0, 2, 0), (7, 0, 0, 2, 0), (0, 0, 0, 1, 1),
         (7, 0, 0, 1, 1), (2, 1, 0, 0, 0), (3, 1, 0, 3, 0), (0, 0, 1, 1, 0), (7, 0, 1, 1, 0),
         (6, 0, 1, 1, 0), (0, 0, 1, 0, 0), (6, 0, 1, 0, 0), (7, 0, 1, 0, 0), (0, 0, 0, 2, 1),
         (7, 0, 0, 2, 1), (0, 0, 0, 3, 0), (7, 0, 0, 3, 0), (6, 0, 0, 3, 0), (0, 0, 1, 1, 1),
         (7, 0, 1, 1, 1), (2, 1, 0, 1, 0), (0, 0, 1, 2, 0), (7, 0, 1, 2, 0), (6, 0, 1, 2, 0),
         (0, 0, 3, 0, 0), (7, 0, 3, 0, 0), (6, 0, 3, 0, 0), (0, 0, 1, 0, 1), (7, 0, 1, 0, 1),
         (0, 1, 1, 1, 0), (7, 1, 1, 1, 0), (0, 1, 0, 0, 1), (7, 1, 0, 0, 1), (0, 0, 0, 3, 1),
         (7, 0, 0, 3, 1),),
        ((5, 0, 1, 0, 1), (0, 0, 3, 2, 1), (7, 0, 3, 2, 1), (0, 0, 3, 1, 0), (5, 0, 3, 1, 0),
         (6, 0, 3, 1, 0), (7, 0, 3, 1, 0), (6, 0, 3, 2, 1), (0, 0, 1, 2, 1), (7, 0, 1, 2, 1),
         (0, 0, 3, 3, 0), (7, 0, 3, 3, 0), (6, 0, 3, 3, 0), (0, 0, 3, 0, 1), (7, 0, 3, 0, 1),
         (5, 0, 1, 1, 1), (0, 0, 1, 3, 1), (7, 0, 1, 3, 1), (6, 0, 1, 3, 1), (0, 0, 3, 1, 1),
         (7, 0, 3, 1, 1), (5, 0, 3, 1, 1), (5, 0, 1, 2, 1), (0, 1, 1, 0, 0), (7, 1, 1, 0, 0),
         (0, 0, 3, 2, 0), (7, 0, 3, 2, 0), (2, 1, 0, 2, 0), (0, 1, 3, 0, 0), (7, 1, 3, 0, 0),
         (0, 1, 3, 2, 0), (6, 1, 3, 2, 0), (7, 1, 3, 2, 0), (6, 1, 1, 0, 0), (0, 0, 3, 3, 1),
         (7, 0, 3, 3, 1),),
        ((0, 1, 2, 0, 0), (7, 1, 2, 0, 0), (0, 0, 2, 0, 0), (7, 0, 2, 0, 0), (6, 1, 1, 1, 0),
         (0, 0, 1, 3, 0), (7, 0, 1, 3, 0),),
        ((0, 1, 3, 3, 0), (7, 1, 3, 3, 0), (6, 1, 3, 0, 0), (0, 1, 3, 2, 1), (7, 1, 3, 2, 1),
         (5, 1, 3, 2, 1), (0, 1, 2, 1, 0), (7, 1, 2, 1, 0), (0, 0, 2, 0, 1), (7, 0, 2, 0, 1),
         (6, 1, 2, 0, 0), (0, 1, 1, 0, 1), (7, 1, 1, 0, 1), (5, 1, 1, 0, 1), (5, 1, 2, 1, 0),
         (0, 1, 1, 2, 0), (7, 1, 1, 2, 0), (0, 1, 1, 1, 1), (7, 1, 1, 1, 1), (5, 1, 1, 1, 1),
         (0, 0, 2, 1, 0), (7, 0, 2, 1, 0), (6, 0, 2, 1, 0), (0, 1, 3, 1, 0), (7, 1, 3, 1, 0),
         (0, 1, 3, 0, 1), (7, 1, 3, 0, 1), (5, 1, 3, 0, 1), (5, 1, 3, 1, 0), (0, 0, 2, 3, 1),
         (7, 0, 2, 3, 1), (6, 0, 2, 3, 1), (0, 1, 2, 0, 1), (7, 1, 2, 0, 1), (5, 1, 2, 0, 0),
         (0, 1, 2, 3, 0), (7, 1, 2, 3, 0), (0, 0, 2, 2, 0), (7, 0, 2, 2, 0), (6, 0, 2, 2, 0),
         (6, 1, 3, 1, 0), (0, 0, 2, 1, 1), (7, 0, 2, 1, 1), (5, 1, 2, 0, 1), (0, 1, 1, 2, 1),
         (7, 1, 1, 2, 1), (6, 1, 3, 3, 0), (0, 0, 2, 3, 0), (7, 0, 2, 3, 0), (0, 1, 1, 3, 0),
         (7, 1, 1, 3, 0), (6, 1, 2, 1, 0), (0, 0, 2, 2, 1), (7, 0, 2, 2, 1),),
        ((0, 1, 1, 3, 1), (7, 1, 1, 3, 1),),
        ((6, 1, 2, 3, 0), (0, 1, 3, 1, 1), (7, 1, 3, 1, 1), (5, 1, 3, 1, 1), (0, 1, 0, 1, 0),
         (7, 1, 0, 1, 0), (6, 1, 0, 0, 1), (0, 1, 3, 3, 1), (7, 1, 3, 3, 1),),
        ((0, 1, 0, 2, 0), (7, 1, 0, 2, 0), (6, 1, 0, 1, 0), (0, 1, 2, 1, 1), (7, 1, 2, 1, 1),
         (0, 1, 2, 2, 0), (7, 1, 2, 2, 0), (6, 1, 0, 2, 0), (0, 1, 2, 3, 1), (7, 1, 2, 3, 1),
         (0, 1, 2, 2, 1), (7, 1, 2, 2, 1),),
        ((0, 1, 0, 0, 0), (7, 1, 0, 0, 0), (0, 1, 0, 3, 0), (7, 1, 0, 3, 0), (0, 1, 0, 1, 1),
         (7, 1, 0, 1, 1), (0, 1, 0, 3, 1), (7, 1, 0, 3, 1), (0, 1, 0, 2, 1), (7, 1, 0, 2, 1),),
        (),
    ),
    (
        ((2, 0, 0, 0, 0), (3, 0, 0, 0, 0),),
        (),
        (),
        (),
        (),
        (),
        (),
        (),
        (),
        ((3, 0, 0, 2, 0),),
        (),
        ((2, 0, 0, 1, 0),),
        (),
        (),
        (),
        (),
        ((3, 0, 0, 3, 0), (2, 1, 0, 2, 0), (3, 1, 0, 0, 0), (2, 1, 0, 1, 0), (3, 1, 0, 3, 0),),
        (),
        (),
        (),
        (),
        (),
        (),
        (),
        (),
    ),
    (
        ((3, 0, 1, 0, 0),),
        ((2, 0, 1, 1, 0),),
        (),
        (),
        (),
        (),
        (),
        (),
        (),
        (),
        (),
        (),
        (),
        (),
        (),
        (),
        ((2, 1, 1, 1, 0), (3, 0, 1, 2, 0),),
        ((3, 0, 1, 3, 0), (1, 0, 1, 0, 0), (4, 0, 1, 0, 0), (3, 1, 1, 0, 0), (3, 0, 1, 1, 0),
         (3, 1, 1, 2, 0), (1, 0, 1, 3, 0), (4, 0, 1, 3, 0), (3, 1, 1, 3, 0), (1, 1, 1, 0, 0),
         (4, 1, 1, 0, 0), (3, 1, 1, 1, 0),),
        ((1, 1, 1, 1, 0), (4, 1, 1, 1, 0),),
        ((1, 1, 1, 2, 0), (4, 1, 1, 2, 0),),
        ((1, 0, 1, 2, 0), (4, 0, 1, 2, 0), (1, 1, 1, 3, 0), (4, 1, 1, 3, 0),),
        (),
        (),
        (),
        (),
    ),
    (
        ((5, 0, 1, 0, 0), (7, 0, 1, 0, 0),),
        (),
        (),
        (),
        (),
        ((7, 0, 1, 0, 1),),
        (),
        (),
        (),
        (),
        ((7, 0, 1, 1, 0),),
        (),
        (),
        (),
        (),
        ((7, 0, 1, 1, 1),),
        ((7, 0, 1, 2, 0), (7, 0, 1, 2, 1), (7, 0, 1, 3, 0), (7, 0, 1, 3, 1), (7, 1, 1, 0, 0),),
        ((7, 1, 1, 0, 1), (0, 0, 0, 0, 0), (5, 0, 0, 0, 0), (7, 0, 0, 0, 0), (7, 1, 1, 1, 0),
         (7, 1, 1, 1, 1), (7, 1, 1, 2, 0), (7, 1, 1, 2, 1), (7, 1, 1, 3, 0), (0, 0, 0, 1, 0),
         (5, 0, 0, 1, 0), (7, 0, 0, 1, 0), (1, 1, 1, 0, 0), (4, 1, 1, 0, 0), (7, 1, 1, 3, 1),
         (0, 0, 3, 2, 0), (6, 0, 3, 2, 0), (7, 0, 3, 2, 0), (0, 0, 0, 3, 0), (7, 0, 0, 3, 0),
         (5, 0, 0, 3, 0), (0, 0, 3, 2, 1), (7, 0, 3, 2, 1), (5, 0, 3, 2, 1), (0, 0, 3, 3, 0),
         (6, 0, 3, 3, 0), (7, 0, 3, 3, 0), (5, 0, 1, 1, 1), (5, 0, 1, 2, 0), (0, 0, 3, 3, 1),
         (7, 0, 3, 3, 1), (0, 1, 3, 2, 0), (6, 1, 3, 2, 0), (7, 1, 3, 2, 0), (5, 0, 1, 2, 1),
         (5, 0, 1, 3, 0), (0, 1, 3, 2, 1), (7, 1, 3, 2, 1), (0, 0, 3, 0, 0), (6, 0, 3, 0, 0),
         (7, 0, 3, 0, 0), (0, 1, 3, 3, 0), (7, 1, 3, 3, 0), (6, 1, 3, 3, 0), (5, 0, 1, 3, 1),
         (0, 0, 0, 2, 0), (7, 0, 0, 2, 0), (6, 0, 0, 2, 0), (0, 0, 3, 0, 1), (7, 0, 3, 0, 1),
         (5, 0, 0, 2, 0), (0, 0, 0, 0, 1), (7, 0, 0, 0, 1), (1, 1, 1, 1, 0), (4, 1, 1, 1, 0),
         (0, 1, 3, 3, 1), (7, 1, 3, 3, 1), (0, 0, 2, 1, 0), (7, 0, 2, 1, 0), (6, 0, 2, 1, 0),
         (0, 0, 0, 2, 1), (7, 0, 0, 2, 1), (5, 0, 0, 2, 1), (0, 0, 3, 1, 1), (6, 0, 3, 1, 1),
         (7, 0, 3, 1, 1), (1, 1, 1, 3, 0), (4, 1, 1, 3, 0), (0, 0, 2, 1, 1), (7, 0, 2, 1, 1),
         (5, 0, 2, 1, 1), (5, 1, 3, 3, 0), (0, 0, 2, 2, 0), (7, 0, 2, 2, 0), (6, 0, 2, 2, 0),
         (0, 1, 0, 1, 0), (7, 1, 0, 1, 0), (0, 0, 3, 1, 0), (7, 0, 3, 1, 0),),
        ((0, 1, 0, 2, 0), (7, 1, 0, 2, 0), (6, 1, 0, 2, 0), (0, 0, 0, 1, 1), (7, 0, 0, 1, 1),
         (0, 0, 2, 2, 1), (7, 0, 2, 2, 1), (5, 0, 2, 2, 1), (5, 1, 0, 1, 0), (0, 0, 2, 3, 0),
         (7, 0, 2, 3, 0), (6, 0, 2, 3, 0), (0, 0, 2, 0, 0), (6, 0, 2, 0, 0), (7, 0, 2, 0, 0),
         (0, 1, 0, 3, 0), (7, 1, 0, 3, 0), (6, 1, 0, 3, 0), (0, 1, 0, 2, 1), (7, 1, 0, 2, 1),
         (5, 1, 3, 2, 1), (0, 0, 0, 3, 1), (7, 0, 0, 3, 1),),
        ((0, 0, 2, 0, 1), (7, 0, 2, 0, 1), (5, 1, 0, 2, 1), (0, 1, 2, 3, 0), (7, 1, 2, 3, 0),
         (0, 1, 3, 0, 1), (6, 1, 3, 0, 1), (7, 1, 3, 0, 1), (0, 0, 2, 3, 1), (7, 0, 2, 3, 1),),
        ((0, 1, 0, 0, 0), (7, 1, 0, 0, 0), (0, 1, 3, 1, 1), (6, 1, 3, 1, 1), (7, 1, 3, 1, 1),
         (6, 1, 0, 0, 0), (0, 1, 0, 3, 1), (7, 1, 0, 3, 1), (5, 1, 0, 3, 1), (5, 1, 1, 0, 0),
         (0, 1, 3, 0, 0), (7, 1, 3, 0, 0), (0, 1, 2, 0, 0), (6, 1, 2, 0, 0), (7, 1, 2, 0, 0),
         (5, 1, 1, 1, 1), (0, 1, 3, 1, 0), (7, 1, 3, 1, 0),),
        ((5, 1, 1, 3, 0), (0, 1, 2, 1, 0), (7, 1, 2, 1, 0), (6, 1, 2, 1, 0), (6, 1, 2, 3, 0),
         (0, 1, 0, 0, 1), (7, 1, 0, 0, 1), (5, 1, 0, 0, 0), (0, 1, 0, 1, 1), (7, 1, 0, 1, 1),),
        ((0, 1, 2, 0, 1), (7, 1, 2, 0, 1), (5, 1, 0, 0, 1), (0, 1, 2, 2, 0), (7, 1, 2, 2, 0),
         (0, 1, 2, 1, 1), (7, 1, 2, 1, 1), (5, 1, 1, 2, 0), (0, 1, 2, 2, 1), (7, 1, 2, 2, 1),
         (0, 1, 2, 3, 1), (7, 1, 2, 3, 1),),
        ((5, 1, 1, 2, 1),),
        (),
    ),
    (
        ((2, 0, 1, 0, 0),),
        ((3, 0, 1, 1, 0),),
        (),
        ((2, 0, 1, 3, 0),),
        (),
        (),
        (),
        (),
        (),
        (),
        (),
        (),
        (),
        (),
        (),
        (),
        ((2, 1, 1, 0, 0), (1, 0, 1, 1, 0), (4, 0, 1, 1, 0), (2, 1, 1, 1, 0), (1, 1, 1, 1, 0),
         (4, 1, 1, 1, 0), (2, 1, 1, 2, 0), (2, 0, 1, 2, 0), (3, 0, 1, 2, 0), (2, 1, 1, 3, 0),
         (3, 0, 1, 3, 0),),
        ((3, 1, 1, 3, 0),),
        (),
        (),
        (),
        (),
        (),
        (),
        (),
    ),
    (
        ((3, 0, 1, 0, 0),),
        (),
        (),
        (),
        (),
        (),
        (),
        (),
        ((2, 1, 1, 0, 0),),
        (),
        (),
        (),
        (),
        (),
        (),
        (),
        ((2, 1, 1, 1, 0), (2, 1, 1, 3, 0), (0, 0, 1, 0, 0), (6, 0, 1, 0, 0), (7, 0, 1, 0, 0),
         (0, 0, 1, 0, 1), (7, 0, 1, 0, 1), (0, 0, 0, 0, 0), (6, 0, 0, 0, 0), (7, 0, 0, 0, 0),
         (0, 0, 3, 0, 0), (7, 0, 3, 0, 0), (6, 0, 3, 0, 0), (5, 0, 3, 0, 0), (0, 0, 0, 1, 0),
         (7, 0, 0, 1, 0), (6, 0, 0, 1, 0), (0, 0, 0, 0, 1), (7, 0, 0, 0, 1), (5, 0, 0, 0, 1),
         (0, 0, 3, 2, 1), (7, 0, 3, 2, 1), (6, 0, 3, 2, 1), (0, 0, 3, 0, 1), (7, 0, 3, 0, 1),
         (0, 0, 3, 1, 0), (7, 0, 3, 1, 0), (6, 0, 3, 1, 0), (0, 0, 0, 3, 0), (7, 0, 0, 3, 0),
         (0, 0, 0, 1, 1), (7, 0, 0, 1, 1), (0, 0, 1, 1, 1), (7, 0, 1, 1, 1), (6, 0, 0, 3, 0),
         (0, 0, 3, 1, 1), (7, 0, 3, 1, 1), (5, 0, 3, 1, 1), (0, 0, 3, 3, 0), (7, 0, 3, 3, 0),
         (6, 0, 3, 3, 0), (3, 0, 1, 3, 0), (0, 0, 1, 2, 0), (7, 0, 1, 2, 0), (6, 0, 1, 1, 1),
         (0, 0, 3, 2, 0), (7, 0, 3, 2, 0), (5, 0, 0, 1, 1), (0, 0, 1, 2, 1), (7, 0, 1, 2, 1),
         (0, 0, 3, 3, 1), (7, 0, 3, 3, 1),),
        ((0, 1, 3, 0, 0), (7, 1, 3, 0, 0), (6, 1, 3, 0, 0), (3, 0, 1, 1, 0), (0, 0, 1, 3, 0),
         (7, 0, 1, 3, 0), (0, 0, 0, 3, 1), (7, 0, 0, 3, 1), (0, 0, 2, 0, 0), (7, 0, 2, 0, 0),
         (5, 0, 2, 0, 0), (0, 0, 1, 3, 1), (7, 0, 1, 3, 1), (6, 0, 2, 0, 0), (0, 0, 1, 1, 0),
         (7, 0, 1, 1, 0),),
        ((0, 1, 3, 1, 0), (7, 1, 3, 1, 0), (6, 1, 3, 1, 0), (3, 0, 1, 2, 0), (5, 0, 0, 3, 1),
         (0, 0, 0, 2, 0), (7, 0, 0, 2, 0), (0, 1, 3, 0, 1), (7, 1, 3, 0, 1), (5, 1, 3, 0, 1),
         (0, 0, 0, 2, 1), (7, 0, 0, 2, 1),),
        ((0, 0, 2, 3, 0), (6, 0, 2, 3, 0), (7, 0, 2, 3, 0), (0, 1, 3, 1, 1), (7, 1, 3, 1, 1),
         (3, 1, 1, 2, 0), (5, 1, 3, 1, 1), (0, 0, 2, 1, 1), (7, 0, 2, 1, 1), (6, 0, 2, 1, 1),
         (0, 0, 2, 0, 1), (7, 0, 2, 0, 1), (3, 1, 1, 3, 0), (0, 1, 3, 3, 0), (7, 1, 3, 3, 0),
         (6, 1, 3, 3, 0), (0, 0, 2, 3, 1), (7, 0, 2, 3, 1), (0, 0, 2, 2, 1), (7, 0, 2, 2, 1),
         (0, 0, 2, 1, 0), (7, 0, 2, 1, 0), (0, 1, 3, 2, 0), (7, 1, 3, 2, 0), (0, 1, 0, 1, 0),
         (6, 1, 0, 1, 0), (7, 1, 0, 1, 0), (0, 1, 2, 0, 0), (5, 1, 2, 0, 0), (6, 1, 2, 0, 0),
         (7, 1, 2, 0, 0), (0, 1, 3, 3, 1), (7, 1, 3, 3, 1), (0, 1, 3, 2, 1), (7, 1, 3, 2, 1),
         (0, 1, 2, 1, 0), (5, 1, 2, 1, 0), (7, 1, 2, 1, 0), (6, 1, 2, 1, 0), (0, 1, 0, 1, 1),
         (5, 1, 0, 1, 1), (7, 1, 0, 1, 1), (0, 1, 0, 2, 1), (7, 1, 0, 2, 1), (6, 1, 0, 2, 1),
         (0, 1, 2, 2, 0), (7, 1, 2, 2, 0), (6, 1, 2, 2, 0), (5, 1, 2, 2, 0), (0, 1, 2, 0, 1),
         (7, 1, 2, 0, 1), (0, 1, 0, 3, 1), (7, 1, 0, 3, 1), (0, 0, 2, 2, 0), (7, 0, 2, 2, 0),),
        ((0, 1, 2, 1, 1), (7, 1, 2, 1, 1),),
        ((0, 1, 1, 0, 0), (7, 1, 1, 0, 0), (6, 1, 0, 3, 1), (0, 1, 2, 3, 0), (7, 1, 2, 3, 0),
         (6, 1, 2, 3, 0), (0, 1, 2, 2, 1), (5, 1, 2, 2, 1), (7, 1, 2, 2, 1), (0, 1, 1, 1, 1),
         (7, 1, 1, 1, 1), (6, 1, 1, 0, 0), (0, 1, 0, 2, 0), (7, 1, 0, 2, 0), (0, 1, 1, 3, 0),
         (7, 1, 1, 3, 0), (6, 1, 1, 1, 1), (0, 1, 2, 3, 1), (7, 1, 2, 3, 1),),
        ((0, 1, 0, 0, 0), (7, 1, 0, 0, 0), (6, 1, 1, 3, 0), (0, 1, 0, 3, 0), (7, 1, 0, 3, 0),
         (0, 1, 0, 0, 1), (7, 1, 0, 0, 1),),
        ((0, 1, 1, 0, 1), (7, 1, 1, 0, 1), (0, 1, 1, 2, 0), (7, 1, 1, 2, 0), (0, 1, 1, 1, 0),
         (7, 1, 1, 1, 0), (0, 1, 1, 2, 1), (7, 1, 1, 2, 1), (0, 1, 1, 3, 1), (7, 1, 1, 3, 1),),
        (),
    ),
)


def local_plain(tokens, norm_gain, up_trained, down_trained):
    shards = lax.axis_size("fs")
    groups = lax.axis_size("tp")
    rows_local = up_trained.shape[0]
    cols_local = up_trained.shape[1]
    folded = (norm_gain[:, None] * up_trained).astype(jnp.bfloat16)
    stacked = jnp.stack([folded, down_trained.astype(jnp.bfloat16)])
    served_width = cols_local * groups // shards
    blocks_here = cols_local // served_width
    quarter_rows = rows_local // groups
    pieces = stacked.reshape(2, groups, quarter_rows, blocks_here, served_width)
    moved = lax.all_to_all(pieces, "tp", split_axis=1, concat_axis=3, tiled=True)
    placed = lax.all_to_all(moved, "fs", split_axis=3, concat_axis=2, tiled=True)
    ordered = placed.reshape(2, shards, quarter_rows, served_width)
    joined = lax.all_gather(ordered, "tp", axis=2, tiled=True)
    owned = joined.reshape(2, rows_local * shards, served_width)
    up_serving = owned[0]
    down_serving = owned[1]
    values = tokens.astype(jnp.float32)
    scale = lax.rsqrt(jnp.mean(values * values, axis=1, keepdims=True) + epsilon)
    normed = (values * scale).astype(jnp.bfloat16)
    hidden = jnp.dot(normed, up_serving, preferred_element_type=jnp.float32)
    active = jnp.square(jax.nn.relu(hidden)).astype(jnp.bfloat16)
    summed = lax.psum_scatter(
        lax.dot_general(
            down_serving, active, (((1,), (1,)), ((), ())), preferred_element_type=jnp.float32
        ),
        "fs",
        scatter_dimension=0,
        tiled=True,
    )
    prompt_output = summed.T.astype(jnp.bfloat16)
    return (up_serving, down_serving, prompt_output)


def down_block(active, whole, plane, put):
    rows_local = whole.shape[1] // 4
    tile = 256 if rows_local % 256 == 0 else rows_local

    @pl.loop(0, rows_local // tile)
    def _(n):
        rows = pl.ds(pl.multiple_of(plane * rows_local + n * tile, tile), tile)
        product = lax.dot_general(
            active[...], whole[1, rows, :], (((1,), (1,)), ((), ())),
            preferred_element_type=jnp.float32,
        )
        put(pl.ds(pl.multiple_of(n * tile, tile), tile), product)


def kernel(
    tokens_hbm, gain_hbm, up_hbm, down_hbm, whole, active, rs_recv,
    raw, gain_rows, gain, cast, relay, toks, normed, hidden, rs_send,
    in_sem, misc_sem, got_sem, relay_sem, src_sem, out_sem, rs_ssem, rs_rsem,
):
    y = lax.axis_index("grp")
    z = lax.axis_index("fs")
    t = lax.axis_index("tp")
    mirrored = z // 2
    role = jnp.where(mirrored == 1, 4 * (3 - z) + (3 - t), 4 * z + t)
    is_own = z == t
    is_active = t % 2 == z % 2
    t_x = jnp.where(t < 2, t + 2, t - 2)
    t_c = t + 1 - 2 * (t % 2)
    to_x = {"tp": t_x}
    to_c = {"tp": t_c}
    to_y = {"grp": 1 - y}
    rows_local, width = cast.shape[1], cast.shape[2]
    size = rows_local // (2 * PAIRS)
    trained = (up_hbm, down_hbm)
    planes = [jnp.where(mirrored == 1, 3 - k, k) for k in range(4)]
    sides = [y, 1 - y]

    def part(pair, side):
        return 2 * pair + sides[side]

    def ds(start, extent):
        return pl.ds(pl.multiple_of(start, extent), extent)

    def local_rows(pair, side):
        return ds(part(pair, side) * size, size)

    def unit(m, plane, pair, side):
        return whole.at[m, ds(plane * rows_local + part(pair, side) * size, size)]

    def remote(src, dst, ssem, rsem, where):
        return pltpu.make_async_remote_copy(
            src_ref=src, dst_ref=dst, send_sem=ssem, recv_sem=rsem,
            device_id=where, device_id_type=MESH,
        )

    def fetch(m, pair, side):
        rows = local_rows(pair, side)
        return pltpu.make_async_copy(
            trained[m].at[rows], raw.at[m, rows], in_sem.at[m, 2 * pair + side]
        )

    get_gain = pltpu.make_async_copy(gain_hbm, gain_rows, misc_sem.at[0])
    get_toks = pltpu.make_async_copy(tokens_hbm, toks, misc_sem.at[1])
    get_gain.start()
    for pair in range(PAIRS):
        fetch(0, pair, 0).start()

    barrier = pltpu.get_barrier_semaphore()
    others = [{"fs": lax.rem(z + k, 4)} for k in range(1, 4)]
    for where in [to_x, to_c, to_y] + others:
        pl.semaphore_signal(barrier, inc=1, device_id=where, device_id_type=MESH)

    get_gain.wait()
    lanes = gain_rows.shape[1]
    for q in range(gain_rows.shape[0]):
        square = (lanes, lanes)
        chosen = jnp.where(
            lax.broadcasted_iota(jnp.int32, square, 0) == lax.broadcasted_iota(jnp.int32, square, 1),
            jnp.broadcast_to(gain_rows[pl.ds(q, 1), :], square), 0.0,
        )
        column = jnp.sum(chosen, axis=1, keepdims=True)
        gain[pl.ds(q * lanes, lanes), :] = jnp.broadcast_to(column, square)

    piece = 16

    def cast_unit(m, pair, side):
        fetch(m, pair, side).wait()
        base = part(pair, side) * size

        def store(into, shift):
            @pl.loop(0, size // piece)
            def _(i):
                here = ds(base + i * piece, piece)
                there = ds(shift + base + i * piece, piece)
                if m == 0:
                    factor = gain[here, :]
                    for j in range(width // lanes):
                        cols = pl.ds(j * lanes, lanes)
                        into[0, there, cols] = (raw[0, here, cols] * factor).astype(jnp.bfloat16)
                else:
                    into[m, there, :] = raw[m, here, :].astype(jnp.bfloat16)

        @pl.when(is_own)
        def _():
            store(whole, z * rows_local)

        if side == 0:
            @pl.when(jnp.logical_not(is_own))
            def _():
                store(cast, 0)

    def step(kind, m, k, pair, side):
        plane = planes[k]
        place = part(pair, side)
        if kind == GET:
            here = unit(m, plane, pair, side)
            remote(here, here, out_sem.at[0, m], got_sem.at[m, plane, place], to_x).wait_recv()
        elif kind == GET_RELAY:
            here = relay.at[m, ds(place * size, size)]
            remote(here, here, src_sem.at[m], relay_sem.at[m, pair], to_x).wait_recv()
        elif kind == SWAP:
            remote(
                cast.at[m, local_rows(pair, side)], relay.at[m, ds(place * size, size)],
                src_sem.at[m], relay_sem.at[m, pair], to_x,
            ).start()
        elif kind in (HOP, HOP_RELAY):
            src = (cast if kind == HOP else relay).at[m, ds(place * size, size)]
            remote(
                src, unit(m, z, pair, side), src_sem.at[m], got_sem.at[m, z, place],
                {"fs": t if kind == HOP else t_x},
            ).start()
        elif kind == SEND_CORE:
            here = unit(m, plane, pair, side)
            remote(here, here, out_sem.at[2, m], got_sem.at[m, plane, 0], to_c).start()
        else:
            here = unit(m, plane, pair, side)
            i = kind - SEND_X
            remote(
                here, here, out_sem.at[i, m], got_sem.at[m, plane, place], (to_x, to_y)[i]
            ).start()

    def run(segment):
        for r in range(8):
            if SCHEDULE[r][segment]:
                @pl.when(role == r)
                def _():
                    for s in SCHEDULE[r][segment]:
                        step(*s)

    casts = [(m, pair, side) for m in range(2) for side in range(2) for pair in range(PAIRS)]
    segment = 0
    for m, pair, side in casts:
        if side == 1:
            pl.when(is_own)(lambda: cast_unit(m, pair, side))
        else:
            cast_unit(m, pair, side)
        if segment == 0:
            @pl.when(is_own)
            def _():
                for p in range(PAIRS):
                    fetch(0, p, 1).start()
            for p in range(PAIRS):
                fetch(1, p, 0).start()
            @pl.when(is_own)
            def _():
                for p in range(PAIRS):
                    fetch(1, p, 1).start()
            get_toks.start()
            pl.semaphore_wait(barrier, 6)
        run(segment)
        segment += 1

    get_toks.wait()
    tokens_here = toks.shape[0]

    @pl.loop(0, tokens_here // piece)
    def _(i):
        here = ds(i * piece, piece)
        values = toks[here, :].astype(jnp.float32)
        scale = lax.rsqrt(jnp.mean(values * values, axis=1, keepdims=True) + epsilon)
        normed[here, :] = (values * scale).astype(jnp.bfloat16)

    def pick(table):
        chosen = planes[table[0]]
        for r in range(1, 8):
            if table[r] != table[0]:
                chosen = jnp.where(role == r, planes[table[r]], chosen)
        return chosen

    def listen(m, plane):
        @pl.when(jnp.logical_not(is_active))
        def _():
            here = whole.at[m, ds(plane * rows_local, rows_local)]
            remote(here, here, out_sem.at[2, m], got_sem.at[m, plane, 0], to_c).wait_recv()

    tile = 512 if width % 512 == 0 else width

    def compute_up(k):
        plane = pick(ORDER[0][k])
        listen(0, plane)
        rows = ds(plane * rows_local, rows_local)

        @pl.loop(0, width // tile)
        def _(n):
            cols = ds(n * tile, tile)
            product = jnp.dot(
                normed[:, rows], whole[0, rows, cols], preferred_element_type=jnp.float32
            )
            if k > 0:
                product = product + hidden[:, cols]
            if k < 3:
                hidden[:, cols] = product
            else:
                active[:, cols] = jnp.square(jnp.maximum(product, 0.0)).astype(jnp.bfloat16)

    def scatter(k, plane):
        slot = lax.rem(z - plane + 3, 4)
        return remote(
            rs_send.at[k], rs_recv.at[slot], rs_ssem.at[k], rs_rsem.at[slot], {"fs": plane}
        )

    def compute_down(k):
        plane = pick(ORDER[1][k])
        listen(1, plane)

        down_block(
            active, whole, plane,
            lambda cols, product: rs_send.__setitem__((k, slice(None), cols), product.astype(jnp.bfloat16)),
        )
        scatter(k, plane).start()

    for m in range(2):
        for k in range(4):
            run(segment)
            segment += 1
            if m == 0:
                compute_up(k)
            elif k < 3:
                compute_down(k)
            else:
                listen(1, z)
    run(segment)

    for k in range(3):
        here = rs_recv.at[k]
        remote(here, here, rs_ssem.at[k], rs_rsem.at[k], {"fs": lax.rem(z + 1, 4)}).wait_recv()

    def drain(sem, m, count):
        sent = whole.at[m, pl.ds(0, count * size)]
        remote(sent, sent, sem, got_sem.at[0, 0, 0], to_x).wait_send()

    for r in range(8):
        @pl.when(role == r)
        def _():
            for m in range(2):
                steps = [s for part_of in SCHEDULE[r] for s in part_of if s[1] == m]
                hops = sum(s[0] in (SWAP, HOP, HOP_RELAY) for s in steps)
                if hops:
                    drain(src_sem.at[m], m, hops)
                for i, kind in enumerate((SEND_X, SEND_Y, SEND_CORE)):
                    sends = sum(s[0] == kind for s in steps)
                    if sends:
                        drain(out_sem.at[i, m], m, sends)
    for k in range(3):
        here = rs_send.at[k]
        remote(here, here, rs_ssem.at[k], rs_rsem.at[k], {"fs": lax.rem(z + 1, 4)}).wait_send()


pieces_out = 8


def deliver(whole, active, rs_recv, up_out, down_out, prompt_out, own, prompt, sems, last):
    rows = whole.shape[1] // pieces_out
    copies = [
        pltpu.make_async_copy(
            whole.at[m, pl.ds(i * rows, rows)], out.at[pl.ds(i * rows, rows)], sems.at[m]
        )
        for m, out in enumerate((up_out, down_out))
        for i in range(pieces_out)
    ]
    for copy in copies:
        copy.start()
    down_block(
        active, whole, lax.axis_index("fs"),
        lambda cols, product: own.__setitem__((slice(None), cols), product),
    )
    piece = 16

    @pl.loop(0, own.shape[0] // piece)
    def _(i):
        here = pl.ds(pl.multiple_of(i * piece, piece), piece)
        total = own[here, :]
        for k in range(3):
            total = total + rs_recv[k, here, :].astype(jnp.float32)
        prompt[here, :] = total.astype(prompt.dtype)

    final = pltpu.make_async_copy(prompt, prompt_out, last)
    final.start()
    for m, out in enumerate((up_out, down_out)):
        pltpu.make_async_copy(whole.at[m], out, sems.at[m]).wait()
    final.wait()


def local_kernel(tokens, norm_gain, up_trained, down_trained):
    shards = lax.axis_size("fs")
    rows_local, width = up_trained.shape
    tokens_here, features = tokens.shape
    any_space = pl.BlockSpec(memory_space=pl.ANY)
    dma = pltpu.SemaphoreType.DMA
    bf16, f32 = jnp.bfloat16, jnp.float32
    results = pl.pallas_call(
        kernel,
        out_shape=(
            pltpu.VMEM((2, rows_local * shards, width), bf16),
            pltpu.VMEM((tokens_here, width), bf16),
            pltpu.VMEM((3, tokens_here, rows_local), bf16),
        ),
        in_specs=[any_space] * 4,
        out_specs=(pl.BlockSpec(memory_space=pltpu.VMEM),) * 3,
        scratch_shapes=[
            pltpu.VMEM((2, rows_local, width), f32),
            pltpu.VMEM((rows_local // 128, 128), f32),
            pltpu.VMEM((rows_local, 128), f32),
            pltpu.VMEM((2, rows_local, width), bf16),
            pltpu.VMEM((2, rows_local, width), bf16),
            pltpu.VMEM((tokens_here, features), bf16),
            pltpu.VMEM((tokens_here, features), bf16),
            pltpu.VMEM((tokens_here, width), f32),
            pltpu.VMEM((3, tokens_here, rows_local), bf16),
            dma((2, 2 * PAIRS)), dma((2,)),
            dma((2, 4, 2 * PAIRS)), dma((2, PAIRS)),
            dma((2,)), dma((3, 2)), dma((3,)), dma((3,)),
        ],
        compiler_params=pltpu.CompilerParams(
            collective_id=0, has_side_effects=True, vmem_limit_bytes=40 * 1024 * 1024
        ),
    )(tokens, norm_gain.reshape(rows_local // 128, 128), up_trained, down_trained)
    held = pl.BlockSpec(memory_space=pltpu.VMEM)
    return tuple(pl.pallas_call(
        deliver,
        out_shape=(
            jax.ShapeDtypeStruct((rows_local * shards, width), bf16),
            jax.ShapeDtypeStruct((rows_local * shards, width), bf16),
            jax.ShapeDtypeStruct((tokens_here, rows_local), bf16),
        ),
        in_specs=[held] * 3,
        out_specs=(any_space,) * 3,
        scratch_shapes=[
            pltpu.VMEM((tokens_here, rows_local), f32), pltpu.VMEM((tokens_here, rows_local), bf16),
            dma((2,)), dma(()),
        ],
        compiler_params=pltpu.CompilerParams(vmem_limit_bytes=8 * 1024 * 1024),
    )(*results))


def solution(mesh):
    in_specs = (P(("grp", "tp"), None), P("fs"), P("fs", "tp"), P("fs", "tp"))
    out_specs = (P("grp", "fs"), P("grp", "fs"), P(("grp", "tp"), "fs"))
    sizes = mesh.shape
    square = sizes["grp"] == 2 and sizes["fs"] == 4 and sizes["tp"] == 4
    local = local_kernel if square else local_plain
    return jax.shard_map(local, mesh=mesh, in_specs=in_specs, out_specs=out_specs, check_vma=False)
```

```python
import jax
import jax.numpy as jnp
from jax import lax
from jax.experimental import pallas as pl
from jax.experimental.pallas import tpu as pltpu
from jax.sharding import PartitionSpec as P

epsilon = 1e-06
MESH = pl.DeviceIdType.MESH

GET, GET_RELAY, SWAP, HOP, HOP_RELAY, SEND_X, SEND_Y, SEND_CORE = range(8)
PAIRS = 4
ORDER = (
    (
        (0, 0, 0, 0, 1, 1, 3, 3),
        (3, 3, 3, 3, 3, 3, 1, 1),
        (1, 1, 1, 1, 0, 0, 0, 0),
        (2, 2, 2, 2, 2, 2, 2, 2),
    ),
    (
        (1, 1, 1, 1, 3, 3, 3, 3),
        (2, 2, 3, 3, 0, 0, 2, 2),
        (3, 3, 2, 2, 2, 2, 0, 0),
        (0, 0, 0, 0, 1, 1, 1, 1),
    ),
)
SCHEDULE = (
    (
        ((5, 0, 0, 0, 0), (7, 0, 0, 0, 0),),
        ((5, 0, 0, 1, 0),),
        (),
        (),
        (),
        ((7, 0, 0, 0, 1),),
        (),
        ((5, 0, 0, 2, 0),),
        (),
        (),
        ((7, 0, 0, 1, 0),),
        (),
        (),
        (),
        (),
        ((7, 0, 0, 1, 1),),
        ((7, 0, 0, 2, 0), (7, 0, 0, 2, 1), (7, 0, 0, 3, 0), (7, 0, 0, 3, 1), (7, 1, 0, 0, 0),),
        ((7, 1, 0, 0, 1), (7, 1, 0, 1, 0), (7, 1, 0, 1, 1), (7, 1, 0, 2, 0), (7, 1, 0, 2, 1),
         (7, 1, 0, 3, 0), (5, 0, 0, 3, 0), (7, 1, 0, 3, 1), (1, 0, 0, 0, 0), (4, 0, 0, 0, 0),
         (0, 0, 1, 0, 0), (7, 0, 1, 0, 0), (5, 0, 1, 0, 0), (0, 0, 3, 0, 0), (6, 0, 3, 0, 0),
         (7, 0, 3, 0, 0), (5, 1, 0, 0, 1), (0, 0, 3, 0, 1), (7, 0, 3, 0, 1), (1, 0, 0, 1, 0),
         (4, 0, 0, 1, 0), (0, 0, 1, 2, 0), (7, 0, 1, 2, 0), (5, 0, 1, 2, 0), (0, 0, 3, 2, 0),
         (6, 0, 3, 2, 0), (7, 0, 3, 2, 0), (0, 0, 3, 2, 1), (7, 0, 3, 2, 1), (5, 0, 3, 2, 1),
         (1, 0, 0, 3, 0), (4, 0, 0, 3, 0), (0, 0, 1, 3, 0), (6, 0, 1, 3, 0), (7, 0, 1, 3, 0),
         (0, 0, 3, 3, 0), (7, 0, 3, 3, 0), (6, 0, 3, 3, 0), (5, 0, 3, 3, 0), (0, 0, 1, 3, 1),
         (7, 0, 1, 3, 1), (5, 0, 1, 3, 1), (1, 1, 0, 0, 0), (4, 1, 0, 0, 0), (0, 1, 3, 0, 0),
         (7, 1, 3, 0, 0), (0, 0, 3, 3, 1), (7, 0, 3, 3, 1), (5, 1, 3, 0, 0), (1, 1, 0, 1, 0),
         (4, 1, 0, 1, 0), (0, 1, 1, 0, 0), (7, 1, 1, 0, 0), (5, 1, 1, 0, 0), (0, 1, 3, 3, 0),
         (6, 1, 3, 3, 0), (7, 1, 3, 3, 0), (0, 0, 3, 1, 0), (7, 0, 3, 1, 0), (5, 1, 3, 3, 0),
         (0, 1, 3, 3, 1), (7, 1, 3, 3, 1), (0, 0, 1, 0, 1), (7, 0, 1, 0, 1), (0, 0, 2, 0, 0),
         (6, 0, 2, 0, 0), (5, 0, 2, 0, 0), (0, 0, 1, 1, 0), (7, 0, 1, 1, 0), (7, 0, 2, 0, 0),
         (0, 0, 3, 1, 1), (7, 0, 3, 1, 1),),
        ((0, 0, 2, 0, 1), (7, 0, 2, 0, 1), (5, 0, 2, 0, 1), (0, 0, 1, 1, 1), (7, 0, 1, 1, 1),
         (0, 1, 1, 2, 0), (6, 1, 1, 2, 0), (5, 1, 1, 2, 0), (7, 1, 1, 2, 0), (0, 0, 2, 3, 0),
         (6, 0, 2, 3, 0), (7, 0, 2, 3, 0), (0, 0, 1, 2, 1), (7, 0, 1, 2, 1),),
        ((0, 1, 1, 2, 1), (7, 1, 1, 2, 1), (1, 1, 0, 2, 0), (4, 1, 0, 2, 0), (0, 1, 1, 3, 0),
         (6, 1, 1, 3, 0), (7, 1, 1, 3, 0), (0, 0, 2, 1, 0), (7, 0, 2, 1, 0), (5, 0, 2, 1, 0),
         (6, 0, 2, 1, 0), (0, 0, 2, 3, 1), (7, 0, 2, 3, 1), (5, 0, 2, 3, 1), (0, 1, 3, 2, 1),
         (7, 1, 3, 2, 1), (6, 1, 3, 2, 1), (0, 1, 1, 3, 1), (7, 1, 1, 3, 1), (5, 1, 1, 2, 1),
         (0, 1, 1, 0, 1), (7, 1, 1, 0, 1), (0, 0, 2, 2, 0), (7, 0, 2, 2, 0), (5, 0, 2, 2, 0),
         (6, 0, 2, 2, 0), (0, 0, 2, 1, 1), (7, 0, 2, 1, 1), (5, 1, 1, 3, 0), (0, 1, 1, 1, 1),
         (7, 1, 1, 1, 1), (0, 1, 2, 2, 0), (7, 1, 2, 2, 0), (6, 1, 2, 2, 0), (0, 1, 3, 2, 0),
         (7, 1, 3, 2, 0), (5, 1, 1, 3, 1), (0, 1, 1, 1, 0), (7, 1, 1, 1, 0), (0, 1, 2, 1, 0),
         (6, 1, 2, 1, 0), (7, 1, 2, 1, 0), (0, 1, 2, 3, 0), (6, 1, 2, 3, 0), (7, 1, 2, 3, 0),
         (0, 0, 2, 2, 1), (7, 0, 2, 2, 1),),
        ((5, 1, 0, 1, 0),),
        ((0, 1, 3, 0, 1), (7, 1, 3, 0, 1), (0, 1, 2, 2, 1), (7, 1, 2, 2, 1), (5, 1, 0, 2, 0),
         (0, 1, 3, 1, 0), (7, 1, 3, 1, 0), (0, 1, 2, 1, 1), (7, 1, 2, 1, 1), (5, 1, 2, 2, 0),
         (0, 1, 2, 0, 0), (7, 1, 2, 0, 0), (0, 1, 2, 3, 1), (7, 1, 2, 3, 1), (5, 1, 2, 2, 1),
         (0, 1, 2, 0, 1), (7, 1, 2, 0, 1),),
        ((5, 1, 0, 3, 0), (0, 1, 3, 1, 1), (7, 1, 3, 1, 1),),
        (),
        ((5, 1, 0, 3, 1),),
    ),
    (
        ((3, 0, 0, 0, 0),),
        ((3, 0, 0, 1, 0),),
        (),
        (),
        (),
        (),
        (),
        (),
        (),
        (),
        (),
        ((3, 0, 0, 3, 0),),
        (),
        (),
        (),
        (),
        (),
        ((1, 0, 0, 0, 0), (4, 0, 0, 0, 0), (1, 0, 0, 1, 0), (4, 0, 0, 1, 0), (3, 0, 0, 2, 0),
         (1, 1, 0, 2, 0), (4, 1, 0, 2, 0), (3, 1, 0, 1, 0), (3, 1, 0, 2, 0), (3, 1, 0, 3, 0),),
        ((1, 1, 0, 1, 0), (4, 1, 0, 1, 0), (3, 1, 0, 0, 0),),
        (),
        (),
        (),
        (),
        (),
        (),
    ),
    (
        ((2, 0, 0, 0, 0),),
        (),
        ((3, 0, 0, 2, 0),),
        (),
        (),
        (),
        (),
        (),
        (),
        (),
        (),
        ((2, 0, 0, 1, 0),),
        (),
        (),
        (),
        (),
        ((3, 0, 0, 3, 0), (0, 0, 0, 0, 0), (6, 0, 0, 0, 0), (7, 0, 0, 0, 0), (2, 0, 0, 3, 0),
         (3, 1, 0, 2, 0), (0, 0, 0, 1, 0), (6, 0, 0, 1, 0), (7, 0, 0, 1, 0), (0, 0, 0, 0, 1),
         (7, 0, 0, 0, 1), (0, 0, 0, 2, 0), (6, 0, 0, 2, 0), (7, 0, 0, 2, 0), (0, 0, 0, 1, 1),
         (7, 0, 0, 1, 1), (2, 1, 0, 0, 0), (3, 1, 0, 3, 0), (0, 0, 1, 1, 0), (7, 0, 1, 1, 0),
         (6, 0, 1, 1, 0), (0, 0, 1, 0, 0), (6, 0, 1, 0, 0), (7, 0, 1, 0, 0), (0, 0, 0, 2, 1),
         (7, 0, 0, 2, 1), (0, 0, 0, 3, 0), (7, 0, 0, 3, 0), (6, 0, 0, 3, 0), (0, 0, 1, 1, 1),
         (7, 0, 1, 1, 1), (2, 1, 0, 1, 0), (0, 0, 1, 2, 0), (7, 0, 1, 2, 0), (6, 0, 1, 2, 0),
         (0, 0, 3, 0, 0), (7, 0, 3, 0, 0), (6, 0, 3, 0, 0), (0, 0, 1, 0, 1), (7, 0, 1, 0, 1),
         (0, 1, 1, 1, 0), (7, 1, 1, 1, 0), (0, 1, 0, 0, 1), (7, 1, 0, 0, 1), (0, 0, 0, 3, 1),
         (7, 0, 0, 3, 1),),
        ((5, 0, 1, 0, 1), (0, 0, 3, 2, 1), (7, 0, 3, 2, 1), (0, 0, 3, 1, 0), (5, 0, 3, 1, 0),
         (6, 0, 3, 1, 0), (7, 0, 3, 1, 0), (6, 0, 3, 2, 1), (0, 0, 1, 2, 1), (7, 0, 1, 2, 1),
         (0, 0, 3, 3, 0), (7, 0, 3, 3, 0), (6, 0, 3, 3, 0), (0, 0, 3, 0, 1), (7, 0, 3, 0, 1),
         (5, 0, 1, 1, 1), (0, 0, 1, 3, 1), (7, 0, 1, 3, 1), (6, 0, 1, 3, 1), (0, 0, 3, 1, 1),
         (7, 0, 3, 1, 1), (5, 0, 3, 1, 1), (5, 0, 1, 2, 1), (0, 1, 1, 0, 0), (7, 1, 1, 0, 0),
         (0, 0, 3, 2, 0), (7, 0, 3, 2, 0), (2, 1, 0, 2, 0), (0, 1, 3, 0, 0), (7, 1, 3, 0, 0),
         (0, 1, 3, 2, 0), (6, 1, 3, 2, 0), (7, 1, 3, 2, 0), (6, 1, 1, 0, 0), (0, 0, 3, 3, 1),
         (7, 0, 3, 3, 1),),
        ((0, 1, 2, 0, 0), (7, 1, 2, 0, 0), (0, 0, 2, 0, 0), (7, 0, 2, 0, 0), (6, 1, 1, 1, 0),
         (0, 0, 1, 3, 0), (7, 0, 1, 3, 0),),
        ((0, 1, 3, 3, 0), (7, 1, 3, 3, 0), (6, 1, 3, 0, 0), (0, 1, 3, 2, 1), (7, 1, 3, 2, 1),
         (5, 1, 3, 2, 1), (0, 1, 2, 1, 0), (7, 1, 2, 1, 0), (0, 0, 2, 0, 1), (7, 0, 2, 0, 1),
         (6, 1, 2, 0, 0), (0, 1, 1, 0, 1), (7, 1, 1, 0, 1), (5, 1, 1, 0, 1), (5, 1, 2, 1, 0),
         (0, 1, 1, 2, 0), (7, 1, 1, 2, 0), (0, 1, 1, 1, 1), (7, 1, 1, 1, 1), (5, 1, 1, 1, 1),
         (0, 0, 2, 1, 0), (7, 0, 2, 1, 0), (6, 0, 2, 1, 0), (0, 1, 3, 1, 0), (7, 1, 3, 1, 0),
         (0, 1, 3, 0, 1), (7, 1, 3, 0, 1), (5, 1, 3, 0, 1), (5, 1, 3, 1, 0), (0, 0, 2, 3, 1),
         (7, 0, 2, 3, 1), (6, 0, 2, 3, 1), (0, 1, 2, 0, 1), (7, 1, 2, 0, 1), (5, 1, 2, 0, 0),
         (0, 1, 2, 3, 0), (7, 1, 2, 3, 0), (0, 0, 2, 2, 0), (7, 0, 2, 2, 0), (6, 0, 2, 2, 0),
         (6, 1, 3, 1, 0), (0, 0, 2, 1, 1), (7, 0, 2, 1, 1), (5, 1, 2, 0, 1), (0, 1, 1, 2, 1),
         (7, 1, 1, 2, 1), (6, 1, 3, 3, 0), (0, 0, 2, 3, 0), (7, 0, 2, 3, 0), (0, 1, 1, 3, 0),
         (7, 1, 1, 3, 0), (6, 1, 2, 1, 0), (0, 0, 2, 2, 1), (7, 0, 2, 2, 1),),
        ((0, 1, 1, 3, 1), (7, 1, 1, 3, 1),),
        ((6, 1, 2, 3, 0), (0, 1, 3, 1, 1), (7, 1, 3, 1, 1), (5, 1, 3, 1, 1), (0, 1, 0, 1, 0),
         (7, 1, 0, 1, 0), (6, 1, 0, 0, 1), (0, 1, 3, 3, 1), (7, 1, 3, 3, 1),),
        ((0, 1, 0, 2, 0), (7, 1, 0, 2, 0), (6, 1, 0, 1, 0), (0, 1, 2, 1, 1), (7, 1, 2, 1, 1),
         (0, 1, 2, 2, 0), (7, 1, 2, 2, 0), (6, 1, 0, 2, 0), (0, 1, 2, 3, 1), (7, 1, 2, 3, 1),
         (0, 1, 2, 2, 1), (7, 1, 2, 2, 1),),
        ((0, 1, 0, 0, 0), (7, 1, 0, 0, 0), (0, 1, 0, 3, 0), (7, 1, 0, 3, 0), (0, 1, 0, 1, 1),
         (7, 1, 0, 1, 1), (0, 1, 0, 3, 1), (7, 1, 0, 3, 1), (0, 1, 0, 2, 1), (7, 1, 0, 2, 1),),
        (),
    ),
    (
        ((2, 0, 0, 0, 0), (3, 0, 0, 0, 0),),
        (),
        (),
        (),
        (),
        (),
        (),
        (),
        (),
        ((3, 0, 0, 2, 0),),
        (),
        ((2, 0, 0, 1, 0),),
        (),
        (),
        (),
        (),
        ((3, 0, 0, 3, 0), (2, 1, 0, 2, 0), (3, 1, 0, 0, 0), (2, 1, 0, 1, 0), (3, 1, 0, 3, 0),),
        (),
        (),
        (),
        (),
        (),
        (),
        (),
        (),
    ),
    (
        ((3, 0, 1, 0, 0),),
        ((2, 0, 1, 1, 0),),
        (),
        (),
        (),
        (),
        (),
        (),
        (),
        (),
        (),
        (),
        (),
        (),
        (),
        (),
        ((2, 1, 1, 1, 0), (3, 0, 1, 2, 0),),
        ((3, 0, 1, 3, 0), (1, 0, 1, 0, 0), (4, 0, 1, 0, 0), (3, 1, 1, 0, 0), (3, 0, 1, 1, 0),
         (3, 1, 1, 2, 0), (1, 0, 1, 3, 0), (4, 0, 1, 3, 0), (3, 1, 1, 3, 0), (1, 1, 1, 0, 0),
         (4, 1, 1, 0, 0), (3, 1, 1, 1, 0),),
        ((1, 1, 1, 1, 0), (4, 1, 1, 1, 0),),
        ((1, 1, 1, 2, 0), (4, 1, 1, 2, 0),),
        ((1, 0, 1, 2, 0), (4, 0, 1, 2, 0), (1, 1, 1, 3, 0), (4, 1, 1, 3, 0),),
        (),
        (),
        (),
        (),
    ),
    (
        ((5, 0, 1, 0, 0), (7, 0, 1, 0, 0),),
        (),
        (),
        (),
        (),
        ((7, 0, 1, 0, 1),),
        (),
        (),
        (),
        (),
        ((7, 0, 1, 1, 0),),
        (),
        (),
        (),
        (),
        ((7, 0, 1, 1, 1),),
        ((7, 0, 1, 2, 0), (7, 0, 1, 2, 1), (7, 0, 1, 3, 0), (7, 0, 1, 3, 1), (7, 1, 1, 0, 0),),
        ((7, 1, 1, 0, 1), (0, 0, 0, 0, 0), (5, 0, 0, 0, 0), (7, 0, 0, 0, 0), (7, 1, 1, 1, 0),
         (7, 1, 1, 1, 1), (7, 1, 1, 2, 0), (7, 1, 1, 2, 1), (7, 1, 1, 3, 0), (0, 0, 0, 1, 0),
         (5, 0, 0, 1, 0), (7, 0, 0, 1, 0), (1, 1, 1, 0, 0), (4, 1, 1, 0, 0), (7, 1, 1, 3, 1),
         (0, 0, 3, 2, 0), (6, 0, 3, 2, 0), (7, 0, 3, 2, 0), (0, 0, 0, 3, 0), (7, 0, 0, 3, 0),
         (5, 0, 0, 3, 0), (0, 0, 3, 2, 1), (7, 0, 3, 2, 1), (5, 0, 3, 2, 1), (0, 0, 3, 3, 0),
         (6, 0, 3, 3, 0), (7, 0, 3, 3, 0), (5, 0, 1, 1, 1), (5, 0, 1, 2, 0), (0, 0, 3, 3, 1),
         (7, 0, 3, 3, 1), (0, 1, 3, 2, 0), (6, 1, 3, 2, 0), (7, 1, 3, 2, 0), (5, 0, 1, 2, 1),
         (5, 0, 1, 3, 0), (0, 1, 3, 2, 1), (7, 1, 3, 2, 1), (0, 0, 3, 0, 0), (6, 0, 3, 0, 0),
         (7, 0, 3, 0, 0), (0, 1, 3, 3, 0), (7, 1, 3, 3, 0), (6, 1, 3, 3, 0), (5, 0, 1, 3, 1),
         (0, 0, 0, 2, 0), (7, 0, 0, 2, 0), (6, 0, 0, 2, 0), (0, 0, 3, 0, 1), (7, 0, 3, 0, 1),
         (5, 0, 0, 2, 0), (0, 0, 0, 0, 1), (7, 0, 0, 0, 1), (1, 1, 1, 1, 0), (4, 1, 1, 1, 0),
         (0, 1, 3, 3, 1), (7, 1, 3, 3, 1), (0, 0, 2, 1, 0), (7, 0, 2, 1, 0), (6, 0, 2, 1, 0),
         (0, 0, 0, 2, 1), (7, 0, 0, 2, 1), (5, 0, 0, 2, 1), (0, 0, 3, 1, 1), (6, 0, 3, 1, 1),
         (7, 0, 3, 1, 1), (1, 1, 1, 3, 0), (4, 1, 1, 3, 0), (0, 0, 2, 1, 1), (7, 0, 2, 1, 1),
         (5, 0, 2, 1, 1), (5, 1, 3, 3, 0), (0, 0, 2, 2, 0), (7, 0, 2, 2, 0), (6, 0, 2, 2, 0),
         (0, 1, 0, 1, 0), (7, 1, 0, 1, 0), (0, 0, 3, 1, 0), (7, 0, 3, 1, 0),),
        ((0, 1, 0, 2, 0), (7, 1, 0, 2, 0), (6, 1, 0, 2, 0), (0, 0, 0, 1, 1), (7, 0, 0, 1, 1),
         (0, 0, 2, 2, 1), (7, 0, 2, 2, 1), (5, 0, 2, 2, 1), (5, 1, 0, 1, 0), (0, 0, 2, 3, 0),
         (7, 0, 2, 3, 0), (6, 0, 2, 3, 0), (0, 0, 2, 0, 0), (6, 0, 2, 0, 0), (7, 0, 2, 0, 0),
         (0, 1, 0, 3, 0), (7, 1, 0, 3, 0), (6, 1, 0, 3, 0), (0, 1, 0, 2, 1), (7, 1, 0, 2, 1),
         (5, 1, 3, 2, 1), (0, 0, 0, 3, 1), (7, 0, 0, 3, 1),),
        ((0, 0, 2, 0, 1), (7, 0, 2, 0, 1), (5, 1, 0, 2, 1), (0, 1, 2, 3, 0), (7, 1, 2, 3, 0),
         (0, 1, 3, 0, 1), (6, 1, 3, 0, 1), (7, 1, 3, 0, 1), (0, 0, 2, 3, 1), (7, 0, 2, 3, 1),),
        ((0, 1, 0, 0, 0), (7, 1, 0, 0, 0), (0, 1, 3, 1, 1), (6, 1, 3, 1, 1), (7, 1, 3, 1, 1),
         (6, 1, 0, 0, 0), (0, 1, 0, 3, 1), (7, 1, 0, 3, 1), (5, 1, 0, 3, 1), (5, 1, 1, 0, 0),
         (0, 1, 3, 0, 0), (7, 1, 3, 0, 0), (0, 1, 2, 0, 0), (6, 1, 2, 0, 0), (7, 1, 2, 0, 0),
         (5, 1, 1, 1, 1), (0, 1, 3, 1, 0), (7, 1, 3, 1, 0),),
        ((5, 1, 1, 3, 0), (0, 1, 2, 1, 0), (7, 1, 2, 1, 0), (6, 1, 2, 1, 0), (6, 1, 2, 3, 0),
         (0, 1, 0, 0, 1), (7, 1, 0, 0, 1), (5, 1, 0, 0, 0), (0, 1, 0, 1, 1), (7, 1, 0, 1, 1),),
        ((0, 1, 2, 0, 1), (7, 1, 2, 0, 1), (5, 1, 0, 0, 1), (0, 1, 2, 2, 0), (7, 1, 2, 2, 0),
         (0, 1, 2, 1, 1), (7, 1, 2, 1, 1), (5, 1, 1, 2, 0), (0, 1, 2, 2, 1), (7, 1, 2, 2, 1),
         (0, 1, 2, 3, 1), (7, 1, 2, 3, 1),),
        ((5, 1, 1, 2, 1),),
        (),
    ),
    (
        ((2, 0, 1, 0, 0),),
        ((3, 0, 1, 1, 0),),
        (),
        ((2, 0, 1, 3, 0),),
        (),
        (),
        (),
        (),
        (),
        (),
        (),
        (),
        (),
        (),
        (),
        (),
        ((2, 1, 1, 0, 0), (1, 0, 1, 1, 0), (4, 0, 1, 1, 0), (2, 1, 1, 1, 0), (1, 1, 1, 1, 0),
         (4, 1, 1, 1, 0), (2, 1, 1, 2, 0), (2, 0, 1, 2, 0), (3, 0, 1, 2, 0), (2, 1, 1, 3, 0),
         (3, 0, 1, 3, 0),),
        ((3, 1, 1, 3, 0),),
        (),
        (),
        (),
        (),
        (),
        (),
        (),
    ),
    (
        ((3, 0, 1, 0, 0),),
        (),
        (),
        (),
        (),
        (),
        (),
        (),
        ((2, 1, 1, 0, 0),),
        (),
        (),
        (),
        (),
        (),
        (),
        (),
        ((2, 1, 1, 1, 0), (2, 1, 1, 3, 0), (0, 0, 1, 0, 0), (6, 0, 1, 0, 0), (7, 0, 1, 0, 0),
         (0, 0, 1, 0, 1), (7, 0, 1, 0, 1), (0, 0, 0, 0, 0), (6, 0, 0, 0, 0), (7, 0, 0, 0, 0),
         (0, 0, 3, 0, 0), (7, 0, 3, 0, 0), (6, 0, 3, 0, 0), (5, 0, 3, 0, 0), (0, 0, 0, 1, 0),
         (7, 0, 0, 1, 0), (6, 0, 0, 1, 0), (0, 0, 0, 0, 1), (7, 0, 0, 0, 1), (5, 0, 0, 0, 1),
         (0, 0, 3, 2, 1), (7, 0, 3, 2, 1), (6, 0, 3, 2, 1), (0, 0, 3, 0, 1), (7, 0, 3, 0, 1),
         (0, 0, 3, 1, 0), (7, 0, 3, 1, 0), (6, 0, 3, 1, 0), (0, 0, 0, 3, 0), (7, 0, 0, 3, 0),
         (0, 0, 0, 1, 1), (7, 0, 0, 1, 1), (0, 0, 1, 1, 1), (7, 0, 1, 1, 1), (6, 0, 0, 3, 0),
         (0, 0, 3, 1, 1), (7, 0, 3, 1, 1), (5, 0, 3, 1, 1), (0, 0, 3, 3, 0), (7, 0, 3, 3, 0),
         (6, 0, 3, 3, 0), (3, 0, 1, 3, 0), (0, 0, 1, 2, 0), (7, 0, 1, 2, 0), (6, 0, 1, 1, 1),
         (0, 0, 3, 2, 0), (7, 0, 3, 2, 0), (5, 0, 0, 1, 1), (0, 0, 1, 2, 1), (7, 0, 1, 2, 1),
         (0, 0, 3, 3, 1), (7, 0, 3, 3, 1),),
        ((0, 1, 3, 0, 0), (7, 1, 3, 0, 0), (6, 1, 3, 0, 0), (3, 0, 1, 1, 0), (0, 0, 1, 3, 0),
         (7, 0, 1, 3, 0), (0, 0, 0, 3, 1), (7, 0, 0, 3, 1), (0, 0, 2, 0, 0), (7, 0, 2, 0, 0),
         (5, 0, 2, 0, 0), (0, 0, 1, 3, 1), (7, 0, 1, 3, 1), (6, 0, 2, 0, 0), (0, 0, 1, 1, 0),
         (7, 0, 1, 1, 0),),
        ((0, 1, 3, 1, 0), (7, 1, 3, 1, 0), (6, 1, 3, 1, 0), (3, 0, 1, 2, 0), (5, 0, 0, 3, 1),
         (0, 0, 0, 2, 0), (7, 0, 0, 2, 0), (0, 1, 3, 0, 1), (7, 1, 3, 0, 1), (5, 1, 3, 0, 1),
         (0, 0, 0, 2, 1), (7, 0, 0, 2, 1),),
        ((0, 0, 2, 3, 0), (6, 0, 2, 3, 0), (7, 0, 2, 3, 0), (0, 1, 3, 1, 1), (7, 1, 3, 1, 1),
         (3, 1, 1, 2, 0), (5, 1, 3, 1, 1), (0, 0, 2, 1, 1), (7, 0, 2, 1, 1), (6, 0, 2, 1, 1),
         (0, 0, 2, 0, 1), (7, 0, 2, 0, 1), (3, 1, 1, 3, 0), (0, 1, 3, 3, 0), (7, 1, 3, 3, 0),
         (6, 1, 3, 3, 0), (0, 0, 2, 3, 1), (7, 0, 2, 3, 1), (0, 0, 2, 2, 1), (7, 0, 2, 2, 1),
         (0, 0, 2, 1, 0), (7, 0, 2, 1, 0), (0, 1, 3, 2, 0), (7, 1, 3, 2, 0), (0, 1, 0, 1, 0),
         (6, 1, 0, 1, 0), (7, 1, 0, 1, 0), (0, 1, 2, 0, 0), (5, 1, 2, 0, 0), (6, 1, 2, 0, 0),
         (7, 1, 2, 0, 0), (0, 1, 3, 3, 1), (7, 1, 3, 3, 1), (0, 1, 3, 2, 1), (7, 1, 3, 2, 1),
         (0, 1, 2, 1, 0), (5, 1, 2, 1, 0), (7, 1, 2, 1, 0), (6, 1, 2, 1, 0), (0, 1, 0, 1, 1),
         (5, 1, 0, 1, 1), (7, 1, 0, 1, 1), (0, 1, 0, 2, 1), (7, 1, 0, 2, 1), (6, 1, 0, 2, 1),
         (0, 1, 2, 2, 0), (7, 1, 2, 2, 0), (6, 1, 2, 2, 0), (5, 1, 2, 2, 0), (0, 1, 2, 0, 1),
         (7, 1, 2, 0, 1), (0, 1, 0, 3, 1), (7, 1, 0, 3, 1), (0, 0, 2, 2, 0), (7, 0, 2, 2, 0),),
        ((0, 1, 2, 1, 1), (7, 1, 2, 1, 1),),
        ((0, 1, 1, 0, 0), (7, 1, 1, 0, 0), (6, 1, 0, 3, 1), (0, 1, 2, 3, 0), (7, 1, 2, 3, 0),
         (6, 1, 2, 3, 0), (0, 1, 2, 2, 1), (5, 1, 2, 2, 1), (7, 1, 2, 2, 1), (0, 1, 1, 1, 1),
         (7, 1, 1, 1, 1), (6, 1, 1, 0, 0), (0, 1, 0, 2, 0), (7, 1, 0, 2, 0), (0, 1, 1, 3, 0),
         (7, 1, 1, 3, 0), (6, 1, 1, 1, 1), (0, 1, 2, 3, 1), (7, 1, 2, 3, 1),),
        ((0, 1, 0, 0, 0), (7, 1, 0, 0, 0), (6, 1, 1, 3, 0), (0, 1, 0, 3, 0), (7, 1, 0, 3, 0),
         (0, 1, 0, 0, 1), (7, 1, 0, 0, 1),),
        ((0, 1, 1, 0, 1), (7, 1, 1, 0, 1), (0, 1, 1, 2, 0), (7, 1, 1, 2, 0), (0, 1, 1, 1, 0),
         (7, 1, 1, 1, 0), (0, 1, 1, 2, 1), (7, 1, 1, 2, 1), (0, 1, 1, 3, 1), (7, 1, 1, 3, 1),),
        (),
    ),
)


def local_plain(tokens, norm_gain, up_trained, down_trained):
    shards = lax.axis_size("fs")
    groups = lax.axis_size("tp")
    rows_local = up_trained.shape[0]
    cols_local = up_trained.shape[1]
    folded = (norm_gain[:, None] * up_trained).astype(jnp.bfloat16)
    stacked = jnp.stack([folded, down_trained.astype(jnp.bfloat16)])
    served_width = cols_local * groups // shards
    blocks_here = cols_local // served_width
    quarter_rows = rows_local // groups
    pieces = stacked.reshape(2, groups, quarter_rows, blocks_here, served_width)
    moved = lax.all_to_all(pieces, "tp", split_axis=1, concat_axis=3, tiled=True)
    placed = lax.all_to_all(moved, "fs", split_axis=3, concat_axis=2, tiled=True)
    ordered = placed.reshape(2, shards, quarter_rows, served_width)
    joined = lax.all_gather(ordered, "tp", axis=2, tiled=True)
    owned = joined.reshape(2, rows_local * shards, served_width)
    up_serving = owned[0]
    down_serving = owned[1]
    values = tokens.astype(jnp.float32)
    scale = lax.rsqrt(jnp.mean(values * values, axis=1, keepdims=True) + epsilon)
    normed = (values * scale).astype(jnp.bfloat16)
    hidden = jnp.dot(normed, up_serving, preferred_element_type=jnp.float32)
    active = jnp.square(jax.nn.relu(hidden)).astype(jnp.bfloat16)
    summed = lax.psum_scatter(
        lax.dot_general(
            down_serving, active, (((1,), (1,)), ((), ())), preferred_element_type=jnp.float32
        ),
        "fs",
        scatter_dimension=0,
        tiled=True,
    )
    prompt_output = summed.T.astype(jnp.bfloat16)
    return (up_serving, down_serving, prompt_output)


def down_block(active, whole, plane, put):
    rows_local = whole.shape[1] // 4
    tile = 256 if rows_local % 256 == 0 else rows_local

    @pl.loop(0, rows_local // tile)
    def _(n):
        rows = pl.ds(pl.multiple_of(plane * rows_local + n * tile, tile), tile)
        product = lax.dot_general(
            active[...], whole[1, rows, :], (((1,), (1,)), ((), ())),
            preferred_element_type=jnp.float32,
        )
        put(pl.ds(pl.multiple_of(n * tile, tile), tile), product)


def kernel(
    tokens_hbm, gain_hbm, up_hbm, down_hbm, whole, active, rs_recv,
    raw, gain_rows, gain, cast, relay, toks, normed, hidden, rs_send,
    in_sem, misc_sem, got_sem, relay_sem, src_sem, out_sem, rs_ssem, rs_rsem,
):
    y = lax.axis_index("grp")
    z = lax.axis_index("fs")
    t = lax.axis_index("tp")
    mirrored = z // 2
    role = jnp.where(mirrored == 1, 4 * (3 - z) + (3 - t), 4 * z + t)
    is_own = z == t
    is_active = t % 2 == z % 2
    t_x = jnp.where(t < 2, t + 2, t - 2)
    t_c = t + 1 - 2 * (t % 2)
    to_x = {"tp": t_x}
    to_c = {"tp": t_c}
    to_y = {"grp": 1 - y}
    rows_local, width = cast.shape[1], cast.shape[2]
    size = rows_local // (2 * PAIRS)
    trained = (up_hbm, down_hbm)
    planes = [jnp.where(mirrored == 1, 3 - k, k) for k in range(4)]
    sides = [y, 1 - y]

    def part(pair, side):
        return 2 * pair + sides[side]

    def ds(start, extent):
        return pl.ds(pl.multiple_of(start, extent), extent)

    def local_rows(pair, side):
        return ds(part(pair, side) * size, size)

    def unit(m, plane, pair, side):
        return whole.at[m, ds(plane * rows_local + part(pair, side) * size, size)]

    def remote(src, dst, ssem, rsem, where):
        return pltpu.make_async_remote_copy(
            src_ref=src, dst_ref=dst, send_sem=ssem, recv_sem=rsem,
            device_id=where, device_id_type=MESH,
        )

    def fetch(m, pair, side):
        rows = local_rows(pair, side)
        return pltpu.make_async_copy(
            trained[m].at[rows], raw.at[m, rows], in_sem.at[m, 2 * pair + side]
        )

    get_gain = pltpu.make_async_copy(gain_hbm, gain_rows, misc_sem.at[0])
    get_toks = pltpu.make_async_copy(tokens_hbm, toks, misc_sem.at[1])
    get_gain.start()
    for pair in range(PAIRS):
        fetch(0, pair, 0).start()

    barrier = pltpu.get_barrier_semaphore()
    others = [{"fs": lax.rem(z + k, 4)} for k in range(1, 4)]
    for where in [to_x, to_c, to_y] + others:
        pl.semaphore_signal(barrier, inc=1, device_id=where, device_id_type=MESH)

    get_gain.wait()
    lanes = gain_rows.shape[1]
    for q in range(gain_rows.shape[0]):
        square = (lanes, lanes)
        chosen = jnp.where(
            lax.broadcasted_iota(jnp.int32, square, 0) == lax.broadcasted_iota(jnp.int32, square, 1),
            jnp.broadcast_to(gain_rows[pl.ds(q, 1), :], square), 0.0,
        )
        column = jnp.sum(chosen, axis=1, keepdims=True)
        gain[pl.ds(q * lanes, lanes), :] = jnp.broadcast_to(column, square)

    tokens_here = toks.shape[0]
    piece = 16

    def norm():
        get_toks.wait()

        @pl.loop(0, tokens_here // piece)
        def _(i):
            here = ds(i * piece, piece)
            values = toks[here, :].astype(jnp.float32)
            scale = lax.rsqrt(jnp.mean(values * values, axis=1, keepdims=True) + epsilon)
            normed[here, :] = (values * scale).astype(jnp.bfloat16)

    def cast_unit(m, pair, side):
        fetch(m, pair, side).wait()
        base = part(pair, side) * size

        def store(into, shift):
            @pl.loop(0, size // piece)
            def _(i):
                here = ds(base + i * piece, piece)
                there = ds(shift + base + i * piece, piece)
                if m == 0:
                    factor = gain[here, :]
                    for j in range(width // lanes):
                        cols = pl.ds(j * lanes, lanes)
                        into[0, there, cols] = (raw[0, here, cols] * factor).astype(jnp.bfloat16)
                else:
                    into[m, there, :] = raw[m, here, :].astype(jnp.bfloat16)

        @pl.when(is_own)
        def _():
            store(whole, z * rows_local)

        if side == 0:
            @pl.when(jnp.logical_not(is_own))
            def _():
                store(cast, 0)

    def step(kind, m, k, pair, side):
        plane = planes[k]
        place = part(pair, side)
        if kind == GET:
            here = unit(m, plane, pair, side)
            remote(here, here, out_sem.at[0, m], got_sem.at[m, plane, place], to_x).wait_recv()
        elif kind == GET_RELAY:
            here = relay.at[m, ds(place * size, size)]
            remote(here, here, src_sem.at[m], relay_sem.at[m, pair], to_x).wait_recv()
        elif kind == SWAP:
            remote(
                cast.at[m, local_rows(pair, side)], relay.at[m, ds(place * size, size)],
                src_sem.at[m], relay_sem.at[m, pair], to_x,
            ).start()
        elif kind in (HOP, HOP_RELAY):
            src = (cast if kind == HOP else relay).at[m, ds(place * size, size)]
            remote(
                src, unit(m, z, pair, side), src_sem.at[m], got_sem.at[m, z, place],
                {"fs": t if kind == HOP else t_x},
            ).start()
        elif kind == SEND_CORE:
            here = unit(m, plane, pair, side)
            remote(here, here, out_sem.at[2, m], got_sem.at[m, plane, 0], to_c).start()
        else:
            here = unit(m, plane, pair, side)
            i = kind - SEND_X
            remote(
                here, here, out_sem.at[i, m], got_sem.at[m, plane, place], (to_x, to_y)[i]
            ).start()

    def run(segment):
        for r in range(8):
            if SCHEDULE[r][segment]:
                @pl.when(role == r)
                def _():
                    for s in SCHEDULE[r][segment]:
                        step(*s)

    casts = [(m, pair, side) for m in range(2) for side in range(2) for pair in range(PAIRS)]
    segment = 0
    for m, pair, side in casts:
        if side == 1:
            pl.when(is_own)(lambda: cast_unit(m, pair, side))
        else:
            cast_unit(m, pair, side)
        if segment == 0:
            @pl.when(is_own)
            def _():
                for p in range(PAIRS):
                    fetch(0, p, 1).start()
            for p in range(PAIRS):
                fetch(1, p, 0).start()
            @pl.when(is_own)
            def _():
                for p in range(PAIRS):
                    fetch(1, p, 1).start()
            get_toks.start()
            pl.when(z == 0)(norm)
            pl.semaphore_wait(barrier, 6)
        run(segment)
        segment += 1

    pl.when(z != 0)(norm)

    def pick(table):
        chosen = planes[table[0]]
        for r in range(1, 8):
            if table[r] != table[0]:
                chosen = jnp.where(role == r, planes[table[r]], chosen)
        return chosen

    def listen(m, plane):
        @pl.when(jnp.logical_not(is_active))
        def _():
            here = whole.at[m, ds(plane * rows_local, rows_local)]
            remote(here, here, out_sem.at[2, m], got_sem.at[m, plane, 0], to_c).wait_recv()

    tile = 512 if width % 512 == 0 else width

    def compute_up(k):
        plane = pick(ORDER[0][k])
        listen(0, plane)
        rows = ds(plane * rows_local, rows_local)

        @pl.loop(0, width // tile)
        def _(n):
            cols = ds(n * tile, tile)
            product = jnp.dot(
                normed[:, rows], whole[0, rows, cols], preferred_element_type=jnp.float32
            )
            if k > 0:
                product = product + hidden[:, cols]
            if k < 3:
                hidden[:, cols] = product
            else:
                active[:, cols] = jnp.square(jnp.maximum(product, 0.0)).astype(jnp.bfloat16)

    def scatter(k, plane):
        slot = lax.rem(z - plane + 3, 4)
        return remote(
            rs_send.at[k], rs_recv.at[slot], rs_ssem.at[k], rs_rsem.at[slot], {"fs": plane}
        )

    def compute_down(k):
        plane = pick(ORDER[1][k])
        listen(1, plane)

        down_block(
            active, whole, plane,
            lambda cols, product: rs_send.__setitem__((k, slice(None), cols), product.astype(jnp.bfloat16)),
        )
        scatter(k, plane).start()

    for m in range(2):
        for k in range(4):
            run(segment)
            segment += 1
            if m == 0:
                compute_up(k)
            elif k < 3:
                compute_down(k)
            else:
                listen(1, z)
    run(segment)

    for k in range(3):
        here = rs_recv.at[k]
        remote(here, here, rs_ssem.at[k], rs_rsem.at[k], {"fs": lax.rem(z + 1, 4)}).wait_recv()

    def drain(sem, m, count):
        sent = whole.at[m, pl.ds(0, count * size)]
        remote(sent, sent, sem, got_sem.at[0, 0, 0], to_x).wait_send()

    for r in range(8):
        @pl.when(role == r)
        def _():
            for m in range(2):
                steps = [s for part_of in SCHEDULE[r] for s in part_of if s[1] == m]
                hops = sum(s[0] in (SWAP, HOP, HOP_RELAY) for s in steps)
                if hops:
                    drain(src_sem.at[m], m, hops)
                for i, kind in enumerate((SEND_X, SEND_Y, SEND_CORE)):
                    sends = sum(s[0] == kind for s in steps)
                    if sends:
                        drain(out_sem.at[i, m], m, sends)
    for k in range(3):
        here = rs_send.at[k]
        remote(here, here, rs_ssem.at[k], rs_rsem.at[k], {"fs": lax.rem(z + 1, 4)}).wait_send()


pieces_out = 8


def deliver(whole, active, rs_recv, up_out, down_out, prompt_out, own, prompt, sems, last):
    rows = whole.shape[1] // pieces_out
    copies = [
        pltpu.make_async_copy(
            whole.at[m, pl.ds(i * rows, rows)], out.at[pl.ds(i * rows, rows)], sems.at[m]
        )
        for m, out in enumerate((up_out, down_out))
        for i in range(pieces_out)
    ]
    for copy in copies:
        copy.start()
    down_block(
        active, whole, lax.axis_index("fs"),
        lambda cols, product: own.__setitem__((slice(None), cols), product),
    )
    piece = 16

    @pl.loop(0, own.shape[0] // piece)
    def _(i):
        here = pl.ds(pl.multiple_of(i * piece, piece), piece)
        total = own[here, :]
        for k in range(3):
            total = total + rs_recv[k, here, :].astype(jnp.float32)
        prompt[here, :] = total.astype(prompt.dtype)

    final = pltpu.make_async_copy(prompt, prompt_out, last)
    final.start()
    for m, out in enumerate((up_out, down_out)):
        pltpu.make_async_copy(whole.at[m], out, sems.at[m]).wait()
    final.wait()


def local_kernel(tokens, norm_gain, up_trained, down_trained):
    shards = lax.axis_size("fs")
    rows_local, width = up_trained.shape
    tokens_here, features = tokens.shape
    any_space = pl.BlockSpec(memory_space=pl.ANY)
    dma = pltpu.SemaphoreType.DMA
    bf16, f32 = jnp.bfloat16, jnp.float32
    results = pl.pallas_call(
        kernel,
        out_shape=(
            pltpu.VMEM((2, rows_local * shards, width), bf16),
            pltpu.VMEM((tokens_here, width), bf16),
            pltpu.VMEM((3, tokens_here, rows_local), bf16),
        ),
        in_specs=[any_space] * 4,
        out_specs=(pl.BlockSpec(memory_space=pltpu.VMEM),) * 3,
        scratch_shapes=[
            pltpu.VMEM((2, rows_local, width), f32),
            pltpu.VMEM((rows_local // 128, 128), f32),
            pltpu.VMEM((rows_local, 128), f32),
            pltpu.VMEM((2, rows_local, width), bf16),
            pltpu.VMEM((2, rows_local, width), bf16),
            pltpu.VMEM((tokens_here, features), bf16),
            pltpu.VMEM((tokens_here, features), bf16),
            pltpu.VMEM((tokens_here, width), f32),
            pltpu.VMEM((3, tokens_here, rows_local), bf16),
            dma((2, 2 * PAIRS)), dma((2,)),
            dma((2, 4, 2 * PAIRS)), dma((2, PAIRS)),
            dma((2,)), dma((3, 2)), dma((3,)), dma((3,)),
        ],
        compiler_params=pltpu.CompilerParams(
            collective_id=0, has_side_effects=True, vmem_limit_bytes=40 * 1024 * 1024
        ),
    )(tokens, norm_gain.reshape(rows_local // 128, 128), up_trained, down_trained)
    held = pl.BlockSpec(memory_space=pltpu.VMEM)
    return tuple(pl.pallas_call(
        deliver,
        out_shape=(
            jax.ShapeDtypeStruct((rows_local * shards, width), bf16),
            jax.ShapeDtypeStruct((rows_local * shards, width), bf16),
            jax.ShapeDtypeStruct((tokens_here, rows_local), bf16),
        ),
        in_specs=[held] * 3,
        out_specs=(any_space,) * 3,
        scratch_shapes=[
            pltpu.VMEM((tokens_here, rows_local), f32), pltpu.VMEM((tokens_here, rows_local), bf16),
            dma((2,)), dma(()),
        ],
        compiler_params=pltpu.CompilerParams(vmem_limit_bytes=8 * 1024 * 1024),
    )(*results))


def solution(mesh):
    in_specs = (P(("grp", "tp"), None), P("fs"), P("fs", "tp"), P("fs", "tp"))
    out_specs = (P("grp", "fs"), P("grp", "fs"), P(("grp", "tp"), "fs"))
    sizes = mesh.shape
    square = sizes["grp"] == 2 and sizes["fs"] == 4 and sizes["tp"] == 4
    local = local_kernel if square else local_plain
    return jax.shard_map(local, mesh=mesh, in_specs=in_specs, out_specs=out_specs, check_vma=False)
```
